512 devices in a mesh: sp: 32 (over z, x), tp: 16 (over y, core).
Axes of the slice: x: 4, y: 8, z: 8, core: 2. Of those that a mesh axis runs over, the one named last changes fastest.
Arguments:
- query_matrix: bfloat16 [8192, 1024], P('sp', 'tp'), may hold values from -6 to 6
- key_matrix: bfloat16 [8192, 1024], P('sp', 'tp'), may hold values from -6 to 6
- value_matrix: bfloat16 [8192, 2048], P('sp', 'tp'), may hold values from -6 to 6
- output_gate_rows: bfloat16 [8192, 2048], P('sp', 'tp'), may hold values from -6 to 6
- decay_preactivation: bfloat16 [8192, 1024], P('sp', 'tp'), may hold values from -5 to 5
- channel_decay_bias: float32 [1024], P('tp'), may hold values from 0 to 10
- extra_log_decay: float32 [8192, 16], P('sp', 'tp'), may hold values from -0.7 to 0
- head_norm_gain: float32 [128], replicated, may hold values from 0.1 to 1.9
- output_projection: bfloat16 [2048, 2048], P('tp'), may hold values from -0.125 to 0.125
- residual_input: bfloat16 [8192, 2048], P(('sp', 'tp')), may hold values from -6 to 6
- attention_norm_gain: float32 [2048], replicated, may hold values from 0.1 to 1.9
- expert_before_gain: float32 [2048], replicated, may hold values from 0.1 to 1.9
- expert_after_gain: float32 [2048], replicated, may hold values from 0.1 to 1.9
- expert_gate_weight: bfloat16 [32, 2048, 4096], P('sp', None, 'tp'), may hold values from -0.125 to 0.125
- expert_up_weight: bfloat16 [32, 2048, 4096], P('sp', None, 'tp'), may hold values from -0.125 to 0.125
- expert_down_weight: bfloat16 [32, 4096, 2048], P('sp', 'tp'), may hold values from -0.09375 to 0.09375
- token_expert_index: int32 [8192, 2], P('sp'), may hold values from 0 to 31, as said below
- routing_weight_matrix: float32 [8192, 2], P('sp'), may hold values from 0.1 to 1
Outputs:
- layer_out: bfloat16 [8192, 2048], P(('sp', 'tp'))
The draws below stay inside these ranges and needn't reach their ends.
Inputs may be any that keep to these rules, and one draw needn't show every extreme that they name: `token_expert_index`: the 2 experts of a token differ and lie in one group: they have the same value of e // 4. In each aligned block of 256 rows (the rows of one index of sp) no expert is named by more than 20 rows, and the 4 experts of one group are each named by exactly 20 rows in every block.
All inputs are finite; a program needn't handle non-finite values.
Results may differ from the reference program's by a relative error of at most 0.024.
Values may be sent and summed in bfloat16 or wider, within the bound.
A program may use at most 64 MiB of HBM per device.

```python
import jax
import jax.numpy as jnp
from jax import lax

D = 2048
HEAD_TOTAL = 16
KEY_CHANNELS = 64
DV = 128
FF = 4096
GROUP_SIZE = 4
TOP = 2
BLOCK = 64
TOK_DEV = 256
SEQUENCE_TOKENS = 8192
KEYW = 1024
VALW = 2048
EXPERTS = 32
N_SP = 32
N_TP = 16


def draw_decay_preactivation(key, part):
    noise_key, shift_key = jax.random.split(jax.random.fold_in(key, 12))
    block_count = SEQUENCE_TOKENS // TOK_DEV
    noise = jnp.clip(jax.random.normal(noise_key, (block_count, TOK_DEV, KEYW), jnp.float32), -4.0, 4.0)
    shift = jax.random.uniform(shift_key, (block_count, 1, KEYW), jnp.float32, -1.0, 1.0)
    return (noise + shift).reshape(SEQUENCE_TOKENS, KEYW).astype(jnp.bfloat16)


def draw_channel_decay_bias(key, part):
    pick_key, fast_key, slow_key = jax.random.split(jax.random.fold_in(key, 11), 3)
    fast_share = 0.5
    fast_head = jax.random.uniform(pick_key, (HEAD_TOTAL, 1), jnp.float32) < fast_share
    fast_bias = jax.random.uniform(fast_key, (HEAD_TOTAL, KEY_CHANNELS), jnp.float32, 0.0, 1.0)
    slow_bias = jax.random.uniform(slow_key, (HEAD_TOTAL, KEY_CHANNELS), jnp.float32, 8.5, 10.0)
    return jnp.where(fast_head, fast_bias, slow_bias).reshape(HEAD_TOTAL * KEY_CHANNELS)


def draw_extra_log_decay(key, part):
    position_random_key, size_key = jax.random.split(jax.random.fold_in(key, 13))
    spike_positions = jax.random.randint(position_random_key, (3, HEAD_TOTAL), 0, SEQUENCE_TOKENS)
    kept_share = jax.random.uniform(size_key, (3, HEAD_TOTAL), jnp.float32, 0.5, 0.8)
    match_table = (jnp.arange(SEQUENCE_TOKENS)[:, None, None] == spike_positions[None]).astype(jnp.float32)
    return jnp.sum(match_table * jnp.log(kept_share)[None], axis=1)


def draw_token_expert_index(key, part):
    base_key = jax.random.fold_in(key, 14)
    group_count = N_SP // GROUP_SIZE
    capacity = 5 * TOK_DEV // (2 * N_SP)
    full_rows = 2 * capacity
    others = group_count - 1
    unit_count = (TOK_DEV - full_rows) // GROUP_SIZE
    full_group = jax.random.randint(jax.random.fold_in(base_key, 0), (), 0, group_count)
    mark_index = jnp.arange(others + 1, dtype=jnp.int32)
    marks_base = mark_index * unit_count // others
    interior = ((mark_index > 0) & (mark_index < others)).astype(jnp.int32)
    jitter = jax.random.randint(jax.random.fold_in(base_key, 1), (N_SP, others + 1), 0, 2) * interior[None, :]
    bounds = full_rows + GROUP_SIZE * (marks_base[None, :] + jitter)
    ranks = jnp.arange(TOK_DEV, dtype=jnp.int32)
    passed = jnp.sum((ranks[None, :, None] >= bounds[:, None, 1:others]).astype(jnp.int32), axis=2)
    group_start = jnp.take_along_axis(bounds, passed, axis=1)
    in_full = ranks[None, :] < full_rows
    local_rank = jnp.where(in_full, ranks[None, :], ranks[None, :] - group_start)
    group_id = jnp.where(in_full, full_group, passed + (passed >= full_group).astype(jnp.int32))
    offsets = jax.random.randint(jax.random.fold_in(base_key, 2), (N_SP, group_count), 0, GROUP_SIZE)
    strides = jax.random.randint(jax.random.fold_in(base_key, 3), (N_SP, group_count), 1, GROUP_SIZE)
    offset_row = jnp.take_along_axis(offsets, group_id, axis=1)
    stride_row = jnp.take_along_axis(strides, group_id, axis=1)
    first_expert = group_id * GROUP_SIZE + (local_rank + offset_row) % GROUP_SIZE
    second_expert = group_id * GROUP_SIZE + (local_rank + offset_row + stride_row) % GROUP_SIZE
    paired = jnp.stack([first_expert, second_expert], axis=-1)
    order_keys = jax.random.split(jax.random.fold_in(base_key, 4), N_SP)
    orders = jax.vmap(lambda order_key: jax.random.permutation(order_key, TOK_DEV))(order_keys)
    block_rows = jnp.arange(N_SP, dtype=jnp.int32)[:, None]
    placed = jnp.zeros_like(paired).at[block_rows, orders].set(paired)
    return placed.reshape(SEQUENCE_TOKENS, TOP).astype(jnp.int32)


def block_levels(rng, shape, shards, least, top_value):
    def one(axis_at, blocks):
        draws = jax.random.uniform(jax.random.fold_in(jax.random.fold_in(rng, 6), axis_at), (blocks,), jnp.float32, least / len(shards), top_value / len(shards))
        return jnp.repeat(jnp.exp(draws), shape[axis_at] // blocks).reshape((-1,) + (1,) * (len(shape) - axis_at - 1))

    loudness = one(*shards[0])
    for cut in shards[1:]:
        loudness = loudness * one(*cut)
    return loudness


def gaussian(key, extent, deviation, bound, cuts=(), kind=jnp.bfloat16):
    gain = block_levels(key, extent, cuts, -0.22, 0.18) if cuts else 1.0
    entries = jax.random.normal(key, extent, jnp.float32) * deviation * gain
    return jnp.minimum(jnp.maximum(entries, -bound), bound).astype(kind)


def setup_inputs(seed: int = 0) -> dict:
    streams_of = jax.random.split(jax.random.key(seed), 19)
    return {
        "query_matrix": gaussian(streams_of[0], (SEQUENCE_TOKENS, KEYW), 1.0, 6.0, ((0, 32), (1, 16))),
        "key_matrix": gaussian(streams_of[1], (SEQUENCE_TOKENS, KEYW), 1.0, 6.0, ((0, 32), (1, 16))),
        "value_matrix": gaussian(streams_of[2], (SEQUENCE_TOKENS, VALW), 1.0, 6.0, ((0, 32), (1, 16))),
        "output_gate_rows": gaussian(streams_of[3], (SEQUENCE_TOKENS, VALW), 1.0, 6.0, ((0, 32), (1, 16))),
        "decay_preactivation": draw_decay_preactivation(jax.random.fold_in(streams_of[18], 71), 0),
        "channel_decay_bias": draw_channel_decay_bias(jax.random.fold_in(streams_of[18], 71), 0),
        "extra_log_decay": draw_extra_log_decay(jax.random.fold_in(streams_of[18], 71), 0),
        "head_norm_gain": jnp.clip(1.0 + 0.18 * jax.random.normal(streams_of[7], (DV,), jnp.float32), 0.1, 1.9),
        "output_projection": gaussian(streams_of[8], (VALW, D), VALW ** -0.5, 0.125, ((0, 16),)),
        "residual_input": gaussian(streams_of[9], (SEQUENCE_TOKENS, D), 1.0, 6.0, ((0, 512),)),
        "attention_norm_gain": jnp.clip(1.0 + 0.18 * jax.random.normal(streams_of[10], (D,), jnp.float32), 0.1, 1.9),
        "expert_before_gain": jnp.clip(1.0 + 0.18 * jax.random.normal(streams_of[11], (D,), jnp.float32), 0.1, 1.9),
        "expert_after_gain": jnp.clip(1.0 + 0.18 * jax.random.normal(streams_of[12], (D,), jnp.float32), 0.1, 1.9),
        "expert_gate_weight": gaussian(streams_of[13], (EXPERTS, D, FF), D ** -0.5, 0.125, ((0, 32), (2, 16))),
        "expert_up_weight": gaussian(streams_of[14], (EXPERTS, D, FF), D ** -0.5, 0.125, ((0, 32), (2, 16))),
        "expert_down_weight": gaussian(streams_of[15], (EXPERTS, FF, D), FF ** -0.5, 0.09375, ((0, 32), (1, 16))),
        "token_expert_index": draw_token_expert_index(jax.random.fold_in(streams_of[18], 71), 0),
        "routing_weight_matrix": jnp.clip(0.1 + 0.9 * jax.random.uniform(streams_of[17], (SEQUENCE_TOKENS, TOP), jnp.float32) ** block_levels(streams_of[17], (SEQUENCE_TOKENS, TOP), ((0, 32),), -0.2, 0.2), 0.1, 1.0),
    }


EPSILON = 1e-06
DECAY_NORMALIZER = 16.0
HIGHEST = lax.Precision.HIGHEST

def rms_scale(values, gain_row):
    return values * lax.rsqrt(lax.optimization_barrier(jnp.mean(values * values, axis=-1, keepdims=True)) + EPSILON) * gain_row

def rounded(values):
    return lax.optimization_barrier(values.astype(jnp.bfloat16)).astype(jnp.float32)

def blockwise_state(queries, keys_all, values_all, decay_logarithm):
    sequence_length, number_heads, width_k = queries.shape
    width_v = values_all.shape[-1]
    blocks = sequence_length // BLOCK
    q_blocks = queries.reshape(blocks, BLOCK, number_heads, width_k)
    k_blocks = keys_all.reshape(blocks, BLOCK, number_heads, width_k)
    v_blocks = values_all.reshape(blocks, BLOCK, number_heads, width_v)
    inside = jnp.cumsum(decay_logarithm.reshape(blocks, BLOCK, number_heads, width_k), axis=1)
    block_end = inside[:, -1:]
    q_decayed = q_blocks * jnp.exp(inside)
    k_inverse = k_blocks * jnp.exp(-inside)
    k_to_end = k_blocks * jnp.exp(block_end - inside)
    causal = jnp.tril(jnp.ones((BLOCK, BLOCK), dtype=bool))
    scores = jnp.einsum('nihd,njhd->nhij', q_decayed, k_inverse, precision=HIGHEST)
    scores = jnp.where(causal, scores, 0.0)
    within = jnp.einsum('nhij,njhv->nihv', scores, v_blocks, precision=HIGHEST)
    growth = jnp.einsum('nchd,nchv->nhdv', k_to_end, v_blocks, precision=HIGHEST)
    fade_rows = jnp.exp(block_end[:, 0])

    def advance(running_state, inputs_pair):
        fade_now, grow_now = inputs_pair
        return (fade_now[..., None] * running_state + grow_now, running_state)
    zero_state = jnp.zeros((number_heads, width_k, width_v), jnp.float32)
    _, starts = lax.scan(advance, zero_state, (fade_rows, growth))
    across = jnp.einsum('nchd,nhdv->nchv', q_decayed, starts, precision=HIGHEST)
    return (within + across).reshape(sequence_length, number_heads, width_v)

def reference(query_matrix, key_matrix, value_matrix, output_gate_rows, decay_preactivation, channel_decay_bias, extra_log_decay, head_norm_gain, output_projection, residual_input, attention_norm_gain, expert_before_gain, expert_after_gain, expert_gate_weight, expert_up_weight, expert_down_weight, token_expert_index, routing_weight_matrix):
    sequence_length = query_matrix.shape[0]
    number_heads = value_matrix.shape[1] // DV
    model_width = residual_input.shape[1]
    queries = query_matrix.astype(jnp.float32).reshape(sequence_length, number_heads, KEY_CHANNELS) * KEY_CHANNELS ** (-0.5)
    keys_all = key_matrix.astype(jnp.float32).reshape(sequence_length, number_heads, KEY_CHANNELS)
    values_all = value_matrix.astype(jnp.float32).reshape(sequence_length, number_heads, DV)
    decay_logarithm = jax.nn.log_sigmoid(decay_preactivation.astype(jnp.float32) + channel_decay_bias) / DECAY_NORMALIZER
    decay_logarithm = decay_logarithm.reshape(sequence_length, number_heads, KEY_CHANNELS) + extra_log_decay[:, :, None]
    attn = blockwise_state(queries, keys_all, values_all, decay_logarithm)
    gate_act = jax.nn.silu(output_gate_rows.astype(jnp.float32).reshape(sequence_length, number_heads, DV))
    gated = (rms_scale(attn, head_norm_gain) * gate_act).astype(jnp.bfloat16)
    per_group = number_heads // N_TP
    grouped = gated.reshape(sequence_length, N_TP, per_group * DV).transpose(1, 0, 2)
    group_weights = output_projection.reshape(N_TP, per_group * DV, model_width)

    def add_group(total_sum, pair_in):
        group_rows, group_weight = pair_in
        return (total_sum + rounded(jnp.dot(group_rows, group_weight, preferred_element_type=jnp.float32)), None)
    mixed, _ = lax.scan(add_group, jnp.zeros((sequence_length, model_width), jnp.float32), (grouped, group_weights))
    layer_mid = (residual_input.astype(jnp.float32) + rms_scale(mixed, attention_norm_gain)).astype(jnp.bfloat16)
    normed = rms_scale(layer_mid.astype(jnp.float32), expert_before_gain).astype(jnp.bfloat16)
    expert_count = N_SP
    capacity = 5 * TOK_DEV // (2 * expert_count)
    block_ids = token_expert_index.reshape(N_SP, TOK_DEV * TOP)
    one_hot = (block_ids[:, :, None] == jnp.arange(expert_count, dtype=jnp.int32)[None, None, :]).astype(jnp.int32)
    slot_index = lax.optimization_barrier(jnp.sum((jnp.cumsum(one_hot, axis=1) - one_hot) * one_hot, axis=2))
    block_index = jnp.arange(N_SP, dtype=jnp.int32)[:, None]
    target = (block_ids * N_SP + block_index) * capacity + slot_index
    owners = jnp.zeros((expert_count * N_SP * capacity,), jnp.int32)
    owners = owners.at[target.reshape(-1)].set(jnp.arange(sequence_length * TOP, dtype=jnp.int32) // TOP)
    owners = owners.reshape(expert_count, N_SP * capacity)
    shard_width = FF // N_TP

    def run_expert(pack):
        row_index, w_gate, w_up, w_down = pack
        rows_in = normed[row_index]
        gate_part = jnp.dot(rows_in, w_gate, preferred_element_type=jnp.float32)
        up_part = jnp.dot(rows_in, w_up, preferred_element_type=jnp.float32)
        hidden = (jax.nn.silu(gate_part) * up_part).astype(jnp.bfloat16)
        hidden_parts = hidden.reshape(rows_in.shape[0], N_TP, shard_width).transpose(1, 0, 2)
        down_parts = w_down.reshape(N_TP, shard_width, model_width)

        def add_part(total_sum, pair_in):
            part_rows, part_weight = pair_in
            return (total_sum + rounded(jnp.dot(part_rows, part_weight, preferred_element_type=jnp.float32)), None)
        summed, _ = lax.scan(add_part, jnp.zeros((rows_in.shape[0], model_width), jnp.float32), (hidden_parts, down_parts))
        return summed.astype(jnp.bfloat16)
    served = lax.map(run_expert, (owners, expert_gate_weight, expert_up_weight, expert_down_weight))
    picked = served.reshape(-1, model_width)[target.reshape(sequence_length, TOP)].astype(jnp.float32)
    branch = lax.optimization_barrier(jnp.sum(routing_weight_matrix[:, :, None] * picked, axis=1))
    return (layer_mid.astype(jnp.float32) + rms_scale(branch, expert_after_gain)).astype(jnp.bfloat16)
```

```python
import functools

import jax
import jax.numpy as jnp
import numpy as np
from jax import lax
from jax.experimental import pallas as pl
from jax.experimental.pallas import tpu as pltpu
from jax.sharding import PartitionSpec as P

KEY_CHANNELS = 64
DV = 128
TOP = 2
BLOCK = 64
GROUP_SIZE = 4
CORES = 2

EPSILON = 1e-06
DECAY_NORMALIZER = 16.0
HIGHEST = lax.Precision.HIGHEST
MESH = pl.DeviceIdType.MESH
BF16 = jnp.bfloat16
F32 = jnp.float32


def dot(a, b):
    return jnp.dot(a, b, preferred_element_type=F32)


class Place:
    def __init__(self, n_sp, n_tp, group):
        self.X, self.Z = group, n_sp // group
        self.C, self.Y = CORES, n_tp // CORES
        self.n_tp = n_tp
        self.sp, self.tp = lax.axis_index("sp"), lax.axis_index("tp")
        self.z, self.x = self.sp // self.X, self.sp % self.X
        self.y, self.c = self.tp // self.C, self.tp % self.C

    def at(self, z=None, x=None, y=None, c=None):
        z = self.z if z is None else z
        x = self.x if x is None else x
        y = self.y if y is None else y
        c = self.c if c is None else c
        return (z * self.X + x, y * self.C + c)


def remote(src, dst, send, recv, to):
    return pltpu.make_async_remote_copy(
        src_ref=src, dst_ref=dst, send_sem=send, recv_sem=recv, device_id=to, device_id_type=MESH
    )


def ring_index(way, step, half, steps):
    return way * (2 * steps - 1) + (0 if step == 1 else 1 + (step - 2) * 2 + half)


def ring_sum(at, part, out, sends, recvs, send_sems, recv_sems):
    Y, steps, y = at.Y, at.Y // 2, at.y

    def copy(way, step, half):
        i = ring_index(way, step, half, steps)
        to = (y + 1) % Y if way == 0 else (y + Y - 1) % Y
        return remote(sends.at[i], recvs.at[i], send_sems.at[i], recv_sems.at[i], at.at(y=to))

    def offset(way, step):
        k = steps - step + 1
        return k if way == 0 or k == steps else -k

    started = []

    def send(way, step, half, value):
        sends[ring_index(way, step, half, steps)] = value.astype(BF16)
        c = copy(way, step, half)
        c.start()
        started.append(c)

    for way, half in ((0, 0), (1, 1)):
        send(way, 1, half, part(offset(way, 1), half))
    for step in range(2, steps + 1):
        for way, half in ((0, 1), (1, 0), (0, 0), (1, 1)):
            value = part(offset(way, step), half)
            if step > 2 or way == half:
                copy(way, step - 1, half).wait_recv()
                value = value + recvs[ring_index(way, step - 1, half, steps)].astype(F32)
            send(way, step, half, value)
    for half in (0, 1):
        total = part(0, half)
        for way in (0, 1):
            copy(way, steps, half).wait_recv()
            total = total + recvs[ring_index(way, steps, half, steps)].astype(F32)
        out(half, total)
    return started


def layer_kernel(
    n_sp, n_tp, group, cap,
    gated, w_out, residual, attention_gain, before_gain, after_gain,
    w_gate, w_up, w_down, ids_col, ids_row, weights, perm_out, perm_back,
    out,
    gu, wd, wo, partner, mixed, mid, normed, block, rows, acc, hid, shares, result,
    zs, zr, xs, xb, zs2, zr2, column, branch,
    sa, ra, sb, rb,
    wsem, wrs, wrr, gsem, as_, ar, zss, zrs, xss, xrs, gs, gr, bs, br, xbs, xbr, zbs, zbr, fs,
):
    at = Place(n_sp, n_tp, group)
    X, Y, Z, C = at.X, at.Y, at.Z, at.C
    x, y, z, c = at.x, at.y, at.z, at.c
    steps = Y // 2
    other = 1 - c

    local = [
        pltpu.make_async_copy(w_gate, gu.at[0], wsem.at[0]),
        pltpu.make_async_copy(w_up, gu.at[1], wsem.at[1]),
        pltpu.make_async_copy(w_down, wd.at[0], wsem.at[2]),
        pltpu.make_async_copy(w_out, wo.at[0], wsem.at[3]),
    ]
    local[3].start()
    for k in (0, 1, 2):
        local[k].start()

    barrier = pltpu.get_barrier_semaphore()

    def greet_tp(k, carry):
        pl.semaphore_signal(barrier, inc=1, device_id=(at.sp, (at.tp + k) % n_tp), device_id_type=MESH)
        return carry

    lax.fori_loop(1, n_tp, greet_tp, 0)
    for k in range(1, Z):
        pl.semaphore_signal(barrier, inc=1, device_id=at.at(z=(z + k) % Z), device_id_type=MESH)
    for k in range(1, X):
        for core in range(C):
            pl.semaphore_signal(barrier, inc=1, device_id=at.at(x=(x + k) % X, c=core), device_id_type=MESH)
    pl.semaphore_wait(barrier, n_tp - 1 + Z - 1 + (X - 1) * C)

    pair = at.at(c=other)
    swap = remote(gated.at[:, other], partner, gsem.at[0], gsem.at[1], pair)
    swap.start()
    crossed = [
        remote(w_out, wo.at[1], wrs.at[3], wrr.at[3], pair),
        remote(w_gate, gu.at[2], wrs.at[0], wrr.at[0], pair),
        remote(w_up, gu.at[3], wrs.at[1], wrr.at[1], pair),
        remote(w_down, wd.at[1], wrs.at[2], wrr.at[2], pair),
    ]
    for k in crossed:
        k.start()

    share = gated.shape[0]
    piece = gated.shape[2]
    width = wo.shape[2]
    swap.wait_recv()
    local[3].wait()
    crossed[0].wait_recv()
    mine = gated[:, pl.ds(c, 1)].reshape(share * piece, DV)
    theirs = partner[...].reshape(share * piece, DV)
    tile = width // 4
    for k in range(4):
        cols = slice(k * tile, (k + 1) * tile)
        value = dot(mine, wo[0, :, cols]) + dot(theirs, wo[1, :, cols])
        mixed[:, :, cols] = value.reshape(share, piece, tile)

    half_width = width // 2

    def mixed_part(k, half):
        d = (y + k + Y) % Y
        return mixed[pl.ds(d, 1), :, half * half_width : (half + 1) * half_width].reshape(piece, half_width)

    total = [None, None]

    def keep(half, value):
        total[half] = value

    sum_a = ring_sum(at, mixed_part, keep, sa, ra, as_.at[0], as_.at[1])
    attn = jnp.concatenate(total, axis=1)
    attn = attn * lax.rsqrt(jnp.mean(attn * attn, axis=1, keepdims=True) + EPSILON) * attention_gain[...]
    mid[...] = (residual[...].astype(F32) + attn).astype(BF16)
    m = mid[...].astype(F32)
    m = m * lax.rsqrt(jnp.mean(m * m, axis=1, keepdims=True) + EPSILON) * before_gain[...]
    normed[...] = m.astype(BF16)

    def share_cols(t):
        return pl.ds(pl.multiple_of(t * DV, DV), DV)

    def share_rows(t):
        return pl.ds(pl.multiple_of(t * piece, piece), piece)

    def to_width(k):
        t = (at.tp + k) % n_tp
        return remote(
            normed.at[:, share_cols(t)], block.at[share_rows(at.tp), :], ar.at[0, k], ar.at[1, k], (at.sp, t)
        )

    def start_width(k, carry):
        to_width(k).start()
        return carry

    def wait_width(k, carry):
        to_width(k).wait_recv()
        return carry

    lax.fori_loop(1, n_tp, start_width, 0)
    block[share_rows(at.tp), :] = normed[:, share_cols(at.tp)]

    tokens = block.shape[0]
    slots = n_sp * cap
    lane = lax.broadcasted_iota(jnp.int32, (tokens, n_sp), 1)
    e0, e1 = ids_col[:, 0:1], ids_col[:, 1:2]
    r, q = (lax.broadcasted_iota(jnp.int32, (tokens, tokens), k) for k in (0, 1))
    named = jnp.where((lane == e0) | (lane == e1), 1.0, 0.0).astype(BF16)
    before = dot(jnp.where(r > q, 1.0, 0.0).astype(BF16), named)
    wide = lax.broadcasted_iota(jnp.int32, (tokens, slots), 1)
    picks = []
    for e in (e0, e1):
        slot = jnp.sum(jnp.where(lane == e, before, 0.0), axis=1, keepdims=True)
        picks.append(e * cap + slot.astype(jnp.int32))
    sub = lax.broadcasted_iota(jnp.int32, (n_sp, tokens), 0)
    f0, f1 = ids_row[0:1, :], ids_row[1:2, :]
    named_t = jnp.where((sub == f0) | (sub == f1), 1.0, 0.0).astype(BF16)
    before_t = dot(named_t, jnp.where(r < q, 1.0, 0.0).astype(BF16))
    tall = lax.broadcasted_iota(jnp.int32, (slots, tokens), 0)
    spread = None
    for f in (f0, f1):
        slot = jnp.sum(jnp.where(sub == f, before_t, 0.0), axis=0, keepdims=True)
        hit = jnp.where(tall == f * cap + slot.astype(jnp.int32), 1.0, 0.0)
        spread = hit if spread is None else spread + hit
    spread = spread.astype(BF16)

    lax.fori_loop(1, n_tp, wait_width, 0)
    picked = dot(spread, block[...]).astype(BF16)
    zs[...] = picked.reshape(zs.shape)

    def z_out(k):
        return remote(zs.at[(z + k) % Z], zr.at[z], zss.at[k], zrs.at[k], at.at(z=(z + k) % Z))

    for k in range(1, Z):
        z_out(k).start()
    zr[pl.ds(z, 1)] = zs[pl.ds(z, 1)]
    for k in range(1, Z):
        z_out(k).wait_recv()

    order = lax.broadcasted_iota(jnp.int32, (slots, slots), 1)
    turn = jnp.where(order == perm_out[...], 1.0, 0.0).astype(BF16)
    xs[...] = dot(turn, zr[...].reshape(slots, DV)).astype(BF16).reshape(xs.shape)

    side = x % C
    mine_half = x // C

    def x_out(k):
        to = (x + k) % X
        return (
            xs.at[to],
            rows.at[y, mine_half, :, share_cols(c)],
            xss.at[k],
            xrs.at[mine_half, c],
            at.at(x=to, c=side),
        )

    for k in range(1, X):
        remote(*x_out(k)).start()
    src, dst, s_sem, r_sem, to = x_out(0)

    @pl.when(side == c)
    def _():
        pltpu.make_async_copy(src, dst, r_sem).start()

    @pl.when(side != c)
    def _():
        remote(src, dst, s_sem, r_sem, pair).start()

    def gather(way, step, half):
        j = (y + Y - (step - 1)) % Y if way == 0 else (y + step - 1) % Y
        to = (y + 1) % Y if way == 0 else (y + Y - 1) % Y
        i = way * (2 * steps - 1) + (step - 1) * 2 + (half if step < steps else 0)
        return remote(rows.at[j, half], rows.at[j, half], gs.at[i], gr.at[i], at.at(y=to))

    gathers = []

    def start_gather(way, step, half):
        g = gather(way, step, half)
        g.start()
        gathers.append(g)

    for half in (0, 1):
        for core in range(C):
            pltpu.make_async_copy(xs.at[0], rows.at[y, half, :, pl.ds(core * DV, DV)], xrs.at[half, core]).wait()
        for way in (0, 1):
            start_gather(way, 1, half)

    count = rows.shape[1] * rows.shape[2]
    chunk = rows.shape[3]
    local[0].wait()
    local[1].wait()
    crossed[1].wait_recv()
    crossed[2].wait_recv()

    def grow(j, first=False):
        a = rows[pl.ds(j, 1)].reshape(count, chunk)
        at_rows = pl.ds(pl.multiple_of(j * chunk, chunk), chunk)
        for k in range(4):
            value = dot(a, gu[k, at_rows, :])
            acc[k] = value if first else acc[k] + value

    grow(y, True)
    for step in range(1, steps):
        for half in (0, 1):
            for way in (0, 1):
                gather(way, step, half).wait_recv()
                if step + 1 < steps or way == half:
                    start_gather(way, step + 1, half)
        grow((y + Y - step) % Y)
        grow((y + step) % Y)
    for way in (0, 1):
        gather(way, steps, way).wait_recv()
    grow((y + steps) % Y)

    for k in (0, 1):
        gate, up = acc[2 * k], acc[2 * k + 1]
        hid[k] = (gate * jax.nn.sigmoid(gate) * up).astype(BF16)

    local[2].wait()
    crossed[3].wait_recv()
    made = {}

    def down(offset):
        d = (y + offset + Y) % Y
        cols = pl.ds(pl.multiple_of(d * chunk, chunk), chunk)
        value = dot(hid[0], wd[0, :, cols]) + dot(hid[1], wd[1, :, cols])
        shares[offset + steps - 1] = value.reshape(2, count // 2, chunk)

    def down_part(offset, half):
        if offset not in made:
            down(offset)
            made[offset] = True
        return shares[offset + steps - 1, half]

    def keep_result(half, value):
        result[half] = value.astype(BF16)

    sum_b = ring_sum(at, down_part, keep_result, sb, rb, bs, br)

    def x_back(half, core):
        home = 2 * half + c
        return (
            result.at[half, :, pl.ds(core * DV, DV)],
            xb.at[x],
            xbs.at[2 * half + core],
            xbr.at[x],
            at.at(x=home, c=core),
        ), (home == x) & (c == core)

    for half in (0, 1):
        for core in range(C):
            args, here = x_back(half, core)

            @pl.when(here)
            def _(args=args):
                pltpu.make_async_copy(args[0], args[1], args[3]).start()

            @pl.when(jnp.logical_not(here))
            def _(args=args):
                remote(*args).start()

    for k in range(X):
        pltpu.make_async_copy(xs.at[0], xb.at[k], xbr.at[k]).wait()
    turn = jnp.where(order == perm_back[...], 1.0, 0.0).astype(BF16)
    zs2[...] = dot(turn, xb[...].reshape(slots, DV)).astype(BF16).reshape(zs2.shape)

    def z_back(k):
        return remote(zs2.at[(z + k) % Z], zr2.at[z], zbs.at[k], zbr.at[k], at.at(z=(z + k) % Z))

    for k in range(1, Z):
        z_back(k).start()
    zr2[pl.ds(z, 1)] = zs2[pl.ds(z, 1)]
    finds = [jnp.where(wide == p, 1.0, 0.0).astype(BF16) for p in picks]
    for k in range(1, Z):
        z_back(k).wait_recv()
    lookup = zr2[...].reshape(slots, DV)
    column[...] = (
        weights[:, 0:1] * dot(finds[0], lookup) + weights[:, 1:2] * dot(finds[1], lookup)
    ).astype(BF16)

    def to_rows(k):
        t = (at.tp + k) % n_tp
        return remote(
            column.at[share_rows(t), :], branch.at[:, share_cols(at.tp)], fs.at[0, k], fs.at[1, k], (at.sp, t)
        )

    def start_rows(k, carry):
        to_rows(k).start()
        return carry

    def wait_rows(k, carry):
        to_rows(k).wait_recv()
        return carry

    lax.fori_loop(1, n_tp, start_rows, 0)
    branch[:, share_cols(at.tp)] = column[share_rows(at.tp), :]
    lax.fori_loop(1, n_tp, wait_rows, 0)
    b = branch[...].astype(F32)
    b = b * lax.rsqrt(jnp.mean(b * b, axis=1, keepdims=True) + EPSILON) * after_gain[...]
    out[...] = (mid[...].astype(F32) + b).astype(BF16)

    swap.wait_send()
    for k in crossed + sum_a + gathers + sum_b:
        k.wait_send()

    def wait_sent(k, carry):
        to_width(k).wait_send()
        to_rows(k).wait_send()
        return carry

    lax.fori_loop(1, n_tp, wait_sent, 0)
    for k in range(1, Z):
        z_out(k).wait_send()
        z_back(k).wait_send()
    for k in range(1, X):
        remote(*x_out(k)).wait_send()

    @pl.when(side != c)
    def _():
        remote(src, dst, s_sem, r_sem, pair).wait_send()

    for half in (0, 1):
        for core in range(C):
            args, here = x_back(half, core)

            @pl.when(jnp.logical_not(here))
            def _(args=args):
                remote(*args).wait_send()


def layer_tail(
    gated, output_projection, residual, attention_gain, before_gain, after_gain,
    w_gate, w_up, w_down, ids, weights,
):
    n_sp, n_tp = lax.axis_size("sp"), lax.axis_size("tp")
    tokens, width = gated.shape[0], residual.shape[1]
    piece = residual.shape[0]
    X, C = GROUP_SIZE, CORES
    Z, Y = n_sp // X, n_tp // C
    cap = 5 * tokens // (2 * n_sp)
    slots = n_sp * cap
    steps = Y // 2
    msgs = 2 * (2 * steps - 1)
    half = slots // 4
    chunk = C * DV
    hidden = w_gate.shape[2]
    order = np.arange(slots).reshape(Z, X, cap)
    perm_out = np.transpose(order, (1, 0, 2)).reshape(slots, 1).astype(np.int32)
    order = np.arange(slots).reshape(X, Z, cap)
    perm_back = np.transpose(order, (1, 0, 2)).reshape(slots, 1).astype(np.int32)
    vm, hbm = pl.BlockSpec(memory_space=pltpu.VMEM), pl.BlockSpec(memory_space=pl.ANY)
    sem = pltpu.SemaphoreType.DMA
    scratch = [
        pltpu.VMEM((4, width, hidden), BF16),
        pltpu.VMEM((2, hidden, width), BF16),
        pltpu.VMEM((2, DV, width), BF16),
        pltpu.VMEM((Y, piece, DV), BF16),
        pltpu.VMEM((Y, piece, width), F32),
        pltpu.VMEM((piece, width), BF16),
        pltpu.VMEM((piece, width), BF16),
        pltpu.VMEM((tokens, DV), BF16),
        pltpu.VMEM((Y, 2, half, chunk), BF16),
        pltpu.VMEM((4, 2 * half, hidden), F32),
        pltpu.VMEM((2, 2 * half, hidden), BF16),
        pltpu.VMEM((Y, 2, half, chunk), F32),
        pltpu.VMEM((2, half, chunk), BF16),
        pltpu.VMEM((Z, X * cap, DV), BF16),
        pltpu.VMEM((Z, X * cap, DV), BF16),
        pltpu.VMEM((X, Z * cap, DV), BF16),
        pltpu.VMEM((X, Z * cap, DV), BF16),
        pltpu.VMEM((Z, X * cap, DV), BF16),
        pltpu.VMEM((Z, X * cap, DV), BF16),
        pltpu.VMEM((tokens, DV), BF16),
        pltpu.VMEM((piece, width), BF16),
        pltpu.VMEM((msgs, piece, width // 2), BF16),
        pltpu.VMEM((msgs, piece, width // 2), BF16),
        pltpu.VMEM((msgs, half, chunk), BF16),
        pltpu.VMEM((msgs, half, chunk), BF16),
        sem((4,)), sem((4,)), sem((4,)), sem((2,)),
        sem((2, msgs)),
        sem((2, n_tp)),
        sem((Z,)), sem((Z,)),
        sem((X,)), sem((2, C)),
        sem((msgs,)), sem((msgs,)),
        sem((msgs,)), sem((msgs,)),
        sem((2 * C,)), sem((X,)),
        sem((Z,)), sem((Z,)),
        sem((2, n_tp)),
    ]
    return pl.pallas_call(
        functools.partial(layer_kernel, n_sp, n_tp, X, cap),
        out_shape=jax.ShapeDtypeStruct((piece, width), BF16),
        in_specs=[vm, hbm, vm, vm, vm, vm, hbm, hbm, hbm, vm, vm, vm, vm, vm],
        out_specs=vm,
        scratch_shapes=scratch,
        name="layer_tail",
        compiler_params=pltpu.CompilerParams(
            collective_id=0, has_side_effects=True, vmem_limit_bytes=60 * 1024 * 1024
        ),
    )(
        gated.reshape(Y, C, piece, DV), output_projection, residual,
        attention_gain[None], before_gain[None], after_gain[None],
        w_gate[0], w_up[0], w_down[0], ids, ids.T, weights,
        jnp.asarray(perm_out), jnp.asarray(perm_back),
    )


def copy_for_each(shard, axis):
    peers = lax.axis_size(axis)
    return lax.all_to_all(
        jnp.broadcast_to(shard[None], (peers, *shard.shape)), axis, 0, 0, tiled=True
    )


def gathered_once(shard, axis):
    leaves = jax.tree.leaves(shard)
    turns = sorted(range(len(leaves)), key=lambda k: -leaves[k].size)
    width = (1, *leaves[turns[0]].shape)[-1]
    lines = [
        jnp.pad(leaves[k].reshape(-1), (0, -leaves[k].size % width)).reshape(-1, width)
        for k in turns
    ]
    both, at, found = (copy_for_each(jnp.concatenate(lines), axis), 0, {})
    for k, line in zip(turns, lines):
        section = both[:, at : at + len(line)].reshape(len(both), -1)
        found[k] = section[:, : leaves[k].size].reshape(-1, *leaves[k].shape)
        at += len(line)
    numbers = iter(range(len(leaves)))
    return jax.tree.map(lambda _: found[next(numbers)], shard)


def combined_pairwise(pieces, combine):
    while len(jax.tree.leaves(pieces)[0]) > 1:
        pieces = jax.vmap(combine)(
            *(jax.tree.map(lambda part: part[side::2], pieces) for side in (0, 1))
        )
    return jax.tree.map(lambda part: part[0], pieces)


def carried_in(shard, axis, combine, identity):
    peers, position = (lax.axis_size(axis), lax.axis_index(axis))
    passed = jnp.arange(peers) < position

    def kept(part, zero, own):
        part = jnp.where(
            passed.reshape(-1, *(1 for _ in own.shape)),
            part.astype(own.dtype),
            jnp.asarray(zero, own.dtype),
        )
        return part

    pieces = gathered_once(
        jax.tree.map(lambda part, kind: part.astype(kind), shard, (jnp.bfloat16, jnp.bfloat16)),
        axis,
    )
    return combined_pairwise(jax.tree.map(kept, pieces, identity, shard), combine)


def rms_scale(values, gain_row):
    return (
        values * lax.rsqrt(jnp.mean(values * values, axis=-1, keepdims=True) + EPSILON) * gain_row
    )


def join_states(earlier, later):
    fade_one, state_one = earlier
    fade_two, state_two = later
    return (fade_one * fade_two, fade_two[..., None] * state_one + state_two)


def advance(running_state, inputs_pair):
    fade_now, grow_now = inputs_pair
    return (fade_now[..., None] * running_state + grow_now, running_state)


def shards(
    query_matrix,
    key_matrix,
    value_matrix,
    output_gate_rows,
    decay_preactivation,
    channel_decay_bias,
    extra_log_decay,
    head_norm_gain,
    output_projection,
    residual_input,
    attention_norm_gain,
    expert_before_gain,
    expert_after_gain,
    expert_gate_weight,
    expert_up_weight,
    expert_down_weight,
    token_expert_index,
    routing_weight_matrix,
):
    sequence_length = query_matrix.shape[0]
    number_heads = value_matrix.shape[1] // DV
    blocks = sequence_length // BLOCK
    queries = query_matrix.astype(jnp.float32).reshape(
        sequence_length, number_heads, KEY_CHANNELS
    ) * KEY_CHANNELS ** (-0.5)
    keys_all = key_matrix.astype(jnp.float32).reshape(sequence_length, number_heads, KEY_CHANNELS)
    values_all = value_matrix.astype(jnp.float32).reshape(sequence_length, number_heads, DV)
    decay_logarithm = (
        jax.nn.log_sigmoid(decay_preactivation.astype(jnp.float32) + channel_decay_bias)
        / DECAY_NORMALIZER
    )
    decay_logarithm = (
        decay_logarithm.reshape(sequence_length, number_heads, KEY_CHANNELS)
        + extra_log_decay[:, :, None]
    )
    running = jnp.cumsum(decay_logarithm, axis=0)
    total_fade = jnp.exp(running[-1])
    keys_to_end = keys_all * jnp.exp(running[-1] - running)
    total_growth = jnp.einsum("thd,thv->hdv", keys_to_end, values_all, precision=HIGHEST)
    q_blocks = queries.reshape(blocks, BLOCK, number_heads, KEY_CHANNELS)
    k_blocks = keys_all.reshape(blocks, BLOCK, number_heads, KEY_CHANNELS)
    v_blocks = values_all.reshape(blocks, BLOCK, number_heads, DV)
    inside = jnp.cumsum(decay_logarithm.reshape(blocks, BLOCK, number_heads, KEY_CHANNELS), axis=1)
    block_end = inside[:, -1:]
    q_decayed = q_blocks * jnp.exp(inside)
    k_inverse = k_blocks * jnp.exp(-inside)
    k_to_end = k_blocks * jnp.exp(block_end - inside)
    causal = jnp.tril(jnp.ones((BLOCK, BLOCK), dtype=bool))
    scores = jnp.einsum("nihd,njhd->nhij", q_decayed, k_inverse, precision=HIGHEST)
    scores = jnp.where(causal, scores, 0.0)
    within = jnp.einsum("nhij,njhv->nihv", scores, v_blocks, precision=HIGHEST)
    growth = jnp.einsum("nchd,nchv->nhdv", k_to_end, v_blocks, precision=HIGHEST)
    fade_rows = jnp.exp(block_end[:, 0])
    identity = (jnp.ones_like(total_fade), jnp.zeros_like(total_growth))
    _, carried = carried_in((total_fade, total_growth), "sp", join_states, identity)
    _, starts = lax.scan(advance, carried, (fade_rows, growth))
    across = jnp.einsum("nchd,nhdv->nchv", q_decayed, starts, precision=HIGHEST)
    attn = (within + across).reshape(sequence_length, number_heads, DV)
    gate_act = jax.nn.silu(
        output_gate_rows.astype(jnp.float32).reshape(sequence_length, number_heads, DV)
    )
    gated = (
        (rms_scale(attn, head_norm_gain) * gate_act)
        .astype(jnp.bfloat16)
        .reshape(sequence_length, number_heads * DV)
    )
    return layer_tail(
        gated, output_projection, residual_input, attention_norm_gain, expert_before_gain, expert_after_gain,
        expert_gate_weight, expert_up_weight, expert_down_weight, token_expert_index, routing_weight_matrix,
    )


def solution(mesh):
    placed = (
        P("sp", "tp"),
        P("sp", "tp"),
        P("sp", "tp"),
        P("sp", "tp"),
        P("sp", "tp"),
        P("tp"),
        P("sp", "tp"),
        P(),
        P("tp", None),
        P(("sp", "tp"), None),
        P(),
        P(),
        P(),
        P("sp", None, "tp"),
        P("sp", None, "tp"),
        P("sp", "tp", None),
        P("sp", None),
        P("sp", None),
    )
    return jax.shard_map(
        shards, mesh=mesh, in_specs=placed, out_specs=P(("sp", "tp"), None), check_vma=False
    )
```

```python
import contextlib
import functools

import jax
import jax.numpy as jnp
from jax import lax
from jax.experimental import pallas as pl
from jax.experimental.pallas import tpu as pltpu
from jax.sharding import PartitionSpec as P

KEY_CHANNELS = 64
DV = 128
TOP = 2
BLOCK = 64
GROUP_SIZE = 4
CORES = 2

EPSILON = 1e-06
DECAY_NORMALIZER = 16.0
MESH = pl.DeviceIdType.MESH
BF16 = jnp.bfloat16
F32 = jnp.float32
PROFILE = False


def scope(name):
    return jax.named_scope(name) if PROFILE else contextlib.nullcontext()


def dot(a, b):
    return jnp.dot(a, b, preferred_element_type=F32)


class Place:
    def __init__(self, n_sp, n_tp, group):
        self.X, self.Z = group, n_sp // group
        self.C, self.Y = CORES, n_tp // CORES
        self.n_tp = n_tp
        self.sp, self.tp = lax.axis_index("sp"), lax.axis_index("tp")
        self.z, self.x = self.sp // self.X, self.sp % self.X
        self.y, self.c = self.tp // self.C, self.tp % self.C

    def at(self, z=None, x=None, y=None, c=None):
        z = self.z if z is None else z
        x = self.x if x is None else x
        y = self.y if y is None else y
        c = self.c if c is None else c
        return (z * self.X + x, y * self.C + c)


def remote(src, dst, send, recv, to):
    return pltpu.make_async_remote_copy(
        src_ref=src, dst_ref=dst, send_sem=send, recv_sem=recv, device_id=to, device_id_type=MESH
    )


def ring_index(way, step, half, steps):
    return way * (2 * steps - 1) + (0 if step == 1 else 1 + (step - 2) * 2 + half)


def ring_sum(at, part, out, sends, recvs, send_sems, recv_sems):
    Y, steps, y = at.Y, at.Y // 2, at.y

    def copy(way, step, half):
        i = ring_index(way, step, half, steps)
        to = (y + 1) % Y if way == 0 else (y + Y - 1) % Y
        return remote(sends.at[i], recvs.at[i], send_sems.at[i], recv_sems.at[i], at.at(y=to))

    def offset(way, step):
        k = steps - step + 1
        return k if way == 0 or k == steps else -k

    started = []

    def send(way, step, half, value):
        sends[ring_index(way, step, half, steps)] = value.astype(BF16)
        c = copy(way, step, half)
        c.start()
        started.append(c)

    for way, half in ((0, 0), (1, 1)):
        send(way, 1, half, part(offset(way, 1), half))
    for step in range(2, steps + 1):
        for way, half in ((0, 1), (1, 0), (0, 0), (1, 1)):
            value = part(offset(way, step), half)
            if step > 2 or way == half:
                copy(way, step - 1, half).wait_recv()
                value = value + recvs[ring_index(way, step - 1, half, steps)].astype(F32)
            send(way, step, half, value)
    for half in (0, 1):
        total = part(0, half)
        for way in (0, 1):
            copy(way, steps, half).wait_recv()
            total = total + recvs[ring_index(way, steps, half, steps)].astype(F32)
        out(half, total)
    return started


def split(value):
    high = value.astype(BF16)
    rest = value - high.astype(F32)
    middle = rest.astype(BF16)
    return high, middle, (rest - middle.astype(F32)).astype(BF16)


def standing(row, count):
    square = (count, row.shape[1])
    same = lax.broadcasted_iota(jnp.int32, square, 0) == lax.broadcasted_iota(jnp.int32, square, 1)
    return jnp.sum(jnp.where(same, row, 0.0), axis=1, keepdims=True)


def lying(col, width):
    square = (col.shape[0], width)
    same = lax.broadcasted_iota(jnp.int32, square, 0) == lax.broadcasted_iota(jnp.int32, square, 1)
    return jnp.sum(jnp.where(same, col, 0.0), axis=0, keepdims=True)


def layer_kernel(
    n_sp, n_tp, group, cap,
    q_t, k_t, values, gate_rows, decay_t, bias, extra, head_gain,
    w_out, residual, attention_gain, before_gain, after_gain,
    w_gate, w_up, w_down, ids_row, weights_row,
    out,
    gated, stack, spread, find, turn_out, turn_back, sx, rx, sz, rz,
    gu, wd, wo, partner, mixed, mid, normed, block, rows, acc, hid, shares, result,
    zs, zr, xs, xb, zs2, zr2, column, branch,
    sa, ra, sb, rb,
    wsem, wrs, wrr, gsem, as_, ar, zss, zrs, xss, xrs, gs, gr, bs, br, xbs, xbr, zbs, zbr, fs,
    sxs, sxr, szs, szr,
):
    at = Place(n_sp, n_tp, group)
    X, Y, Z, C = at.X, at.Y, at.Z, at.C
    x, y, z, c = at.x, at.y, at.z, at.c
    steps = Y // 2
    other = 1 - c

    local = [
        pltpu.make_async_copy(w_gate, gu.at[0], wsem.at[0]),
        pltpu.make_async_copy(w_up, gu.at[1], wsem.at[1]),
        pltpu.make_async_copy(w_down, wd.at[0], wsem.at[2]),
        pltpu.make_async_copy(w_out, wo.at[0], wsem.at[3]),
    ]
    local[3].start()
    for k in (0, 1, 2):
        local[k].start()

    rz[...] = jnp.zeros_like(rz)
    barrier = pltpu.get_barrier_semaphore()

    def greet_tp(k, carry):
        pl.semaphore_signal(barrier, inc=1, device_id=(at.sp, (at.tp + k) % n_tp), device_id_type=MESH)
        return carry

    lax.fori_loop(1, n_tp, greet_tp, 0)
    for k in range(1, Z):
        pl.semaphore_signal(barrier, inc=1, device_id=at.at(z=(z + k) % Z), device_id_type=MESH)
    for k in range(1, X):
        for core in range(C):
            pl.semaphore_signal(barrier, inc=1, device_id=at.at(x=(x + k) % X, c=core), device_id_type=MESH)

    tokens = q_t.shape[1]
    blocks = tokens // BLOCK
    pre = decay_t[...].astype(F32) + standing(bias[...], KEY_CHANNELS)
    log_decay = -(jnp.maximum(-pre, 0.0) + jnp.log1p(jnp.exp(-jnp.abs(pre)))) / DECAY_NORMALIZER + extra[...]
    r, q = (lax.broadcasted_iota(jnp.int32, (tokens, tokens), k) for k in (0, 1))
    one_block = (r // BLOCK) == (q // BLOCK)
    upto = jnp.where((r <= q) & one_block, 1.0, 0.0).astype(BF16)
    inside = sum(dot(term, upto) for term in split(log_decay))
    ends = [inside[:, (b + 1) * BLOCK - 1 : (b + 1) * BLOCK] for b in range(blocks)]
    of_block = lax.broadcasted_iota(jnp.int32, (KEY_CHANNELS, tokens), 1) // BLOCK
    keys = k_t[...].astype(F32)
    to_end = [jnp.where(of_block == b, keys * jnp.exp(jnp.minimum(ends[b] - inside, 0.0)), 0.0) for b in range(blocks)]
    vals = values[...]
    growth = dot(jnp.concatenate(to_end, axis=0).astype(BF16), vals)
    growth = [growth[b * KEY_CHANNELS : (b + 1) * KEY_CHANNELS] for b in range(blocks)]
    fades = [jnp.exp(e) for e in ends]
    state = growth[0]
    for b in range(1, blocks):
        state = fades[b] * state + growth[b]
    fade_row = lying(jnp.exp(sum(ends)), DV)
    tail = KEY_CHANNELS + 16

    def message(ref, state_part, row):
        ref[0:KEY_CHANNELS, :] = state_part.astype(BF16)
        ref[KEY_CHANNELS:tail, :] = jnp.broadcast_to(row, (16, DV)).astype(BF16)

    message(sx, state, fade_row)
    pl.semaphore_wait(barrier, n_tp - 1 + Z - 1 + (X - 1) * C)

    def state_x(k):
        return remote(sx, rx.at[x], sxs.at[k], sxr.at[k], at.at(x=(x + k) % X))

    for k in range(1, X):
        state_x(k).start()
    pair = at.at(c=other)
    crossed = [
        remote(w_out, wo.at[1], wrs.at[3], wrr.at[3], pair),
        remote(w_gate, gu.at[2], wrs.at[0], wrr.at[0], pair),
        remote(w_up, gu.at[3], wrs.at[1], wrr.at[1], pair),
        remote(w_down, wd.at[1], wrs.at[2], wrr.at[2], pair),
    ]
    for k in crossed:
        k.start()
    rx[pl.ds(x, 1)] = sx[...].reshape(1, tail, DV)

    slots = n_sp * cap
    sub = lax.broadcasted_iota(jnp.int32, (n_sp, tokens), 0)
    chosen = [ids_row[k : k + 1, :] for k in range(TOP)]
    named = jnp.where((sub == chosen[0]) | (sub == chosen[1]), 1.0, 0.0).astype(BF16)
    before = dot(named, jnp.where(r < q, 1.0, 0.0).astype(BF16))
    targets = []
    for e in chosen:
        slot = jnp.sum(jnp.where(sub == e, before, 0.0), axis=0, keepdims=True)
        targets.append(e * cap + slot.astype(jnp.int32))
    query = q_t[...].astype(F32) * (KEY_CHANNELS**-0.5 * jnp.exp(inside))
    stack[0:KEY_CHANNELS, :] = query
    stack[KEY_CHANNELS:, :] = jnp.zeros((stack.shape[0] - KEY_CHANNELS, tokens), F32)
    for k in range(TOP):
        stack[KEY_CHANNELS + k : KEY_CHANNELS + k + 1, :] = targets[k].astype(F32)
        stack[KEY_CHANNELS + TOP + k : KEY_CHANNELS + TOP + k + 1, :] = weights_row[k : k + 1, :]
    stood = stack[...].T
    query = stood[:, 0:KEY_CHANNELS].astype(BF16)
    target_cols = [stood[:, KEY_CHANNELS + k : KEY_CHANNELS + k + 1].astype(jnp.int32) for k in range(TOP)]
    weight_cols = [stood[:, KEY_CHANNELS + TOP + k : KEY_CHANNELS + TOP + k + 1] for k in range(TOP)]
    scores = dot(query, (keys * jnp.exp(-inside)).astype(BF16))
    scores = jnp.where((r >= q) & one_block, scores, 0.0).astype(BF16)
    within = dot(scores, vals)

    for k in range(1, X):
        state_x(k).wait_recv()
    plane, plane_row = rx[0, 0:KEY_CHANNELS].astype(F32), rx[0, KEY_CHANNELS:tail][0:1].astype(F32)
    ahead, ahead_fade = jnp.zeros_like(state), jnp.ones((KEY_CHANNELS, 1), F32)
    for k in range(X):
        part, row = rx[k, 0:KEY_CHANNELS].astype(F32), rx[k, KEY_CHANNELS:tail][0:1].astype(F32)
        fade = standing(row, KEY_CHANNELS)
        ahead = jnp.where(k < x, fade * ahead + part, ahead)
        ahead_fade = jnp.where(k < x, fade * ahead_fade, ahead_fade)
        if k:
            plane, plane_row = fade * plane + part, plane_row * row
    message(sz, plane, plane_row)

    def state_z(k):
        return remote(sz, rz.at[z], szs.at[k], szr.at[k], at.at(z=(z + k) % Z))

    for k in range(1, Z):

        @pl.when(z + k < Z)
        def _(k=k):
            state_z(k).start()

    tall = lax.broadcasted_iota(jnp.int32, (slots, tokens), 0)
    hits = [jnp.where(tall == t, 1.0, 0.0) for t in targets]
    spread[...] = (hits[0] + hits[1]).astype(BF16)
    wide = lax.broadcasted_iota(jnp.int32, (tokens, slots), 1)
    for k in range(TOP):
        find[k] = jnp.where(wide == target_cols[k], 1.0, 0.0).astype(BF16)
    lane = lax.broadcasted_iota(jnp.int32, (1, slots), 1)

    def turned(outer, inner):
        a = sum(jnp.where(lane >= k * inner * cap, 1, 0) for k in range(1, outer))
        rest = lane - a * (inner * cap)
        b = sum(jnp.where(rest >= k * cap, 1, 0) for k in range(1, inner))
        return b * (outer * cap) + a * cap + (rest - b * cap)

    down_rows = lax.broadcasted_iota(jnp.int32, (slots, slots), 0)
    turn_out[...] = jnp.where(down_rows == turned(Z, X), 1.0, 0.0).astype(BF16)
    turn_back[...] = jnp.where(down_rows == turned(X, Z), 1.0, 0.0).astype(BF16)
    gate_act = gate_rows[...].astype(F32)
    gate_act = gate_act * jax.nn.sigmoid(gate_act) * head_gain[...]

    for k in range(1, Z):

        @pl.when(z >= k)
        def _(k=k):
            state_z(k).wait_recv()

    carried = jnp.zeros_like(state)
    for k in range(Z - 1):
        fade = standing(rz[k, KEY_CHANNELS:tail][0:1].astype(F32), KEY_CHANNELS)
        carried = jnp.where(k < z, fade * carried + rz[k, 0:KEY_CHANNELS].astype(F32), carried)
    running = ahead_fade * carried + ahead
    across = []
    for b in range(blocks):
        across.append(dot(query[b * BLOCK : (b + 1) * BLOCK], running.astype(BF16)))
        running = fades[b] * running + growth[b]
    heads = within + jnp.concatenate(across, axis=0)
    heads = heads * lax.rsqrt(jnp.mean(heads * heads, axis=1, keepdims=True) + EPSILON) * gate_act
    gated[...] = heads.astype(BF16).reshape(gated.shape)
    swap = remote(gated.at[:, other], partner, gsem.at[0], gsem.at[1], pair)
    swap.start()

    share = gated.shape[0]
    piece = gated.shape[2]
    width = wo.shape[2]
    swap.wait_recv()
    local[3].wait()
    crossed[0].wait_recv()
    mine = gated[:, pl.ds(c, 1)].reshape(share * piece, DV)
    theirs = partner[...].reshape(share * piece, DV)
    tile = width // 4
    for k in range(4):
        cols = slice(k * tile, (k + 1) * tile)
        value = dot(mine, wo[0, :, cols]) + dot(theirs, wo[1, :, cols])
        mixed[:, :, cols] = value.reshape(share, piece, tile)

    half_width = width // 2

    def mixed_part(k, half):
        d = (y + k + Y) % Y
        return mixed[pl.ds(d, 1), :, half * half_width : (half + 1) * half_width].reshape(piece, half_width)

    total = [None, None]

    def keep(half, value):
        total[half] = value

    sum_a = ring_sum(at, mixed_part, keep, sa, ra, as_.at[0], as_.at[1])
    attn = jnp.concatenate(total, axis=1)
    attn = attn * lax.rsqrt(jnp.mean(attn * attn, axis=1, keepdims=True) + EPSILON) * attention_gain[...]
    mid[...] = (residual[...].astype(F32) + attn).astype(BF16)
    m = mid[...].astype(F32)
    m = m * lax.rsqrt(jnp.mean(m * m, axis=1, keepdims=True) + EPSILON) * before_gain[...]
    normed[...] = m.astype(BF16)

    def share_cols(t):
        return pl.ds(pl.multiple_of(t * DV, DV), DV)

    def share_rows(t):
        return pl.ds(pl.multiple_of(t * piece, piece), piece)

    def to_width(k):
        t = (at.tp + k) % n_tp
        return remote(
            normed.at[:, share_cols(t)], block.at[share_rows(at.tp), :], ar.at[0, k], ar.at[1, k], (at.sp, t)
        )

    def start_width(k, carry):
        to_width(k).start()
        return carry

    def wait_width(k, carry):
        to_width(k).wait_recv()
        return carry

    lax.fori_loop(1, n_tp, start_width, 0)
    block[share_rows(at.tp), :] = normed[:, share_cols(at.tp)]

    lax.fori_loop(1, n_tp, wait_width, 0)
    picked = dot(spread[...], block[...]).astype(BF16)
    zs[...] = picked.reshape(zs.shape)

    def z_out(k):
        return remote(zs.at[(z + k) % Z], zr.at[z], zss.at[k], zrs.at[k], at.at(z=(z + k) % Z))

    for k in range(1, Z):
        z_out(k).start()
    zr[pl.ds(z, 1)] = zs[pl.ds(z, 1)]
    for k in range(1, Z):
        z_out(k).wait_recv()

    xs[...] = dot(turn_out[...], zr[...].reshape(slots, DV)).astype(BF16).reshape(xs.shape)

    side = x % C
    mine_half = x // C

    def x_out(k):
        to = (x + k) % X
        return (
            xs.at[to],
            rows.at[y, mine_half, :, share_cols(c)],
            xss.at[k],
            xrs.at[mine_half, c],
            at.at(x=to, c=side),
        )

    for k in range(1, X):
        remote(*x_out(k)).start()
    src, dst, s_sem, r_sem, to = x_out(0)

    @pl.when(side == c)
    def _():
        pltpu.make_async_copy(src, dst, r_sem).start()

    @pl.when(side != c)
    def _():
        remote(src, dst, s_sem, r_sem, pair).start()

    def gather(way, step, half):
        j = (y + Y - (step - 1)) % Y if way == 0 else (y + step - 1) % Y
        to = (y + 1) % Y if way == 0 else (y + Y - 1) % Y
        i = way * (2 * steps - 1) + (step - 1) * 2 + (half if step < steps else 0)
        return remote(rows.at[j, half], rows.at[j, half], gs.at[i], gr.at[i], at.at(y=to))

    gathers = []

    def start_gather(way, step, half):
        g = gather(way, step, half)
        g.start()
        gathers.append(g)

    for half in (0, 1):
        for core in range(C):
            pltpu.make_async_copy(xs.at[0], rows.at[y, half, :, pl.ds(core * DV, DV)], xrs.at[half, core]).wait()
        for way in (0, 1):
            start_gather(way, 1, half)

    count = rows.shape[1] * rows.shape[2]
    chunk = rows.shape[3]
    local[0].wait()
    local[1].wait()
    crossed[1].wait_recv()
    crossed[2].wait_recv()

    def grow(j, first=False):
        a = rows[pl.ds(j, 1)].reshape(count, chunk)
        at_rows = pl.ds(pl.multiple_of(j * chunk, chunk), chunk)
        for k in range(4):
            value = dot(a, gu[k, at_rows, :])
            acc[k] = value if first else acc[k] + value

    grow(y, True)
    for step in range(1, steps):
        for half in (0, 1):
            for way in (0, 1):
                gather(way, step, half).wait_recv()
                if step + 1 < steps or way == half:
                    start_gather(way, step + 1, half)
        grow((y + Y - step) % Y)
        grow((y + step) % Y)
    for way in (0, 1):
        gather(way, steps, way).wait_recv()
    grow((y + steps) % Y)

    for k in (0, 1):
        gate, up = acc[2 * k], acc[2 * k + 1]
        hid[k] = (gate * jax.nn.sigmoid(gate) * up).astype(BF16)

    local[2].wait()
    crossed[3].wait_recv()
    made = {}

    def down(offset):
        d = (y + offset + Y) % Y
        cols = pl.ds(pl.multiple_of(d * chunk, chunk), chunk)
        value = dot(hid[0], wd[0, :, cols]) + dot(hid[1], wd[1, :, cols])
        shares[offset + steps - 1] = value.reshape(2, count // 2, chunk)

    def down_part(offset, half):
        if offset not in made:
            down(offset)
            made[offset] = True
        return shares[offset + steps - 1, half]

    def keep_result(half, value):
        result[half] = value.astype(BF16)

    sum_b = ring_sum(at, down_part, keep_result, sb, rb, bs, br)

    def x_back(half, core):
        home = 2 * half + c
        return (
            result.at[half, :, pl.ds(core * DV, DV)],
            xb.at[x],
            xbs.at[2 * half + core],
            xbr.at[x],
            at.at(x=home, c=core),
        ), (home == x) & (c == core)

    for half in (0, 1):
        for core in range(C):
            args, here = x_back(half, core)

            @pl.when(here)
            def _(args=args):
                pltpu.make_async_copy(args[0], args[1], args[3]).start()

            @pl.when(jnp.logical_not(here))
            def _(args=args):
                remote(*args).start()

    for k in range(X):
        pltpu.make_async_copy(xs.at[0], xb.at[k], xbr.at[k]).wait()
    zs2[...] = dot(turn_back[...], xb[...].reshape(slots, DV)).astype(BF16).reshape(zs2.shape)

    def z_back(k):
        return remote(zs2.at[(z + k) % Z], zr2.at[z], zbs.at[k], zbr.at[k], at.at(z=(z + k) % Z))

    for k in range(1, Z):
        z_back(k).start()
    zr2[pl.ds(z, 1)] = zs2[pl.ds(z, 1)]
    for k in range(1, Z):
        z_back(k).wait_recv()
    lookup = zr2[...].reshape(slots, DV)
    column[...] = (
        weight_cols[0] * dot(find[0], lookup) + weight_cols[1] * dot(find[1], lookup)
    ).astype(BF16)

    def to_rows(k):
        t = (at.tp + k) % n_tp
        return remote(
            column.at[share_rows(t), :], branch.at[:, share_cols(at.tp)], fs.at[0, k], fs.at[1, k], (at.sp, t)
        )

    def start_rows(k, carry):
        to_rows(k).start()
        return carry

    def wait_rows(k, carry):
        to_rows(k).wait_recv()
        return carry

    lax.fori_loop(1, n_tp, start_rows, 0)
    branch[:, share_cols(at.tp)] = column[share_rows(at.tp), :]
    lax.fori_loop(1, n_tp, wait_rows, 0)
    b = branch[...].astype(F32)
    b = b * lax.rsqrt(jnp.mean(b * b, axis=1, keepdims=True) + EPSILON) * after_gain[...]
    out[...] = (mid[...].astype(F32) + b).astype(BF16)

    for k in range(1, X):
        state_x(k).wait_send()
    for k in range(1, Z):

        @pl.when(z + k < Z)
        def _(k=k):
            state_z(k).wait_send()

    swap.wait_send()
    for k in crossed + sum_a + gathers + sum_b:
        k.wait_send()

    def wait_sent(k, carry):
        to_width(k).wait_send()
        to_rows(k).wait_send()
        return carry

    lax.fori_loop(1, n_tp, wait_sent, 0)
    for k in range(1, Z):
        z_out(k).wait_send()
        z_back(k).wait_send()
    for k in range(1, X):
        remote(*x_out(k)).wait_send()

    @pl.when(side != c)
    def _():
        remote(src, dst, s_sem, r_sem, pair).wait_send()

    for half in (0, 1):
        for core in range(C):
            args, here = x_back(half, core)

            @pl.when(jnp.logical_not(here))
            def _(args=args):
                remote(*args).wait_send()


def shards(
    query, key, value, gate_rows, decay, bias, extra, head_gain, output_projection, residual,
    attention_gain, before_gain, after_gain, w_gate, w_up, w_down, ids, weights,
):
    n_sp, n_tp = lax.axis_size("sp"), lax.axis_size("tp")
    tokens, width = query.shape[0], residual.shape[1]
    piece = residual.shape[0]
    X, C = GROUP_SIZE, CORES
    Z, Y = n_sp // X, n_tp // C
    cap = 5 * tokens // (2 * n_sp)
    slots = n_sp * cap
    steps = Y // 2
    msgs = 2 * (2 * steps - 1)
    half = slots // 4
    chunk = C * DV
    hidden = w_gate.shape[2]
    vm, hbm = pl.BlockSpec(memory_space=pltpu.VMEM), pl.BlockSpec(memory_space=pl.ANY)
    sem = pltpu.SemaphoreType.DMA
    message = (KEY_CHANNELS + 16, DV)
    scratch = [
        pltpu.VMEM((Y, C, piece, DV), BF16),
        pltpu.VMEM((128, tokens), F32),
        pltpu.VMEM((slots, tokens), BF16),
        pltpu.VMEM((TOP, tokens, slots), BF16),
        pltpu.VMEM((slots, slots), BF16),
        pltpu.VMEM((slots, slots), BF16),
        pltpu.VMEM(message, BF16),
        pltpu.VMEM((X, *message), BF16),
        pltpu.VMEM(message, BF16),
        pltpu.VMEM((Z, *message), BF16),
        pltpu.VMEM((4, width, hidden), BF16),
        pltpu.VMEM((2, hidden, width), BF16),
        pltpu.VMEM((2, DV, width), BF16),
        pltpu.VMEM((Y, piece, DV), BF16),
        pltpu.VMEM((Y, piece, width), F32),
        pltpu.VMEM((piece, width), BF16),
        pltpu.VMEM((piece, width), BF16),
        pltpu.VMEM((tokens, DV), BF16),
        pltpu.VMEM((Y, 2, half, chunk), BF16),
        pltpu.VMEM((4, 2 * half, hidden), F32),
        pltpu.VMEM((2, 2 * half, hidden), BF16),
        pltpu.VMEM((Y, 2, half, chunk), F32),
        pltpu.VMEM((2, half, chunk), BF16),
        pltpu.VMEM((Z, X * cap, DV), BF16),
        pltpu.VMEM((Z, X * cap, DV), BF16),
        pltpu.VMEM((X, Z * cap, DV), BF16),
        pltpu.VMEM((X, Z * cap, DV), BF16),
        pltpu.VMEM((Z, X * cap, DV), BF16),
        pltpu.VMEM((Z, X * cap, DV), BF16),
        pltpu.VMEM((tokens, DV), BF16),
        pltpu.VMEM((piece, width), BF16),
        pltpu.VMEM((msgs, piece, width // 2), BF16),
        pltpu.VMEM((msgs, piece, width // 2), BF16),
        pltpu.VMEM((msgs, half, chunk), BF16),
        pltpu.VMEM((msgs, half, chunk), BF16),
        sem((4,)), sem((4,)), sem((4,)), sem((2,)),
        sem((2, msgs)),
        sem((2, n_tp)),
        sem((Z,)), sem((Z,)),
        sem((X,)), sem((2, C)),
        sem((msgs,)), sem((msgs,)),
        sem((msgs,)), sem((msgs,)),
        sem((2 * C,)), sem((X,)),
        sem((Z,)), sem((Z,)),
        sem((2, n_tp)),
        sem((X,)), sem((X,)), sem((Z,)), sem((Z,)),
    ]
    return pl.pallas_call(
        functools.partial(layer_kernel, n_sp, n_tp, X, cap),
        out_shape=jax.ShapeDtypeStruct((piece, width), BF16),
        in_specs=[vm] * 8 + [hbm] + [vm] * 4 + [hbm] * 3 + [vm] * 2,
        out_specs=vm,
        scratch_shapes=scratch,
        name="layer",
        compiler_params=pltpu.CompilerParams(
            collective_id=0, has_side_effects=True, vmem_limit_bytes=60 * 1024 * 1024
        ),
    )(
        query.T, key.T, value, gate_rows, decay.T, bias[None], extra.T, head_gain[None],
        output_projection, residual, attention_gain[None], before_gain[None], after_gain[None],
        w_gate[0], w_up[0], w_down[0], ids.T, weights.T,
    )


def solution(mesh):
    placed = (
        P("sp", "tp"),
        P("sp", "tp"),
        P("sp", "tp"),
        P("sp", "tp"),
        P("sp", "tp"),
        P("tp"),
        P("sp", "tp"),
        P(),
        P("tp", None),
        P(("sp", "tp"), None),
        P(),
        P(),
        P(),
        P("sp", None, "tp"),
        P("sp", None, "tp"),
        P("sp", "tp", None),
        P("sp", None),
        P("sp", None),
    )
    return jax.shard_map(
        shards, mesh=mesh, in_specs=placed, out_specs=P(("sp", "tp"), None), check_vma=False
    )
```

```python
import functools

import jax
import jax.numpy as jnp
from jax import lax
from jax.experimental import pallas as pl
from jax.experimental.pallas import tpu as pltpu
from jax.sharding import PartitionSpec as P

KEY_CHANNELS = 64
DV = 128
TOP = 2
BLOCK = 64
GROUP_SIZE = 4
CORES = 2

EPSILON = 1e-06
DECAY_NORMALIZER = 16.0
MESH = pl.DeviceIdType.MESH
BF16 = jnp.bfloat16
F32 = jnp.float32
PARTS = 4


def dot(a, b):
    return jnp.dot(a, b, preferred_element_type=F32)


class Place:
    def __init__(self, n_sp, n_tp, group):
        self.X, self.Z = group, n_sp // group
        self.C, self.Y = CORES, n_tp // CORES
        self.n_tp = n_tp
        self.sp, self.tp = lax.axis_index("sp"), lax.axis_index("tp")
        self.z, self.x = self.sp // self.X, self.sp % self.X
        self.y, self.c = self.tp // self.C, self.tp % self.C

    def at(self, z=None, x=None, y=None, c=None):
        z = self.z if z is None else z
        x = self.x if x is None else x
        y = self.y if y is None else y
        c = self.c if c is None else c
        return (z * self.X + x, y * self.C + c)


def remote(src, dst, send, recv, to):
    return pltpu.make_async_remote_copy(
        src_ref=src, dst_ref=dst, send_sem=send, recv_sem=recv, device_id=to, device_id_type=MESH
    )


def ring_index(way, step, part, steps):
    first = part % (PARTS // 2) if step == 1 else PARTS // 2 + (step - 2) * PARTS + part
    return way * ring_size(steps) + first


def ring_size(steps):
    return PARTS // 2 + (steps - 1) * PARTS


def way_parts(way):
    low, high = list(range(PARTS // 2)), list(range(PARTS // 2, PARTS))
    return (low, high) if way == 0 else (high, low)


def both_ways(pick):
    return [(way, part) for pair in zip(pick(0), pick(1)) for way, part in enumerate(pair)]


def whole(ref, sem):
    return pltpu.make_async_copy(ref, ref, sem)


def ring_sum(at, part_of, out, sends, recvs, send_sem, recv_sems):
    Y, steps, y = at.Y, at.Y // 2, at.y

    def copy(way, step, part):
        i = ring_index(way, step, part, steps)
        to = (y + 1) % Y if way == 0 else (y + Y - 1) % Y
        return remote(sends.at[i], recvs.at[i], send_sem, recv_sems.at[i], at.at(y=to))

    def offset(way, step):
        k = steps - step + 1
        return k if way == 0 or k == steps else -k

    def send(way, step, part, value):
        sends[ring_index(way, step, part, steps)] = value.astype(BF16)
        copy(way, step, part).start()

    for way, part in both_ways(lambda w: way_parts(w)[0]):
        send(way, 1, part, part_of(offset(way, 1), part))
    for step in range(2, steps + 1):
        for way, part in both_ways(lambda w: way_parts(w)[1] + way_parts(w)[0]):
            value = part_of(offset(way, step), part)
            if step > 2 or part in way_parts(way)[0]:
                copy(way, step - 1, part).wait_recv()
                value = value + recvs[ring_index(way, step - 1, part, steps)].astype(F32)
            send(way, step, part, value)
    for part in range(PARTS):
        total = part_of(0, part)
        for way in (0, 1):
            copy(way, steps, part).wait_recv()
            total = total + recvs[ring_index(way, steps, part, steps)].astype(F32)
        out(part, total)


def far_first(count):
    return sorted(range(1, count), key=lambda k: (-min(k, count - k), k))


def split(value):
    high = value.astype(BF16)
    rest = value - high.astype(F32)
    middle = rest.astype(BF16)
    return high, middle, (rest - middle.astype(F32)).astype(BF16)


def standing(row, count):
    square = (count, row.shape[1])
    same = lax.broadcasted_iota(jnp.int32, square, 0) == lax.broadcasted_iota(jnp.int32, square, 1)
    return jnp.sum(jnp.where(same, row, 0.0), axis=1, keepdims=True)


def lying(col, width):
    square = (col.shape[0], width)
    same = lax.broadcasted_iota(jnp.int32, square, 0) == lax.broadcasted_iota(jnp.int32, square, 1)
    return jnp.sum(jnp.where(same, col, 0.0), axis=0, keepdims=True)


def layer_kernel(
    n_sp, n_tp, group, cap,
    operands, w_out, w_gate, w_up, w_down,
    out,
    held,
    gated, stack, spread, find, turn_out, turn_back, sx, rx, sz, rz,
    gu, wd, wo, partner, mixed, mid, normed, block, rows, acc, hid, shares, result,
    zs, zr, xs, xb, zs2, zr2, column, branch,
    sa, ra, sb, rb,
    wsem, wrs, wrr, gsem, sums, gr, xrs, xbs, szs, szr, osem, done, came,
):
    at = Place(n_sp, n_tp, group)
    X, Y, Z, C = at.X, at.Y, at.Z, at.C
    x, y, z, c = at.x, at.y, at.z, at.c
    steps = Y // 2
    other = 1 - c

    (
        q_t, k_t, values, gate_rows, decay_t, bias, extra, head_gain,
        residual, attention_gain, before_gain, after_gain, ids_row, weights_row,
    ) = held
    loads = [pltpu.make_async_copy(a, b, osem.at[k]) for k, (a, b) in enumerate(zip(operands, held))]
    for k in loads:
        k.start()
    local = [
        pltpu.make_async_copy(w_gate, gu.at[0], wsem.at[0]),
        pltpu.make_async_copy(w_up, gu.at[1], wsem.at[1]),
        pltpu.make_async_copy(w_down, wd.at[0], wsem.at[2]),
        pltpu.make_async_copy(w_out, wo.at[0], wsem.at[3]),
    ]
    rz[...] = jnp.zeros_like(rz)
    barrier = pltpu.get_barrier_semaphore()

    def greet_tp(k, carry):
        pl.semaphore_signal(barrier, inc=1, device_id=(at.sp, (at.tp + k) % n_tp), device_id_type=MESH)
        return carry

    lax.fori_loop(1, n_tp, greet_tp, 0)
    for k in range(1, Z):
        pl.semaphore_signal(barrier, inc=1, device_id=at.at(z=(z + k) % Z), device_id_type=MESH)
    for k in range(1, X):
        for core in range(C):
            pl.semaphore_signal(barrier, inc=1, device_id=at.at(x=(x + k) % X, c=core), device_id_type=MESH)

    for k in (3, 0, 1, 2):
        local[k].start()
    for k in loads:
        k.wait()

    tokens = q_t.shape[1]
    blocks = tokens // BLOCK
    pre = decay_t[...].astype(F32) + standing(bias[...], KEY_CHANNELS)
    log_decay = -(jnp.maximum(-pre, 0.0) + jnp.log1p(jnp.exp(-jnp.abs(pre)))) / DECAY_NORMALIZER + extra[...]
    r, q = (lax.broadcasted_iota(jnp.int32, (tokens, tokens), k) for k in (0, 1))
    one_block = (r // BLOCK) == (q // BLOCK)
    upto = jnp.where((r <= q) & one_block, 1.0, 0.0).astype(BF16)
    inside = sum(dot(term, upto) for term in split(log_decay))
    ends = [inside[:, (b + 1) * BLOCK - 1 : (b + 1) * BLOCK] for b in range(blocks)]
    of_block = lax.broadcasted_iota(jnp.int32, (KEY_CHANNELS, tokens), 1) // BLOCK
    keys = k_t[...].astype(F32)
    to_end = [jnp.where(of_block == b, keys * jnp.exp(jnp.minimum(ends[b] - inside, 0.0)), 0.0) for b in range(blocks)]
    vals = values[...]
    growth = dot(jnp.concatenate(to_end, axis=0).astype(BF16), vals)
    growth = [growth[b * KEY_CHANNELS : (b + 1) * KEY_CHANNELS] for b in range(blocks)]
    fades = [jnp.exp(e) for e in ends]
    state = growth[0]
    for b in range(1, blocks):
        state = fades[b] * state + growth[b]
    fade_row = lying(jnp.exp(sum(ends)), DV)
    tail = KEY_CHANNELS + 16

    def message(ref, state_part, row):
        ref[0:KEY_CHANNELS, :] = state_part.astype(BF16)
        ref[KEY_CHANNELS:tail, :] = jnp.broadcast_to(row, (16, DV)).astype(BF16)

    message(sx, state, fade_row)
    pl.semaphore_wait(barrier, n_tp - 1 + Z - 1 + (X - 1) * C)

    def state_x(k):
        return remote(sx, rx.at[x], done.at[7], came.at[4], at.at(x=(x + k) % X))

    for k in range(1, X):
        state_x(k).start()
    pair = at.at(c=other)
    crossed = [
        remote(w_out, wo.at[1], wrs.at[3], wrr.at[3], pair),
        remote(w_gate, gu.at[2], wrs.at[0], wrr.at[0], pair),
        remote(w_up, gu.at[3], wrs.at[1], wrr.at[1], pair),
        remote(w_down, wd.at[1], wrs.at[2], wrr.at[2], pair),
    ]
    for k in crossed:
        k.start()
    rx[pl.ds(x, 1)] = sx[...].reshape(1, tail, DV)

    slots = n_sp * cap
    sub = lax.broadcasted_iota(jnp.int32, (n_sp, tokens), 0)
    chosen = [ids_row[k : k + 1, :] for k in range(TOP)]
    named = jnp.where((sub == chosen[0]) | (sub == chosen[1]), 1.0, 0.0).astype(BF16)
    before = dot(named, jnp.where(r < q, 1.0, 0.0).astype(BF16))
    targets = []
    for e in chosen:
        slot = jnp.sum(jnp.where(sub == e, before, 0.0), axis=0, keepdims=True)
        targets.append(e * cap + slot.astype(jnp.int32))
    query = q_t[...].astype(F32) * (KEY_CHANNELS**-0.5 * jnp.exp(inside))
    stack[0:KEY_CHANNELS, :] = query
    stack[KEY_CHANNELS:, :] = jnp.zeros((stack.shape[0] - KEY_CHANNELS, tokens), F32)
    for k in range(TOP):
        stack[KEY_CHANNELS + k : KEY_CHANNELS + k + 1, :] = targets[k].astype(F32)
        stack[KEY_CHANNELS + TOP + k : KEY_CHANNELS + TOP + k + 1, :] = weights_row[k : k + 1, :]
    stood = stack[...].T
    query = stood[:, 0:KEY_CHANNELS].astype(BF16)
    target_cols = [stood[:, KEY_CHANNELS + k : KEY_CHANNELS + k + 1].astype(jnp.int32) for k in range(TOP)]
    weight_cols = [stood[:, KEY_CHANNELS + TOP + k : KEY_CHANNELS + TOP + k + 1] for k in range(TOP)]
    scores = dot(query, (keys * jnp.exp(-inside)).astype(BF16))
    scores = jnp.where((r >= q) & one_block, scores, 0.0).astype(BF16)
    within = dot(scores, vals)

    whole(rx.at[pl.ds(0, X - 1)], came.at[4]).wait()
    plane, plane_row = rx[0, 0:KEY_CHANNELS].astype(F32), rx[0, KEY_CHANNELS:tail][0:1].astype(F32)
    ahead, ahead_fade = jnp.zeros_like(state), jnp.ones((KEY_CHANNELS, 1), F32)
    for k in range(X):
        part, row = rx[k, 0:KEY_CHANNELS].astype(F32), rx[k, KEY_CHANNELS:tail][0:1].astype(F32)
        fade = standing(row, KEY_CHANNELS)
        ahead = jnp.where(k < x, fade * ahead + part, ahead)
        ahead_fade = jnp.where(k < x, fade * ahead_fade, ahead_fade)
        if k:
            plane, plane_row = fade * plane + part, plane_row * row
    message(sz, plane, plane_row)

    def state_z(k):
        return remote(sz, rz.at[z], szs.at[k], szr.at[k], at.at(z=(z + k) % Z))

    for k in range(1, Z):

        @pl.when(z + k < Z)
        def _(k=k):
            state_z(k).start()

    tall = lax.broadcasted_iota(jnp.int32, (slots, tokens), 0)
    hits = [jnp.where(tall == t, 1.0, 0.0) for t in targets]
    spread[...] = (hits[0] + hits[1]).astype(BF16)
    wide = lax.broadcasted_iota(jnp.int32, (tokens, slots), 1)
    for k in range(TOP):
        find[k] = jnp.where(wide == target_cols[k], 1.0, 0.0).astype(BF16)
    lane = lax.broadcasted_iota(jnp.int32, (1, slots), 1)

    def turned(outer, inner):
        a = sum(jnp.where(lane >= k * inner * cap, 1, 0) for k in range(1, outer))
        rest = lane - a * (inner * cap)
        b = sum(jnp.where(rest >= k * cap, 1, 0) for k in range(1, inner))
        return b * (outer * cap) + a * cap + (rest - b * cap)

    down_rows = lax.broadcasted_iota(jnp.int32, (slots, slots), 0)
    turn_out[...] = jnp.where(down_rows == turned(Z, X), 1.0, 0.0).astype(BF16)
    turn_back[...] = jnp.where(down_rows == turned(X, Z), 1.0, 0.0).astype(BF16)
    gate_act = gate_rows[...].astype(F32)
    gate_act = gate_act * jax.nn.sigmoid(gate_act) * head_gain[...]

    for k in range(1, Z):

        @pl.when(z >= k)
        def _(k=k):
            state_z(k).wait_recv()

    carried = jnp.zeros_like(state)
    for k in range(Z - 1):
        fade = standing(rz[k, KEY_CHANNELS:tail][0:1].astype(F32), KEY_CHANNELS)
        carried = jnp.where(k < z, fade * carried + rz[k, 0:KEY_CHANNELS].astype(F32), carried)
    running = ahead_fade * carried + ahead
    across = []
    for b in range(blocks):
        across.append(dot(query[b * BLOCK : (b + 1) * BLOCK], running.astype(BF16)))
        running = fades[b] * running + growth[b]
    heads = within + jnp.concatenate(across, axis=0)
    heads = heads * lax.rsqrt(jnp.mean(heads * heads, axis=1, keepdims=True) + EPSILON) * gate_act
    gated[...] = heads.astype(BF16).reshape(gated.shape)
    swap = remote(gated.at[:, other], partner, gsem.at[0], gsem.at[1], pair)
    swap.start()

    share = gated.shape[0]
    piece = gated.shape[2]
    width = wo.shape[2]
    swap.wait_recv()
    local[3].wait()
    crossed[0].wait_recv()
    mine = gated[:, pl.ds(c, 1)].reshape(share * piece, DV)
    theirs = partner[...].reshape(share * piece, DV)
    tile = width // 4
    for k in range(4):
        cols = slice(k * tile, (k + 1) * tile)
        value = dot(mine, wo[0, :, cols]) + dot(theirs, wo[1, :, cols])
        mixed[:, :, cols] = value.reshape(share, piece, tile)

    part_width = width // PARTS

    def mixed_part(k, part):
        d = (y + k + Y) % Y
        return mixed[pl.ds(d, 1), :, part * part_width : (part + 1) * part_width].reshape(piece, part_width)

    total = [None] * PARTS

    def keep(part, value):
        total[part] = value

    ring_sum(at, mixed_part, keep, sa, ra, done.at[0], sums)
    attn = jnp.concatenate(total, axis=1)
    attn = attn * lax.rsqrt(jnp.mean(attn * attn, axis=1, keepdims=True) + EPSILON) * attention_gain[...]
    mid[...] = (residual[...].astype(F32) + attn).astype(BF16)
    m = mid[...].astype(F32)
    m = m * lax.rsqrt(jnp.mean(m * m, axis=1, keepdims=True) + EPSILON) * before_gain[...]
    normed[...] = m.astype(BF16)

    def share_cols(t):
        return pl.ds(pl.multiple_of(t * DV, DV), DV)

    def share_rows(t):
        return pl.ds(pl.multiple_of(t * piece, piece), piece)

    def to_width(k):
        t = (at.tp + k) % n_tp
        return remote(
            normed.at[:, share_cols(t)], block.at[share_rows(at.tp), :], done.at[3], came.at[0], (at.sp, t)
        )

    def start_width(k, carry):
        to_width(k).start()
        return carry

    lax.fori_loop(1, n_tp, start_width, 0)
    block[share_rows(at.tp), :] = normed[:, share_cols(at.tp)]

    others = block.at[pl.ds(0, (n_tp - 1) * piece)]
    whole(others, came.at[0]).wait()
    picked = dot(spread[...], block[...]).astype(BF16)
    zs[...] = picked.reshape(zs.shape)

    def z_out(k):
        return remote(zs.at[(z + k) % Z], zr.at[z], done.at[5], came.at[2], at.at(z=(z + k) % Z))

    for k in far_first(Z):
        z_out(k).start()
    zr[pl.ds(z, 1)] = zs[pl.ds(z, 1)]
    whole(zr.at[pl.ds(0, Z - 1)], came.at[2]).wait()

    xs[...] = dot(turn_out[...], zr[...].reshape(slots, DV)).astype(BF16).reshape(xs.shape)

    side = x % C
    mine_half = x // C
    per = PARTS // 2

    def x_out(k):
        to = (x + k) % X
        return (
            xs.at[to],
            rows.at[y, pl.ds(mine_half * per, per), :, share_cols(c)],
            done.at[8 if k else 9],
            xrs.at[mine_half],
            at.at(x=to, c=side),
        )

    for k in range(1, X):
        remote(*x_out(k)).start()
    src, dst, s_sem, r_sem, to = x_out(0)

    @pl.when(side == c)
    def _():
        pltpu.make_async_copy(src, dst, r_sem).start()

    @pl.when(side != c)
    def _():
        remote(src, dst, s_sem, r_sem, pair).start()

    def gather(way, step, part):
        j = (y + Y - (step - 1)) % Y if way == 0 else (y + step - 1) % Y
        to = (y + 1) % Y if way == 0 else (y + Y - 1) % Y
        i = way * ring_size(steps) + (step - 1) * PARTS + (part if step < steps else part % per)
        return remote(rows.at[j, part], rows.at[j, part], done.at[2], gr.at[i], at.at(y=to))

    def start_gather(way, step, part):
        gather(way, step, part).start()

    for half in (0, 1):
        whole(rows.at[y, pl.ds(half * per, per)], xrs.at[half]).wait()
        for part in range(half * per, half * per + per):
            for way in (0, 1):
                start_gather(way, 1, part)

    count = rows.shape[1] * rows.shape[2]
    chunk = rows.shape[3]
    local[0].wait()
    local[1].wait()
    crossed[1].wait_recv()
    crossed[2].wait_recv()

    def grow(j, first=False):
        a = rows[pl.ds(j, 1)].reshape(count, chunk)
        at_rows = pl.ds(pl.multiple_of(j * chunk, chunk), chunk)
        for k in range(4):
            value = dot(a, gu[k, at_rows, :])
            acc[k] = value if first else acc[k] + value

    grow(y, True)
    for step in range(1, steps):
        for part in range(PARTS):
            for way in (0, 1):
                gather(way, step, part).wait_recv()
                if step + 1 < steps or way == part // per:
                    start_gather(way, step + 1, part)
        grow((y + Y - step) % Y)
        grow((y + step) % Y)
    for part in range(PARTS):
        gather(part // per, steps, part).wait_recv()
    grow((y + steps) % Y)

    for k in (0, 1):
        gate, up = acc[2 * k], acc[2 * k + 1]
        hid[k] = (gate * jax.nn.sigmoid(gate) * up).astype(BF16)

    local[2].wait()
    crossed[3].wait_recv()
    made = {}

    def down(offset):
        d = (y + offset + Y) % Y
        cols = pl.ds(pl.multiple_of(d * chunk, chunk), chunk)
        value = dot(hid[0], wd[0, :, cols]) + dot(hid[1], wd[1, :, cols])
        shares[offset + steps - 1] = value.reshape(PARTS, count // PARTS, chunk)

    def down_part(offset, part):
        if offset not in made:
            down(offset)
            made[offset] = True
        return shares[offset + steps - 1, part]

    def x_back(half, core):
        home = 2 * half + c
        return (
            result.at[pl.ds(half * per, per), :, pl.ds(core * DV, DV)],
            xb.at[x],
            xbs.at[2 * half + core],
            came.at[5],
            at.at(x=home, c=core),
        ), (home == x) & (c == core)

    def keep_result(part, value):
        result[part] = value.astype(BF16)
        if part % per < per - 1:
            return
        for core in range(C):
            args, here = x_back(part // per, core)

            @pl.when(here)
            def _(args=args):
                pltpu.make_async_copy(args[0], args[1], args[3]).start()

            @pl.when(jnp.logical_not(here))
            def _(args=args):
                remote(*args).start()

    ring_sum(at, down_part, keep_result, sb, rb, done.at[1], sums)

    whole(xb, came.at[5]).wait()
    zs2[...] = dot(turn_back[...], xb[...].reshape(slots, DV)).astype(BF16).reshape(zs2.shape)

    def z_back(k):
        return remote(zs2.at[(z + k) % Z], zr2.at[z], done.at[6], came.at[3], at.at(z=(z + k) % Z))

    for k in far_first(Z):
        z_back(k).start()
    zr2[pl.ds(z, 1)] = zs2[pl.ds(z, 1)]
    whole(zr2.at[pl.ds(0, Z - 1)], came.at[3]).wait()
    lookup = zr2[...].reshape(slots, DV)
    column[...] = (
        weight_cols[0] * dot(find[0], lookup) + weight_cols[1] * dot(find[1], lookup)
    ).astype(BF16)

    def to_rows(k):
        t = (at.tp + k) % n_tp
        return remote(
            column.at[share_rows(t), :], branch.at[:, share_cols(at.tp)], done.at[4], came.at[1], (at.sp, t)
        )

    def start_rows(k, carry):
        to_rows(k).start()
        return carry

    lax.fori_loop(1, n_tp, start_rows, 0)
    branch[:, share_cols(at.tp)] = column[share_rows(at.tp), :]
    whole(others, came.at[1]).wait()
    b = branch[...].astype(F32)
    b = b * lax.rsqrt(jnp.mean(b * b, axis=1, keepdims=True) + EPSILON) * after_gain[...]
    out[...] = (mid[...].astype(F32) + b).astype(BF16)

    whole(rx.at[pl.ds(0, X - 1)], done.at[7]).wait()
    for k in range(1, Z):

        @pl.when(z + k < Z)
        def _(k=k):
            state_z(k).wait_send()

    swap.wait_send()
    for k in crossed:
        k.wait_send()
    whole(sa, done.at[0]).wait()
    whole(sb, done.at[1]).wait()
    whole(rows.at[pl.ds(0, Y - 1)], done.at[2]).wait()
    whole(others, done.at[3]).wait()
    whole(others, done.at[4]).wait()
    whole(zr.at[pl.ds(0, Z - 1)], done.at[5]).wait()
    whole(zr2.at[pl.ds(0, Z - 1)], done.at[6]).wait()
    whole(xs.at[pl.ds(0, X - 1)], done.at[8]).wait()

    @pl.when(side != c)
    def _():
        remote(src, dst, s_sem, r_sem, pair).wait_send()

    for half in (0, 1):
        for core in range(C):
            args, here = x_back(half, core)

            @pl.when(jnp.logical_not(here))
            def _(args=args):
                remote(*args).wait_send()


def shards(
    query, key, value, gate_rows, decay, bias, extra, head_gain, output_projection, residual,
    attention_gain, before_gain, after_gain, w_gate, w_up, w_down, ids, weights,
):
    n_sp, n_tp = lax.axis_size("sp"), lax.axis_size("tp")
    tokens, width = query.shape[0], residual.shape[1]
    piece = residual.shape[0]
    X, C = GROUP_SIZE, CORES
    Z, Y = n_sp // X, n_tp // C
    cap = 5 * tokens // (2 * n_sp)
    slots = n_sp * cap
    steps = Y // 2
    msgs = 2 * ring_size(steps)
    part = slots // C // PARTS
    chunk = C * DV
    hidden = w_gate.shape[2]
    hbm = pl.BlockSpec(memory_space=pltpu.HBM)
    sem = pltpu.SemaphoreType.DMA
    message = (KEY_CHANNELS + 16, DV)
    operands = [
        query.T, key.T, value, gate_rows, decay.T, bias[None], extra.T, head_gain[None],
        residual, attention_gain[None], before_gain[None], after_gain[None], ids.T, weights.T,
    ]
    scratch = [
        [pltpu.VMEM(a.shape, a.dtype) for a in operands],
        pltpu.VMEM((Y, C, piece, DV), BF16),
        pltpu.VMEM((128, tokens), F32),
        pltpu.VMEM((slots, tokens), BF16),
        pltpu.VMEM((TOP, tokens, slots), BF16),
        pltpu.VMEM((slots, slots), BF16),
        pltpu.VMEM((slots, slots), BF16),
        pltpu.VMEM(message, BF16),
        pltpu.VMEM((X, *message), BF16),
        pltpu.VMEM(message, BF16),
        pltpu.VMEM((Z, *message), BF16),
        pltpu.VMEM((4, width, hidden), BF16),
        pltpu.VMEM((2, hidden, width), BF16),
        pltpu.VMEM((2, DV, width), BF16),
        pltpu.VMEM((Y, piece, DV), BF16),
        pltpu.VMEM((Y, piece, width), F32),
        pltpu.VMEM((piece, width), BF16),
        pltpu.VMEM((piece, width), BF16),
        pltpu.VMEM((tokens, DV), BF16),
        pltpu.VMEM((Y, PARTS, part, chunk), BF16),
        pltpu.VMEM((4, PARTS * part, hidden), F32),
        pltpu.VMEM((2, PARTS * part, hidden), BF16),
        pltpu.VMEM((Y, PARTS, part, chunk), F32),
        pltpu.VMEM((PARTS, part, chunk), BF16),
        pltpu.VMEM((Z, X * cap, DV), BF16),
        pltpu.VMEM((Z, X * cap, DV), BF16),
        pltpu.VMEM((X, PARTS // 2, part, DV), BF16),
        pltpu.VMEM((X, PARTS // 2, part, DV), BF16),
        pltpu.VMEM((Z, X * cap, DV), BF16),
        pltpu.VMEM((Z, X * cap, DV), BF16),
        pltpu.VMEM((tokens, DV), BF16),
        pltpu.VMEM((piece, width), BF16),
        pltpu.VMEM((msgs, piece, width // PARTS), BF16),
        pltpu.VMEM((msgs, piece, width // PARTS), BF16),
        pltpu.VMEM((msgs, part, chunk), BF16),
        pltpu.VMEM((msgs, part, chunk), BF16),
        sem((4,)), sem((4,)), sem((4,)), sem((2,)), sem((msgs,)), sem((msgs,)), sem((2,)), sem((2 * C,)),
        sem((Z,)), sem((Z,)), sem((len(operands),)), sem((10,)), sem((6,)),
    ]
    return pl.pallas_call(
        functools.partial(layer_kernel, n_sp, n_tp, X, cap),
        out_shape=jax.ShapeDtypeStruct((piece, width), BF16),
        in_specs=[[hbm] * len(operands), hbm, hbm, hbm, hbm],
        out_specs=pl.BlockSpec(memory_space=pltpu.VMEM),
        scratch_shapes=scratch,
        name="layer",
        compiler_params=pltpu.CompilerParams(
            collective_id=0, has_side_effects=True, vmem_limit_bytes=40 * 1024 * 1024
        ),
    )(
        *jax.tree.map(lambda a: pltpu.with_memory_space_constraint(a, pltpu.HBM), (operands, output_projection, w_gate[0], w_up[0], w_down[0]))
    )


def solution(mesh):
    placed = (
        P("sp", "tp"),
        P("sp", "tp"),
        P("sp", "tp"),
        P("sp", "tp"),
        P("sp", "tp"),
        P("tp"),
        P("sp", "tp"),
        P(),
        P("tp", None),
        P(("sp", "tp"), None),
        P(),
        P(),
        P(),
        P("sp", None, "tp"),
        P("sp", None, "tp"),
        P("sp", "tp", None),
        P("sp", None),
        P("sp", None),
    )
    return jax.shard_map(
        shards, mesh=mesh, in_specs=placed, out_specs=P(("sp", "tp"), None), check_vma=False
    )
```

```python
import functools

import jax
import jax.numpy as jnp
from jax import lax
from jax.experimental import pallas as pl
from jax.experimental.pallas import tpu as pltpu
from jax.sharding import PartitionSpec as P

KEY_CHANNELS = 64
DV = 128
TOP = 2
BLOCK = 64
GROUP_SIZE = 4
CORES = 2

EPSILON = 1e-06
DECAY_NORMALIZER = 16.0
MESH = pl.DeviceIdType.MESH
BF16 = jnp.bfloat16
F32 = jnp.float32
PARTS = 4


def dot(a, b):
    return jnp.dot(a, b, preferred_element_type=F32)


class Place:
    def __init__(self, n_sp, n_tp, group):
        self.X, self.Z = group, n_sp // group
        self.C, self.Y = CORES, n_tp // CORES
        self.n_tp = n_tp
        self.sp, self.tp = lax.axis_index("sp"), lax.axis_index("tp")
        self.z, self.x = self.sp // self.X, self.sp % self.X
        self.y, self.c = self.tp // self.C, self.tp % self.C

    def at(self, z=None, x=None, y=None, c=None):
        z = self.z if z is None else z
        x = self.x if x is None else x
        y = self.y if y is None else y
        c = self.c if c is None else c
        return (z * self.X + x, y * self.C + c)


def remote(src, dst, send, recv, to):
    return pltpu.make_async_remote_copy(
        src_ref=src, dst_ref=dst, send_sem=send, recv_sem=recv, device_id=to, device_id_type=MESH
    )


def ring_index(way, step, part, steps):
    first = part % (PARTS // 2) if step == 1 else PARTS // 2 + (step - 2) * PARTS + part
    return way * ring_size(steps) + first


def ring_size(steps):
    return PARTS // 2 + (steps - 1) * PARTS


def way_parts(way):
    low, high = list(range(PARTS // 2)), list(range(PARTS // 2, PARTS))
    return (low, high) if way == 0 else (high, low)


def both_ways(pick):
    return [(way, part) for pair in zip(pick(0), pick(1)) for way, part in enumerate(pair)]


def whole(ref, sem):
    return pltpu.make_async_copy(ref, ref, sem)


def ring_sum(at, part_of, out, sends, recvs, send_sem, recv_sems):
    Y, steps, y = at.Y, at.Y // 2, at.y

    def copy(way, step, part):
        i = ring_index(way, step, part, steps)
        to = (y + 1) % Y if way == 0 else (y + Y - 1) % Y
        return remote(sends.at[i], recvs.at[i], send_sem, recv_sems.at[i], at.at(y=to))

    def offset(way, step):
        k = steps - step + 1
        return k if way == 0 or k == steps else -k

    def send(way, step, part, value):
        sends[ring_index(way, step, part, steps)] = value.astype(BF16)
        copy(way, step, part).start()

    for way, part in both_ways(lambda w: way_parts(w)[0]):
        send(way, 1, part, part_of(offset(way, 1), part))
    for step in range(2, steps + 1):
        for way, part in both_ways(lambda w: way_parts(w)[1] + way_parts(w)[0]):
            value = part_of(offset(way, step), part)
            if step > 2 or part in way_parts(way)[0]:
                copy(way, step - 1, part).wait_recv()
                value = value + recvs[ring_index(way, step - 1, part, steps)].astype(F32)
            send(way, step, part, value)
    for part in range(PARTS):
        total = part_of(0, part)
        for way in (0, 1):
            copy(way, steps, part).wait_recv()
            total = total + recvs[ring_index(way, steps, part, steps)].astype(F32)
        out(part, total)


def far_first(count):
    return sorted(range(1, count), key=lambda k: (-min(k, count - k), k))


def split(value):
    high = value.astype(BF16)
    rest = value - high.astype(F32)
    middle = rest.astype(BF16)
    return high, middle, (rest - middle.astype(F32)).astype(BF16)


def standing(row, count):
    square = (count, row.shape[1])
    same = lax.broadcasted_iota(jnp.int32, square, 0) == lax.broadcasted_iota(jnp.int32, square, 1)
    return jnp.sum(jnp.where(same, row, 0.0), axis=1, keepdims=True)


def lying(col, width):
    square = (col.shape[0], width)
    same = lax.broadcasted_iota(jnp.int32, square, 0) == lax.broadcasted_iota(jnp.int32, square, 1)
    return jnp.sum(jnp.where(same, col, 0.0), axis=0, keepdims=True)


def layer_kernel(
    n_sp, n_tp, group, cap,
    operands, w_out, w_gate, w_up, w_down,
    out,
    held,
    gated, stack, facts, spread, find, told, heard, serve, merge, sx, rx, sz, rz,
    gu, wd, wo, partner, mixed, summed, mid, normed, block, rows, acc, hid, shares, result,
    zs, zr, xs, xb, zs2, zr2, column, branch,
    sa, ra, sb, rb,
    wsem, wrs, wrr, gsem, sums, gr, xrs, xbs, szs, szr, osem, done, came,
):
    at = Place(n_sp, n_tp, group)
    X, Y, Z, C = at.X, at.Y, at.Z, at.C
    x, y, z, c = at.x, at.y, at.z, at.c
    steps = Y // 2
    other = 1 - c

    (
        q_t, k_t, values, gate_rows, decay_t, bias, extra, head_gain,
        residual, attention_gain, before_gain, after_gain, ids_row, weights_row,
    ) = held
    loads = [pltpu.make_async_copy(a, b, osem.at[k]) for k, (a, b) in enumerate(zip(operands, held))]
    for k in loads:
        k.start()
    local = [
        pltpu.make_async_copy(w_gate, gu.at[0], wsem.at[0]),
        pltpu.make_async_copy(w_up, gu.at[1], wsem.at[1]),
        pltpu.make_async_copy(w_down, wd.at[0], wsem.at[2]),
        pltpu.make_async_copy(w_out, wo.at[0], wsem.at[3]),
    ]
    rz[...] = jnp.zeros_like(rz)
    barrier = pltpu.get_barrier_semaphore()

    def greet_tp(k, carry):
        pl.semaphore_signal(barrier, inc=1, device_id=(at.sp, (at.tp + k) % n_tp), device_id_type=MESH)
        return carry

    lax.fori_loop(1, n_tp, greet_tp, 0)
    for k in range(1, Z):
        pl.semaphore_signal(barrier, inc=1, device_id=at.at(z=(z + k) % Z), device_id_type=MESH)
    for k in range(1, X):
        for core in range(C):
            pl.semaphore_signal(barrier, inc=1, device_id=at.at(x=(x + k) % X, c=core), device_id_type=MESH)

    for k in (3, 0, 1, 2):
        local[k].start()
    for k in loads:
        k.wait()

    tokens = q_t.shape[1]
    blocks = tokens // BLOCK
    pre = decay_t[...].astype(F32) + standing(bias[...], KEY_CHANNELS)
    log_decay = -(jnp.maximum(-pre, 0.0) + jnp.log1p(jnp.exp(-jnp.abs(pre)))) / DECAY_NORMALIZER + extra[...]
    r, q = (lax.broadcasted_iota(jnp.int32, (tokens, tokens), k) for k in (0, 1))
    one_block = (r // BLOCK) == (q // BLOCK)
    upto = jnp.where((r <= q) & one_block, 1.0, 0.0).astype(BF16)
    inside = sum(dot(term, upto) for term in split(log_decay))
    ends = [inside[:, (b + 1) * BLOCK - 1 : (b + 1) * BLOCK] for b in range(blocks)]
    of_block = lax.broadcasted_iota(jnp.int32, (KEY_CHANNELS, tokens), 1) // BLOCK
    keys = k_t[...].astype(F32)
    to_end = [jnp.where(of_block == b, keys * jnp.exp(jnp.minimum(ends[b] - inside, 0.0)), 0.0) for b in range(blocks)]
    vals = values[...]
    growth = dot(jnp.concatenate(to_end, axis=0).astype(BF16), vals)
    growth = [growth[b * KEY_CHANNELS : (b + 1) * KEY_CHANNELS] for b in range(blocks)]
    fades = [jnp.exp(e) for e in ends]
    state = growth[0]
    for b in range(1, blocks):
        state = fades[b] * state + growth[b]
    fade_row = lying(jnp.exp(sum(ends)), DV)
    tail = KEY_CHANNELS + 16

    def message(ref, state_part, row):
        ref[0:KEY_CHANNELS, :] = state_part.astype(BF16)
        ref[KEY_CHANNELS:tail, :] = jnp.broadcast_to(row, (16, DV)).astype(BF16)

    message(sx, state, fade_row)
    pl.semaphore_wait(barrier, n_tp - 1 + Z - 1 + (X - 1) * C)

    def state_x(k):
        return remote(sx, rx.at[x], done.at[7], came.at[4], at.at(x=(x + k) % X))

    for k in range(1, X):
        state_x(k).start()
    pair = at.at(c=other)
    crossed = [
        remote(w_out, wo.at[1], wrs.at[3], wrr.at[3], pair),
        remote(w_gate, gu.at[2], wrs.at[0], wrr.at[0], pair),
        remote(w_up, gu.at[3], wrs.at[1], wrr.at[1], pair),
        remote(w_down, wd.at[1], wrs.at[2], wrr.at[2], pair),
    ]
    for k in crossed:
        k.start()
    rx[pl.ds(x, 1)] = sx[...].reshape(1, tail, DV)

    slots = n_sp * cap
    seats = zs.shape[1]
    sub = lax.broadcasted_iota(jnp.int32, (n_sp, tokens), 0)
    chosen = [ids_row[k : k + 1, :] for k in range(TOP)]
    named = jnp.where((sub == chosen[0]) | (sub == chosen[1]), 1.0, 0.0).astype(BF16)
    before = dot(named, jnp.where(r < q, 1.0, 0.0).astype(BF16))
    targets = []
    plane_of = chosen[0] // X
    for e in chosen:
        slot = jnp.sum(jnp.where(sub == e, before, 0.0), axis=0, keepdims=True)
        targets.append((e - plane_of * X) * (Z * cap) + z * cap + slot.astype(jnp.int32))
    sub = lax.broadcasted_iota(jnp.int32, (Z, tokens), 0)
    before = dot(jnp.where(sub == plane_of, 1.0, 0.0).astype(BF16), jnp.where(r < q, 1.0, 0.0).astype(BF16))
    rank = jnp.sum(jnp.where(sub == plane_of, before, 0.0), axis=0, keepdims=True)
    seat = plane_of * seats + rank.astype(jnp.int32)
    query = q_t[...].astype(F32) * (KEY_CHANNELS**-0.5 * jnp.exp(inside))
    stack[0:KEY_CHANNELS, :] = query
    stack[KEY_CHANNELS:, :] = jnp.zeros((stack.shape[0] - KEY_CHANNELS, tokens), F32)
    stack[KEY_CHANNELS : KEY_CHANNELS + 1, :] = seat.astype(F32)
    facts[...] = jnp.zeros_like(facts)
    for k in range(TOP):
        facts[k : k + 1, :] = (targets[k] + 1).astype(F32)
        facts[TOP + k : TOP + k + 1, :] = weights_row[k : k + 1, :]
    stood = stack[...].T
    query = stood[:, 0:KEY_CHANNELS].astype(BF16)
    seat_col = stood[:, KEY_CHANNELS : KEY_CHANNELS + 1].astype(jnp.int32)
    scores = dot(query, (keys * jnp.exp(-inside)).astype(BF16))
    scores = jnp.where((r >= q) & one_block, scores, 0.0).astype(BF16)
    within = dot(scores, vals)

    whole(rx.at[pl.ds(0, X - 1)], came.at[4]).wait()
    plane, plane_row = rx[0, 0:KEY_CHANNELS].astype(F32), rx[0, KEY_CHANNELS:tail][0:1].astype(F32)
    ahead, ahead_fade = jnp.zeros_like(state), jnp.ones((KEY_CHANNELS, 1), F32)
    for k in range(X):
        part, row = rx[k, 0:KEY_CHANNELS].astype(F32), rx[k, KEY_CHANNELS:tail][0:1].astype(F32)
        fade = standing(row, KEY_CHANNELS)
        ahead = jnp.where(k < x, fade * ahead + part, ahead)
        ahead_fade = jnp.where(k < x, fade * ahead_fade, ahead_fade)
        if k:
            plane, plane_row = fade * plane + part, plane_row * row
    message(sz, plane, plane_row)

    def state_z(k):
        return remote(sz, rz.at[z], szs.at[k], szr.at[k], at.at(z=(z + k) % Z))

    for k in range(1, Z):

        @pl.when(z + k < Z)
        def _(k=k):
            state_z(k).start()

    all_seats = Z * seats
    tall = lax.broadcasted_iota(jnp.int32, (all_seats, tokens), 0)
    spread[...] = jnp.where(tall == seat, 1.0, 0.0).astype(BF16)
    wide = lax.broadcasted_iota(jnp.int32, (tokens, all_seats), 1)
    find[...] = jnp.where(wide == seat_col, 1.0, 0.0).astype(BF16)
    listed = sum(dot(term, find[...]) for term in split(facts[...]))
    near = lax.broadcasted_iota(jnp.int32, (8, DV), 1) < seats
    for k in range(Z):
        moved = pltpu.roll(listed, (all_seats - k * seats) % all_seats, 1) if k else listed
        told[k] = jnp.where(near, moved[:, 0:DV], 0.0)

    def tell(k):
        return remote(told.at[(z + k) % Z], heard.at[z], done.at[10], came.at[6], at.at(z=(z + k) % Z))

    for k in far_first(Z):
        tell(k).start()
    heard[pl.ds(z, 1)] = told[pl.ds(z, 1)]
    gate_act = gate_rows[...].astype(F32)
    gate_act = gate_act * jax.nn.sigmoid(gate_act) * head_gain[...]

    for k in range(1, Z):

        @pl.when(z >= k)
        def _(k=k):
            state_z(k).wait_recv()

    carried = jnp.zeros_like(state)
    for k in range(Z - 1):
        fade = standing(rz[k, KEY_CHANNELS:tail][0:1].astype(F32), KEY_CHANNELS)
        carried = jnp.where(k < z, fade * carried + rz[k, 0:KEY_CHANNELS].astype(F32), carried)
    running = ahead_fade * carried + ahead
    across = []
    for b in range(blocks):
        across.append(dot(query[b * BLOCK : (b + 1) * BLOCK], running.astype(BF16)))
        running = fades[b] * running + growth[b]
    heads = within + jnp.concatenate(across, axis=0)
    heads = heads * lax.rsqrt(jnp.mean(heads * heads, axis=1, keepdims=True) + EPSILON) * gate_act
    gated[...] = heads.astype(BF16).reshape(gated.shape)
    lead = c == C - 1
    swap = remote(gated, partner, gsem.at[0], gsem.at[1], pair)

    @pl.when(jnp.logical_not(lead))
    def _():
        swap.start()


    piece = gated.shape[2]
    width = wo.shape[2]
    local[3].wait()
    crossed[0].wait_recv()
    part_width = width // PARTS
    handed = remote(summed.at[0], summed.at[0], gsem.at[2], gsem.at[3], pair)

    def mixed_part(k, part):
        d = (y + k + Y) % Y
        return mixed[pl.ds(d, 1), :, part * part_width : (part + 1) * part_width].reshape(C * piece, part_width)

    def keep(part, value):
        summed[:, :, part * part_width : (part + 1) * part_width] = value.reshape(C, piece, part_width)

    @pl.when(lead)
    def _():
        swap.wait_recv()
        mine = gated[...].reshape(tokens, DV)
        theirs = partner[...].reshape(tokens, DV)
        for k in range(PARTS):
            cols = slice(k * part_width, (k + 1) * part_width)
            value = dot(mine, wo[0, :, cols]) + dot(theirs, wo[1, :, cols])
            mixed[:, :, cols] = value.reshape(Y, C * piece, part_width)
        ring_sum(at, mixed_part, keep, sa, ra, done.at[0], sums)
        handed.start()

    @pl.when(jnp.logical_not(lead))
    def _():
        handed.wait_recv()

    attn = summed[pl.ds(c, 1)].reshape(piece, width)
    attn = attn * lax.rsqrt(jnp.mean(attn * attn, axis=1, keepdims=True) + EPSILON) * attention_gain[...]
    mid[...] = (residual[...].astype(F32) + attn).astype(BF16)
    m = mid[...].astype(F32)
    m = m * lax.rsqrt(jnp.mean(m * m, axis=1, keepdims=True) + EPSILON) * before_gain[...]
    normed[...] = m.astype(BF16)

    def share_cols(t):
        return pl.ds(pl.multiple_of(t * DV, DV), DV)

    def share_rows(t):
        return pl.ds(pl.multiple_of(t * piece, piece), piece)

    def to_width(k):
        t = (at.tp + k) % n_tp
        return remote(
            normed.at[:, share_cols(t)], block.at[share_rows(at.tp), :], done.at[3], came.at[0], (at.sp, t)
        )

    def start_width(k, carry):
        to_width(k).start()
        return carry

    lax.fori_loop(1, n_tp, start_width, 0)
    block[share_rows(at.tp), :] = normed[:, share_cols(at.tp)]

    whole(heard.at[pl.ds(0, Z - 1)], came.at[6]).wait()
    lists = None
    for k in range(Z):
        part = jnp.concatenate([heard[k], jnp.zeros((8, all_seats - DV), F32)], axis=1)
        part = pltpu.roll(part, k * seats, 1) if k else part
        lists = part if lists is None else lists + part
    tall = lax.broadcasted_iota(jnp.int32, (slots, all_seats), 0)
    hits = [jnp.where(tall == lists[k : k + 1, :].astype(jnp.int32) - 1, 1.0, 0.0) for k in range(TOP)]
    serve[...] = (hits[0] + hits[1]).astype(BF16)
    stood = jnp.concatenate([lists, jnp.zeros((DV - 8, all_seats), F32)], axis=0).T
    wide = lax.broadcasted_iota(jnp.int32, (all_seats, slots), 1)
    for k in range(TOP):
        merge[k] = jnp.where(wide == stood[:, k : k + 1].astype(jnp.int32) - 1, 1.0, 0.0).astype(BF16)
    shares_of = [stood[:, TOP + k : TOP + k + 1] for k in range(TOP)]
    others = block.at[pl.ds(0, (n_tp - 1) * piece)]
    whole(others, came.at[0]).wait()
    picked = dot(spread[...], block[...]).astype(BF16)
    zs[...] = picked.reshape(zs.shape)

    def z_out(k):
        return remote(zs.at[(z + k) % Z], zr.at[z], done.at[5], came.at[2], at.at(z=(z + k) % Z))

    for k in far_first(Z):
        z_out(k).start()
    zr[pl.ds(z, 1)] = zs[pl.ds(z, 1)]
    whole(zr.at[pl.ds(0, Z - 1)], came.at[2]).wait()

    xs[...] = dot(serve[...], zr[...].reshape(all_seats, DV)).astype(BF16).reshape(xs.shape)

    side = x % C
    mine_half = x // C
    per = PARTS // 2

    def x_out(k):
        to = (x + k) % X
        return (
            xs.at[to],
            rows.at[y, pl.ds(mine_half * per, per), :, share_cols(c)],
            done.at[8 if k else 9],
            xrs.at[mine_half],
            at.at(x=to, c=side),
        )

    for k in range(1, X):
        remote(*x_out(k)).start()
    src, dst, s_sem, r_sem, to = x_out(0)

    @pl.when(side == c)
    def _():
        pltpu.make_async_copy(src, dst, r_sem).start()

    @pl.when(side != c)
    def _():
        remote(src, dst, s_sem, r_sem, pair).start()

    def gather(way, step, part):
        j = (y + Y - (step - 1)) % Y if way == 0 else (y + step - 1) % Y
        to = (y + 1) % Y if way == 0 else (y + Y - 1) % Y
        i = way * ring_size(steps) + (step - 1) * PARTS + (part if step < steps else part % per)
        return remote(rows.at[j, part], rows.at[j, part], done.at[2], gr.at[i], at.at(y=to))

    def start_gather(way, step, part):
        gather(way, step, part).start()

    for half in (0, 1):
        whole(rows.at[y, pl.ds(half * per, per)], xrs.at[half]).wait()
        for part in range(half * per, half * per + per):
            for way in (0, 1):
                start_gather(way, 1, part)

    count = rows.shape[1] * rows.shape[2]
    chunk = rows.shape[3]
    local[0].wait()
    local[1].wait()
    crossed[1].wait_recv()
    crossed[2].wait_recv()

    def grow(j, first=False):
        a = rows[pl.ds(j, 1)].reshape(count, chunk)
        at_rows = pl.ds(pl.multiple_of(j * chunk, chunk), chunk)
        for k in range(4):
            value = dot(a, gu[k, at_rows, :])
            acc[k] = value if first else acc[k] + value

    grow(y, True)
    for step in range(1, steps):
        for part in range(PARTS):
            for way in (0, 1):
                gather(way, step, part).wait_recv()
                if step + 1 < steps or way == part // per:
                    start_gather(way, step + 1, part)
        grow((y + Y - step) % Y)
        grow((y + step) % Y)
    for part in range(PARTS):
        gather(part // per, steps, part).wait_recv()
    grow((y + steps) % Y)

    for k in (0, 1):
        gate, up = acc[2 * k], acc[2 * k + 1]
        hid[k] = (gate * jax.nn.sigmoid(gate) * up).astype(BF16)

    local[2].wait()
    crossed[3].wait_recv()
    made = {}

    def down(offset):
        d = (y + offset + Y) % Y
        cols = pl.ds(pl.multiple_of(d * chunk, chunk), chunk)
        value = dot(hid[0], wd[0, :, cols]) + dot(hid[1], wd[1, :, cols])
        shares[offset + steps - 1] = value.reshape(PARTS, count // PARTS, chunk)

    def down_part(offset, part):
        if offset not in made:
            down(offset)
            made[offset] = True
        return shares[offset + steps - 1, part]

    def x_back(half, core):
        home = 2 * half + c
        return (
            result.at[pl.ds(half * per, per), :, pl.ds(core * DV, DV)],
            xb.at[x],
            xbs.at[2 * half + core],
            came.at[5],
            at.at(x=home, c=core),
        ), (home == x) & (c == core)

    def keep_result(part, value):
        result[part] = value.astype(BF16)
        if part % per < per - 1:
            return
        for core in range(C):
            args, here = x_back(part // per, core)

            @pl.when(here)
            def _(args=args):
                pltpu.make_async_copy(args[0], args[1], args[3]).start()

            @pl.when(jnp.logical_not(here))
            def _(args=args):
                remote(*args).start()

    ring_sum(at, down_part, keep_result, sb, rb, done.at[1], sums)

    whole(xb, came.at[5]).wait()
    served = xb[...].reshape(slots, DV)
    served = shares_of[0] * dot(merge[0], served) + shares_of[1] * dot(merge[1], served)
    zs2[...] = served.astype(BF16).reshape(zs2.shape)

    def z_back(k):
        return remote(zs2.at[(z + k) % Z], zr2.at[z], done.at[6], came.at[3], at.at(z=(z + k) % Z))

    for k in far_first(Z):
        z_back(k).start()
    zr2[pl.ds(z, 1)] = zs2[pl.ds(z, 1)]
    whole(zr2.at[pl.ds(0, Z - 1)], came.at[3]).wait()
    column[...] = dot(find[...], zr2[...].reshape(all_seats, DV)).astype(BF16)

    def to_rows(k):
        t = (at.tp + k) % n_tp
        return remote(
            column.at[share_rows(t), :], branch.at[:, share_cols(at.tp)], done.at[4], came.at[1], (at.sp, t)
        )

    def start_rows(k, carry):
        to_rows(k).start()
        return carry

    lax.fori_loop(1, n_tp, start_rows, 0)
    branch[:, share_cols(at.tp)] = column[share_rows(at.tp), :]
    whole(others, came.at[1]).wait()
    b = branch[...].astype(F32)
    b = b * lax.rsqrt(jnp.mean(b * b, axis=1, keepdims=True) + EPSILON) * after_gain[...]
    out[...] = (mid[...].astype(F32) + b).astype(BF16)

    whole(rx.at[pl.ds(0, X - 1)], done.at[7]).wait()
    for k in range(1, Z):

        @pl.when(z + k < Z)
        def _(k=k):
            state_z(k).wait_send()

    @pl.when(jnp.logical_not(lead))
    def _():
        swap.wait_send()

    @pl.when(lead)
    def _():
        handed.wait_send()
        whole(sa, done.at[0]).wait()

    for k in crossed:
        k.wait_send()
    whole(sb, done.at[1]).wait()
    whole(rows.at[pl.ds(0, Y - 1)], done.at[2]).wait()
    whole(others, done.at[3]).wait()
    whole(others, done.at[4]).wait()
    whole(zr.at[pl.ds(0, Z - 1)], done.at[5]).wait()
    whole(told.at[pl.ds(0, Z - 1)], done.at[10]).wait()
    whole(zr2.at[pl.ds(0, Z - 1)], done.at[6]).wait()
    whole(xs.at[pl.ds(0, X - 1)], done.at[8]).wait()

    @pl.when(side != c)
    def _():
        remote(src, dst, s_sem, r_sem, pair).wait_send()

    for half in (0, 1):
        for core in range(C):
            args, here = x_back(half, core)

            @pl.when(jnp.logical_not(here))
            def _(args=args):
                remote(*args).wait_send()


def shards(
    query, key, value, gate_rows, decay, bias, extra, head_gain, output_projection, residual,
    attention_gain, before_gain, after_gain, w_gate, w_up, w_down, ids, weights,
):
    n_sp, n_tp = lax.axis_size("sp"), lax.axis_size("tp")
    tokens, width = query.shape[0], residual.shape[1]
    piece = residual.shape[0]
    X, C = GROUP_SIZE, CORES
    Z, Y = n_sp // X, n_tp // C
    cap = 5 * tokens // (2 * n_sp)
    slots = n_sp * cap
    seats = -(-(X * cap // TOP) // 16) * 16
    steps = Y // 2
    msgs = 2 * ring_size(steps)
    part = slots // C // PARTS
    chunk = C * DV
    hidden = w_gate.shape[2]
    hbm = pl.BlockSpec(memory_space=pltpu.HBM)
    sem = pltpu.SemaphoreType.DMA
    message = (KEY_CHANNELS + 16, DV)
    operands = [
        query.T, key.T, value, gate_rows, decay.T, bias[None], extra.T, head_gain[None],
        residual, attention_gain[None], before_gain[None], after_gain[None], ids.T, weights.T,
    ]
    scratch = [
        [pltpu.VMEM(a.shape, a.dtype) for a in operands],
        pltpu.VMEM((Y, C, piece, DV), BF16),
        pltpu.VMEM((128, tokens), F32),
        pltpu.VMEM((8, tokens), F32),
        pltpu.VMEM((Z * seats, tokens), BF16),
        pltpu.VMEM((tokens, Z * seats), BF16),
        pltpu.VMEM((Z, 8, DV), F32),
        pltpu.VMEM((Z, 8, DV), F32),
        pltpu.VMEM((slots, Z * seats), BF16),
        pltpu.VMEM((TOP, Z * seats, slots), BF16),
        pltpu.VMEM(message, BF16),
        pltpu.VMEM((X, *message), BF16),
        pltpu.VMEM(message, BF16),
        pltpu.VMEM((Z, *message), BF16),
        pltpu.VMEM((4, width, hidden), BF16),
        pltpu.VMEM((2, hidden, width), BF16),
        pltpu.VMEM((2, DV, width), BF16),
        pltpu.VMEM((Y, C, piece, DV), BF16),
        pltpu.VMEM((Y, C * piece, width), F32),
        pltpu.VMEM((C, piece, width), F32),
        pltpu.VMEM((piece, width), BF16),
        pltpu.VMEM((piece, width), BF16),
        pltpu.VMEM((tokens, DV), BF16),
        pltpu.VMEM((Y, PARTS, part, chunk), BF16),
        pltpu.VMEM((4, PARTS * part, hidden), F32),
        pltpu.VMEM((2, PARTS * part, hidden), BF16),
        pltpu.VMEM((Y, PARTS, part, chunk), F32),
        pltpu.VMEM((PARTS, part, chunk), BF16),
        pltpu.VMEM((Z, seats, DV), BF16),
        pltpu.VMEM((Z, seats, DV), BF16),
        pltpu.VMEM((X, PARTS // 2, part, DV), BF16),
        pltpu.VMEM((X, PARTS // 2, part, DV), BF16),
        pltpu.VMEM((Z, seats, DV), BF16),
        pltpu.VMEM((Z, seats, DV), BF16),
        pltpu.VMEM((tokens, DV), BF16),
        pltpu.VMEM((piece, width), BF16),
        pltpu.VMEM((msgs, C * piece, width // PARTS), BF16),
        pltpu.VMEM((msgs, C * piece, width // PARTS), BF16),
        pltpu.VMEM((msgs, part, chunk), BF16),
        pltpu.VMEM((msgs, part, chunk), BF16),
        sem((4,)), sem((4,)), sem((4,)), sem((4,)), sem((msgs,)), sem((msgs,)), sem((2,)), sem((2 * C,)),
        sem((Z,)), sem((Z,)), sem((len(operands),)), sem((11,)), sem((7,)),
    ]
    return pl.pallas_call(
        functools.partial(layer_kernel, n_sp, n_tp, X, cap),
        out_shape=jax.ShapeDtypeStruct((piece, width), BF16),
        in_specs=[[hbm] * len(operands), hbm, hbm, hbm, hbm],
        out_specs=pl.BlockSpec(memory_space=pltpu.VMEM),
        scratch_shapes=scratch,
        name="layer",
        compiler_params=pltpu.CompilerParams(
            collective_id=0, has_side_effects=True, vmem_limit_bytes=40 * 1024 * 1024
        ),
    )(
        *jax.tree.map(lambda a: pltpu.with_memory_space_constraint(a, pltpu.HBM), (operands, output_projection, w_gate[0], w_up[0], w_down[0]))
    )


def solution(mesh):
    placed = (
        P("sp", "tp"),
        P("sp", "tp"),
        P("sp", "tp"),
        P("sp", "tp"),
        P("sp", "tp"),
        P("tp"),
        P("sp", "tp"),
        P(),
        P("tp", None),
        P(("sp", "tp"), None),
        P(),
        P(),
        P(),
        P("sp", None, "tp"),
        P("sp", None, "tp"),
        P("sp", "tp", None),
        P("sp", None),
        P("sp", None),
    )
    return jax.shard_map(
        shards, mesh=mesh, in_specs=placed, out_specs=P(("sp", "tp"), None), check_vma=False
    )
```

```python
import functools

import jax
import jax.numpy as jnp
from jax import lax
from jax.experimental import pallas as pl
from jax.experimental.pallas import tpu as pltpu
from jax.sharding import PartitionSpec as P

KEY_CHANNELS = 64
DV = 128
TOP = 2
BLOCK = 64
GROUP_SIZE = 4
CORES = 2

EPSILON = 1e-06
DECAY_NORMALIZER = 16.0
MESH = pl.DeviceIdType.MESH
BF16 = jnp.bfloat16
F32 = jnp.float32
PARTS = 4


def dot(a, b):
    return jnp.dot(a, b, preferred_element_type=F32)


class Place:
    def __init__(self, n_sp, n_tp, group):
        self.X, self.Z = group, n_sp // group
        self.C, self.Y = CORES, n_tp // CORES
        self.n_tp = n_tp
        self.sp, self.tp = lax.axis_index("sp"), lax.axis_index("tp")
        self.z, self.x = self.sp // self.X, self.sp % self.X
        self.y, self.c = self.tp // self.C, self.tp % self.C

    def at(self, z=None, x=None, y=None, c=None):
        z = self.z if z is None else z
        x = self.x if x is None else x
        y = self.y if y is None else y
        c = self.c if c is None else c
        return (z * self.X + x, y * self.C + c)


def remote(src, dst, send, recv, to):
    return pltpu.make_async_remote_copy(
        src_ref=src, dst_ref=dst, send_sem=send, recv_sem=recv, device_id=to, device_id_type=MESH
    )


def ring_index(way, step, part, steps):
    first = part % (PARTS // 2) if step == 1 else PARTS // 2 + (step - 2) * PARTS + part
    return way * ring_size(steps) + first


def ring_size(steps):
    return PARTS // 2 + (steps - 1) * PARTS


def way_parts(way):
    low, high = list(range(PARTS // 2)), list(range(PARTS // 2, PARTS))
    return (low, high) if way == 0 else (high, low)


def both_ways(pick):
    return [(way, part) for pair in zip(pick(0), pick(1)) for way, part in enumerate(pair)]


def whole(ref, sem):
    return pltpu.make_async_copy(ref, ref, sem)


def ring_sum(at, part_of, out, sends, recvs, send_sem, recv_sems):
    Y, steps, y = at.Y, at.Y // 2, at.y

    def copy(way, step, part):
        i = ring_index(way, step, part, steps)
        to = (y + 1) % Y if way == 0 else (y + Y - 1) % Y
        return remote(sends.at[i], recvs.at[i], send_sem, recv_sems.at[i], at.at(y=to))

    def offset(way, step):
        k = steps - step + 1
        return k if way == 0 or k == steps else -k

    def send(way, step, part, value):
        sends[ring_index(way, step, part, steps)] = value.astype(BF16)
        copy(way, step, part).start()

    for way, part in both_ways(lambda w: way_parts(w)[0]):
        send(way, 1, part, part_of(offset(way, 1), part))
    for step in range(2, steps + 1):
        for way, part in both_ways(lambda w: way_parts(w)[1] + way_parts(w)[0]):
            value = part_of(offset(way, step), part)
            if step > 2 or part in way_parts(way)[0]:
                copy(way, step - 1, part).wait_recv()
                value = value + recvs[ring_index(way, step - 1, part, steps)].astype(F32)
            send(way, step, part, value)
    for part in range(PARTS):
        total = part_of(0, part)
        for way in (0, 1):
            copy(way, steps, part).wait_recv()
            total = total + recvs[ring_index(way, steps, part, steps)].astype(F32)
        out(part, total)


def relay_sum(at, prepare, part_of, out, sends, recvs, send_sem, recv_sems):
    Y, y = at.Y, at.y
    hops = (2, 1, 2, 1)
    starts = (0, PARTS // 2, PARTS // 2 + PARTS, PARTS // 2 + 2 * PARTS)

    def slot(way, kind, part):
        return way * ring_size(Y // 2) + starts[kind] + (part % (PARTS // 2) if kind == 0 else part)

    def copy(way, kind, part):
        i = slot(way, kind, part)
        to = (y + hops[kind]) % Y if way == 0 else (y + Y - hops[kind]) % Y
        return remote(sends.at[i], recvs.at[i], send_sem, recv_sems.at[i], at.at(y=to))

    def send(way, kind, part, value):
        sends[slot(way, kind, part)] = value.astype(BF16)
        copy(way, kind, part).start()

    def received(way, kind, part):
        copy(way, kind, part).wait_recv()
        return recvs[slot(way, kind, part)].astype(F32)

    def own(way, k, part):
        return part_of(k if way == 0 or k == Y // 2 else -k, part)

    def direct(part):
        for way in (0, 1):
            send(way, 3, part, own(way, 1, part))

    for pair in zip(way_parts(0)[0], way_parts(1)[0]):
        for part in pair:
            prepare(part)
            for way in (0, 1):
                if part in way_parts(way)[0]:
                    send(way, 0, part, own(way, Y // 2, part))
                send(way, 1, part, own(way, 3, part))
    early = way_parts(0)[0]
    for part in early:
        direct(part)
    for way, part in both_ways(lambda w: way_parts(w)[1] + way_parts(w)[0]):
        value = own(way, 2, part) + received(way, 1, part)
        if part in way_parts(way)[0]:
            value = value + received(way, 0, part)
        send(way, 2, part, value)
    for part in range(PARTS):
        if part not in early:
            direct(part)
    for part in range(PARTS):
        total = part_of(0, part)
        for way in (0, 1):
            total = total + received(way, 3, part) + received(way, 2, part)
        out(part, total)


def far_first(count):
    return sorted(range(1, count), key=lambda k: (-min(k, count - k), k))


def near_order(count):
    return sorted(range(count), key=lambda k: (min(k, count - k), k))


def split(value):
    high = value.astype(BF16)
    rest = value - high.astype(F32)
    middle = rest.astype(BF16)
    return high, middle, (rest - middle.astype(F32)).astype(BF16)


def standing(row, count):
    square = (count, row.shape[1])
    same = lax.broadcasted_iota(jnp.int32, square, 0) == lax.broadcasted_iota(jnp.int32, square, 1)
    return jnp.sum(jnp.where(same, row, 0.0), axis=1, keepdims=True)


def lying(col, width):
    square = (col.shape[0], width)
    same = lax.broadcasted_iota(jnp.int32, square, 0) == lax.broadcasted_iota(jnp.int32, square, 1)
    return jnp.sum(jnp.where(same, col, 0.0), axis=0, keepdims=True)


def layer_kernel(
    n_sp, n_tp, group, cap,
    operands, w_out, w_gate, w_up, w_down,
    out,
    held,
    gated, stack, facts, spread, find, told, heard, serve, merge, sx, rx, sz, rz,
    gu, wd, wo, partner, mixed, summed, mid, normed, block, rows, acc, hid, shares, result,
    zs, zr, xs, xb, zs2, zr2, column, branch,
    sa, ra, sb, rb,
    wsem, wrs, wrr, gsem, sums, gr, xrs, xbs, szs, szr, osem, done, came,
):
    at = Place(n_sp, n_tp, group)
    X, Y, Z, C = at.X, at.Y, at.Z, at.C
    x, y, z, c = at.x, at.y, at.z, at.c
    steps = Y // 2
    other = 1 - c

    (
        q_t, k_t, values, gate_rows, decay_t, bias, extra, head_gain,
        residual, attention_gain, before_gain, after_gain, ids_row, weights_row,
    ) = held
    loads = [pltpu.make_async_copy(a, b, osem.at[k]) for k, (a, b) in enumerate(zip(operands, held))]
    for k in loads:
        k.start()
    local = [
        pltpu.make_async_copy(w_gate, gu.at[0], wsem.at[0]),
        pltpu.make_async_copy(w_up, gu.at[1], wsem.at[1]),
        pltpu.make_async_copy(w_down, wd.at[0], wsem.at[2]),
        pltpu.make_async_copy(w_out, wo.at[0], wsem.at[3]),
    ]
    rz[...] = jnp.zeros_like(rz)
    barrier = pltpu.get_barrier_semaphore()

    def greet_tp(k, carry):
        pl.semaphore_signal(barrier, inc=1, device_id=(at.sp, (at.tp + k) % n_tp), device_id_type=MESH)
        return carry

    lax.fori_loop(1, n_tp, greet_tp, 0)
    for k in range(1, Z):
        pl.semaphore_signal(barrier, inc=1, device_id=at.at(z=(z + k) % Z), device_id_type=MESH)
    for k in range(1, X):
        for core in range(C):
            pl.semaphore_signal(barrier, inc=1, device_id=at.at(x=(x + k) % X, c=core), device_id_type=MESH)

    for k in (3, 0, 1, 2):
        local[k].start()
    for k in loads:
        k.wait()

    tokens = q_t.shape[1]
    blocks = tokens // BLOCK
    pre = decay_t[...].astype(F32) + standing(bias[...], KEY_CHANNELS)
    log_decay = -(jnp.maximum(-pre, 0.0) + jnp.log1p(jnp.exp(-jnp.abs(pre)))) / DECAY_NORMALIZER + extra[...]
    r, q = (lax.broadcasted_iota(jnp.int32, (tokens, tokens), k) for k in (0, 1))
    one_block = (r // BLOCK) == (q // BLOCK)
    upto = jnp.where((r <= q) & one_block, 1.0, 0.0).astype(BF16)
    inside = sum(dot(term, upto) for term in split(log_decay))
    ends = [inside[:, (b + 1) * BLOCK - 1 : (b + 1) * BLOCK] for b in range(blocks)]
    of_block = lax.broadcasted_iota(jnp.int32, (KEY_CHANNELS, tokens), 1) // BLOCK
    keys = k_t[...].astype(F32)
    to_end = [jnp.where(of_block == b, keys * jnp.exp(jnp.minimum(ends[b] - inside, 0.0)), 0.0) for b in range(blocks)]
    vals = values[...]
    growth = dot(jnp.concatenate(to_end, axis=0).astype(BF16), vals)
    growth = [growth[b * KEY_CHANNELS : (b + 1) * KEY_CHANNELS] for b in range(blocks)]
    fades = [jnp.exp(e) for e in ends]
    state = growth[0]
    for b in range(1, blocks):
        state = fades[b] * state + growth[b]
    fade_row = lying(jnp.exp(sum(ends)), DV)
    tail = KEY_CHANNELS + 16

    def message(ref, state_part, row):
        ref[0:KEY_CHANNELS, :] = state_part.astype(BF16)
        ref[KEY_CHANNELS:tail, :] = jnp.broadcast_to(row, (16, DV)).astype(BF16)

    message(sx, state, fade_row)
    pl.semaphore_wait(barrier, n_tp - 1 + Z - 1 + (X - 1) * C)

    def state_x(k):
        return remote(sx, rx.at[x], done.at[7], came.at[4], at.at(x=(x + k) % X))

    for k in range(1, X):
        state_x(k).start()
    pair = at.at(c=other)
    crossed = [
        remote(w_out, wo.at[1], wrs.at[3], wrr.at[3], pair),
        remote(w_gate, gu.at[2], wrs.at[0], wrr.at[0], pair),
        remote(w_up, gu.at[3], wrs.at[1], wrr.at[1], pair),
        remote(w_down, wd.at[1], wrs.at[2], wrr.at[2], pair),
    ]
    for k in crossed:
        k.start()
    rx[pl.ds(x, 1)] = sx[...].reshape(1, tail, DV)

    slots = n_sp * cap
    seats = zs.shape[1]
    sub = lax.broadcasted_iota(jnp.int32, (n_sp, tokens), 0)
    chosen = [ids_row[k : k + 1, :] for k in range(TOP)]
    named = jnp.where((sub == chosen[0]) | (sub == chosen[1]), 1.0, 0.0).astype(BF16)
    before = dot(named, jnp.where(r < q, 1.0, 0.0).astype(BF16))
    targets = []
    plane_of = chosen[0] // X
    order = near_order(Z)
    group_size = Z // 2
    away = z - plane_of
    away = jnp.where(away < 0, away + Z, away)
    base = jnp.zeros_like(away)
    for i, k in enumerate(order):
        start = (i // group_size) * (X * group_size * cap) + (i % group_size) * cap
        base = jnp.where(away == k, start, base)
    for e in chosen:
        slot = jnp.sum(jnp.where(sub == e, before, 0.0), axis=0, keepdims=True)
        targets.append((e - plane_of * X) * (group_size * cap) + base + slot.astype(jnp.int32))
    sub = lax.broadcasted_iota(jnp.int32, (Z, tokens), 0)
    before = dot(jnp.where(sub == plane_of, 1.0, 0.0).astype(BF16), jnp.where(r < q, 1.0, 0.0).astype(BF16))
    rank = jnp.sum(jnp.where(sub == plane_of, before, 0.0), axis=0, keepdims=True)
    seat = plane_of * seats + rank.astype(jnp.int32)
    query = q_t[...].astype(F32) * (KEY_CHANNELS**-0.5 * jnp.exp(inside))
    stack[0:KEY_CHANNELS, :] = query
    stack[KEY_CHANNELS:, :] = jnp.zeros((stack.shape[0] - KEY_CHANNELS, tokens), F32)
    stack[KEY_CHANNELS : KEY_CHANNELS + 1, :] = seat.astype(F32)
    facts[...] = jnp.zeros_like(facts)
    for k in range(TOP):
        facts[k : k + 1, :] = (targets[k] + 1).astype(F32)
        facts[TOP + k : TOP + k + 1, :] = weights_row[k : k + 1, :]
    stood = stack[...].T
    query = stood[:, 0:KEY_CHANNELS].astype(BF16)
    seat_col = stood[:, KEY_CHANNELS : KEY_CHANNELS + 1].astype(jnp.int32)
    scores = dot(query, (keys * jnp.exp(-inside)).astype(BF16))
    scores = jnp.where((r >= q) & one_block, scores, 0.0).astype(BF16)
    within = dot(scores, vals)

    whole(rx.at[pl.ds(0, X - 1)], came.at[4]).wait()
    plane, plane_row = rx[0, 0:KEY_CHANNELS].astype(F32), rx[0, KEY_CHANNELS:tail][0:1].astype(F32)
    ahead, ahead_fade = jnp.zeros_like(state), jnp.ones((KEY_CHANNELS, 1), F32)
    for k in range(X):
        part, row = rx[k, 0:KEY_CHANNELS].astype(F32), rx[k, KEY_CHANNELS:tail][0:1].astype(F32)
        fade = standing(row, KEY_CHANNELS)
        ahead = jnp.where(k < x, fade * ahead + part, ahead)
        ahead_fade = jnp.where(k < x, fade * ahead_fade, ahead_fade)
        if k:
            plane, plane_row = fade * plane + part, plane_row * row
    message(sz, plane, plane_row)

    def state_z(k):
        return remote(sz, rz.at[z], szs.at[k], szr.at[k], at.at(z=(z + k) % Z))

    for k in range(1, Z):

        @pl.when(z + k < Z)
        def _(k=k):
            state_z(k).start()

    all_seats = Z * seats
    tall = lax.broadcasted_iota(jnp.int32, (all_seats, tokens), 0)
    spread[...] = jnp.where(tall == seat, 1.0, 0.0).astype(BF16)
    wide = lax.broadcasted_iota(jnp.int32, (tokens, all_seats), 1)
    find[...] = jnp.where(wide == seat_col, 1.0, 0.0).astype(BF16)
    listed = sum(dot(term, find[...]) for term in split(facts[...]))
    near = lax.broadcasted_iota(jnp.int32, (8, DV), 1) < seats
    for k in range(Z):
        moved = pltpu.roll(listed, (all_seats - k * seats) % all_seats, 1) if k else listed
        told[k] = jnp.where(near, moved[:, 0:DV], 0.0)

    def tell(k):
        return remote(
            told.at[(z + k) % Z], heard.at[order.index(Z - k)], done.at[10], came.at[6], at.at(z=(z + k) % Z)
        )

    for k in far_first(Z):
        tell(k).start()
    heard[0:1] = told[pl.ds(z, 1)]
    gate_act = gate_rows[...].astype(F32)
    gate_act = gate_act * jax.nn.sigmoid(gate_act) * head_gain[...]

    for k in range(1, Z):

        @pl.when(z >= k)
        def _(k=k):
            state_z(k).wait_recv()

    carried = jnp.zeros_like(state)
    for k in range(Z - 1):
        fade = standing(rz[k, KEY_CHANNELS:tail][0:1].astype(F32), KEY_CHANNELS)
        carried = jnp.where(k < z, fade * carried + rz[k, 0:KEY_CHANNELS].astype(F32), carried)
    running = ahead_fade * carried + ahead
    across = []
    for b in range(blocks):
        across.append(dot(query[b * BLOCK : (b + 1) * BLOCK], running.astype(BF16)))
        running = fades[b] * running + growth[b]
    heads = within + jnp.concatenate(across, axis=0)
    heads = heads * lax.rsqrt(jnp.mean(heads * heads, axis=1, keepdims=True) + EPSILON) * gate_act
    gated[...] = heads.astype(BF16).reshape(gated.shape)
    lead = c == C - 1
    swap = remote(gated, partner, gsem.at[0], gsem.at[1], pair)

    @pl.when(jnp.logical_not(lead))
    def _():
        swap.start()


    piece = gated.shape[2]
    width = wo.shape[2]
    local[3].wait()
    crossed[0].wait_recv()
    part_width = width // PARTS
    handed = remote(summed.at[0], summed.at[0], gsem.at[2], gsem.at[3], pair)

    def mixed_part(k, part):
        d = (y + k + Y) % Y
        return mixed[pl.ds(d, 1), :, part * part_width : (part + 1) * part_width].reshape(C * piece, part_width)

    def keep(part, value):
        summed[:, :, part * part_width : (part + 1) * part_width] = value.reshape(C, piece, part_width)

    @pl.when(lead)
    def _():
        swap.wait_recv()
        mine = gated[...].reshape(tokens, DV)
        theirs = partner[...].reshape(tokens, DV)

        def prepare(part):
            cols = slice(part * part_width, (part + 1) * part_width)
            value = dot(mine, wo[0, :, cols]) + dot(theirs, wo[1, :, cols])
            mixed[:, :, cols] = value.reshape(Y, C * piece, part_width)

        relay_sum(at, prepare, mixed_part, keep, sa, ra, done.at[0], sums)
        handed.start()

    @pl.when(jnp.logical_not(lead))
    def _():
        handed.wait_recv()

    attn = summed[pl.ds(c, 1)].reshape(piece, width)
    attn = attn * lax.rsqrt(jnp.mean(attn * attn, axis=1, keepdims=True) + EPSILON) * attention_gain[...]
    mid[...] = (residual[...].astype(F32) + attn).astype(BF16)
    m = mid[...].astype(F32)
    m = m * lax.rsqrt(jnp.mean(m * m, axis=1, keepdims=True) + EPSILON) * before_gain[...]
    normed[...] = m.astype(BF16)

    def share_cols(t):
        return pl.ds(pl.multiple_of(t * DV, DV), DV)

    def share_rows(t):
        return pl.ds(pl.multiple_of(t * piece, piece), piece)

    def to_width(k):
        t = (at.tp + k) % n_tp
        return remote(
            normed.at[:, share_cols(t)], block.at[share_rows(at.tp), :], done.at[3], came.at[0], (at.sp, t)
        )

    def start_width(k, carry):
        to_width(k).start()
        return carry

    lax.fori_loop(1, n_tp, start_width, 0)
    block[share_rows(at.tp), :] = normed[:, share_cols(at.tp)]

    whole(heard.at[pl.ds(1, Z - 1)], came.at[6]).wait()
    lists = None
    for k in range(Z):
        part = jnp.concatenate([heard[k], jnp.zeros((8, all_seats - DV), F32)], axis=1)
        part = pltpu.roll(part, k * seats, 1) if k else part
        lists = part if lists is None else lists + part
    tall = lax.broadcasted_iota(jnp.int32, (slots, all_seats), 0)
    hits = [jnp.where(tall == lists[k : k + 1, :].astype(jnp.int32) - 1, 1.0, 0.0) for k in range(TOP)]
    serve[...] = (hits[0] + hits[1]).astype(BF16)
    stood = jnp.concatenate([lists, jnp.zeros((DV - 8, all_seats), F32)], axis=0).T
    wide = lax.broadcasted_iota(jnp.int32, (all_seats, slots), 1)
    for k in range(TOP):
        merge[k] = jnp.where(wide == stood[:, k : k + 1].astype(jnp.int32) - 1, 1.0, 0.0).astype(BF16)
    shares_of = [stood[:, TOP + k : TOP + k + 1] for k in range(TOP)]
    others = block.at[pl.ds(0, (n_tp - 1) * piece)]
    whole(others, came.at[0]).wait()
    picked = dot(spread[...], block[...]).astype(BF16)
    zs[...] = picked.reshape(zs.shape)

    def z_out(k):
        i = order.index(Z - k)
        return remote(
            zs.at[(z + k) % Z], zr.at[i], done.at[5], came.at[2 if i < group_size else 7], at.at(z=(z + k) % Z)
        )

    for k in order[1:]:
        z_out(Z - k).start()
    zr[0:1] = zs[pl.ds(z, 1)]

    side = x % C
    mine_half = x // C
    per = PARTS // 2

    def x_out(half, k):
        to = (x + k) % X
        return (
            xs.at[half, to],
            rows.at[y, half * per + mine_half, :, share_cols(c)],
            done.at[8 if k else 9],
            xrs.at[half],
            at.at(x=to, c=side),
        )

    for half in (0, 1):
        first = 1 - half
        arrived = zr.at[pl.ds(half * group_size + first, group_size - first)]
        whole(arrived, came.at[7 if half else 2]).wait()
        listed_rows = slice(half * (slots // 2), (half + 1) * (slots // 2))
        listed_seats = slice(half * (all_seats // 2), (half + 1) * (all_seats // 2))
        group_rows = zr[half * group_size : (half + 1) * group_size].reshape(all_seats // 2, DV)
        picked = dot(serve[listed_rows, listed_seats], group_rows)
        xs[half] = picked.astype(BF16).reshape(xs.shape[1:])
        for k in range(1, X):
            remote(*x_out(half, k)).start()
        src, dst, s_sem, r_sem, to = x_out(half, 0)

        @pl.when(side == c)
        def _(src=src, dst=dst, r_sem=r_sem):
            pltpu.make_async_copy(src, dst, r_sem).start()

        @pl.when(side != c)
        def _(args=(src, dst, s_sem, r_sem, pair)):
            remote(*args).start()

    def gather(way, step, part):
        j = (y + Y - (step - 1)) % Y if way == 0 else (y + step - 1) % Y
        to = (y + 1) % Y if way == 0 else (y + Y - 1) % Y
        i = way * ring_size(steps) + (step - 1) * PARTS + (part if step < steps else part % per)
        return remote(rows.at[j, part], rows.at[j, part], done.at[2], gr.at[i], at.at(y=to))

    def start_gather(way, step, part):
        gather(way, step, part).start()

    for half in (0, 1):
        whole(rows.at[y, pl.ds(half * per, per)], xrs.at[half]).wait()
        for part in range(half * per, half * per + per):
            for way in (0, 1):
                start_gather(way, 1, part)

    count = rows.shape[1] * rows.shape[2]
    chunk = rows.shape[3]
    local[0].wait()
    local[1].wait()
    crossed[1].wait_recv()
    crossed[2].wait_recv()

    def grow(j, first=False):
        a = rows[pl.ds(j, 1)].reshape(count, chunk)
        at_rows = pl.ds(pl.multiple_of(j * chunk, chunk), chunk)
        for k in range(4):
            value = dot(a, gu[k, at_rows, :])
            acc[k] = value if first else acc[k] + value

    grow(y, True)
    for step in range(1, steps):
        for part in range(PARTS):
            for way in (0, 1):
                gather(way, step, part).wait_recv()
                if step + 1 < steps or way == part // per:
                    start_gather(way, step + 1, part)
        grow((y + Y - step) % Y)
        grow((y + step) % Y)
    for part in range(PARTS):
        gather(part // per, steps, part).wait_recv()
    grow((y + steps) % Y)

    for k in (0, 1):
        gate, up = acc[2 * k], acc[2 * k + 1]
        hid[k] = (gate * jax.nn.sigmoid(gate) * up).astype(BF16)

    local[2].wait()
    crossed[3].wait_recv()
    made = {}

    def down(offset):
        d = (y + offset + Y) % Y
        cols = pl.ds(pl.multiple_of(d * chunk, chunk), chunk)
        value = dot(hid[0], wd[0, :, cols]) + dot(hid[1], wd[1, :, cols])
        shares[offset + steps - 1] = value.reshape(PARTS, count // PARTS, chunk)

    def down_part(offset, part):
        if offset not in made:
            down(offset)
            made[offset] = True
        return shares[offset + steps - 1, part]

    def x_back(half, column_of, core):
        home = column_of * C + c
        return (
            result.at[half * per + column_of, :, pl.ds(core * DV, DV)],
            xb.at[half, x],
            xbs.at[(half * per + column_of) * C + core],
            came.at[5],
            at.at(x=home, c=core),
        ), (home == x) & (c == core)

    def keep_result(part, value):
        result[part] = value.astype(BF16)
        for core in range(C):
            args, here = x_back(part // per, part % per, core)

            @pl.when(here)
            def _(args=args):
                pltpu.make_async_copy(args[0], args[1], args[3]).start()

            @pl.when(jnp.logical_not(here))
            def _(args=args):
                remote(*args).start()

    ring_sum(at, down_part, keep_result, sb, rb, done.at[1], sums)

    whole(xb, came.at[5]).wait()
    served = xb[...].reshape(slots, DV)
    served = shares_of[0] * dot(merge[0], served) + shares_of[1] * dot(merge[1], served)
    zs2[...] = served.astype(BF16).reshape(zs2.shape)

    def z_back(k):
        return remote(zs2.at[order.index(k)], zr2.at[z], done.at[6], came.at[3], at.at(z=(z + k) % Z))

    for k in far_first(Z):
        z_back(k).start()
    zr2[pl.ds(z, 1)] = zs2[0:1]
    whole(zr2.at[pl.ds(0, Z - 1)], came.at[3]).wait()
    column[...] = dot(find[...], zr2[...].reshape(all_seats, DV)).astype(BF16)

    def to_rows(k):
        t = (at.tp + k) % n_tp
        return remote(
            column.at[share_rows(t), :], branch.at[:, share_cols(at.tp)], done.at[4], came.at[1], (at.sp, t)
        )

    def start_rows(k, carry):
        to_rows(k).start()
        return carry

    lax.fori_loop(1, n_tp, start_rows, 0)
    branch[:, share_cols(at.tp)] = column[share_rows(at.tp), :]
    whole(others, came.at[1]).wait()
    b = branch[...].astype(F32)
    b = b * lax.rsqrt(jnp.mean(b * b, axis=1, keepdims=True) + EPSILON) * after_gain[...]
    out[...] = (mid[...].astype(F32) + b).astype(BF16)

    whole(rx.at[pl.ds(0, X - 1)], done.at[7]).wait()
    for k in range(1, Z):

        @pl.when(z + k < Z)
        def _(k=k):
            state_z(k).wait_send()

    @pl.when(jnp.logical_not(lead))
    def _():
        swap.wait_send()

    @pl.when(lead)
    def _():
        handed.wait_send()
        whole(sa, done.at[0]).wait()

    for k in crossed:
        k.wait_send()
    whole(sb, done.at[1]).wait()
    whole(rows.at[pl.ds(0, Y - 1)], done.at[2]).wait()
    whole(others, done.at[3]).wait()
    whole(others, done.at[4]).wait()
    whole(zr.at[pl.ds(0, Z - 1)], done.at[5]).wait()
    whole(told.at[pl.ds(0, Z - 1)], done.at[10]).wait()
    whole(zr2.at[pl.ds(0, Z - 1)], done.at[6]).wait()
    whole(xs.at[:, pl.ds(0, X - 1)], done.at[8]).wait()

    @pl.when(side != c)
    def _():
        whole(xs.at[:, 0], done.at[9]).wait()

    for part in range(PARTS):
        for core in range(C):
            args, here = x_back(part // per, part % per, core)

            @pl.when(jnp.logical_not(here))
            def _(args=args):
                remote(*args).wait_send()


def shards(
    query, key, value, gate_rows, decay, bias, extra, head_gain, output_projection, residual,
    attention_gain, before_gain, after_gain, w_gate, w_up, w_down, ids, weights,
):
    n_sp, n_tp = lax.axis_size("sp"), lax.axis_size("tp")
    tokens, width = query.shape[0], residual.shape[1]
    piece = residual.shape[0]
    X, C = GROUP_SIZE, CORES
    Z, Y = n_sp // X, n_tp // C
    cap = 5 * tokens // (2 * n_sp)
    slots = n_sp * cap
    seats = -(-(X * cap // TOP) // 16) * 16
    steps = Y // 2
    msgs = 2 * ring_size(steps)
    part = slots // C // PARTS
    chunk = C * DV
    hidden = w_gate.shape[2]
    hbm = pl.BlockSpec(memory_space=pltpu.HBM)
    sem = pltpu.SemaphoreType.DMA
    message = (KEY_CHANNELS + 16, DV)
    operands = [
        query.T, key.T, value, gate_rows, decay.T, bias[None], extra.T, head_gain[None],
        residual, attention_gain[None], before_gain[None], after_gain[None], ids.T, weights.T,
    ]
    scratch = [
        [pltpu.VMEM(a.shape, a.dtype) for a in operands],
        pltpu.VMEM((Y, C, piece, DV), BF16),
        pltpu.VMEM((128, tokens), F32),
        pltpu.VMEM((8, tokens), F32),
        pltpu.VMEM((Z * seats, tokens), BF16),
        pltpu.VMEM((tokens, Z * seats), BF16),
        pltpu.VMEM((Z, 8, DV), F32),
        pltpu.VMEM((Z, 8, DV), F32),
        pltpu.VMEM((slots, Z * seats), BF16),
        pltpu.VMEM((TOP, Z * seats, slots), BF16),
        pltpu.VMEM(message, BF16),
        pltpu.VMEM((X, *message), BF16),
        pltpu.VMEM(message, BF16),
        pltpu.VMEM((Z, *message), BF16),
        pltpu.VMEM((4, width, hidden), BF16),
        pltpu.VMEM((2, hidden, width), BF16),
        pltpu.VMEM((2, DV, width), BF16),
        pltpu.VMEM((Y, C, piece, DV), BF16),
        pltpu.VMEM((Y, C * piece, width), F32),
        pltpu.VMEM((C, piece, width), F32),
        pltpu.VMEM((piece, width), BF16),
        pltpu.VMEM((piece, width), BF16),
        pltpu.VMEM((tokens, DV), BF16),
        pltpu.VMEM((Y, PARTS, part, chunk), BF16),
        pltpu.VMEM((4, PARTS * part, hidden), F32),
        pltpu.VMEM((2, PARTS * part, hidden), BF16),
        pltpu.VMEM((Y, PARTS, part, chunk), F32),
        pltpu.VMEM((PARTS, part, chunk), BF16),
        pltpu.VMEM((Z, seats, DV), BF16),
        pltpu.VMEM((Z, seats, DV), BF16),
        pltpu.VMEM((2, X, part, DV), BF16),
        pltpu.VMEM((2, X, part, DV), BF16),
        pltpu.VMEM((Z, seats, DV), BF16),
        pltpu.VMEM((Z, seats, DV), BF16),
        pltpu.VMEM((tokens, DV), BF16),
        pltpu.VMEM((piece, width), BF16),
        pltpu.VMEM((msgs, C * piece, width // PARTS), BF16),
        pltpu.VMEM((msgs, C * piece, width // PARTS), BF16),
        pltpu.VMEM((msgs, part, chunk), BF16),
        pltpu.VMEM((msgs, part, chunk), BF16),
        sem((4,)), sem((4,)), sem((4,)), sem((4,)), sem((msgs,)), sem((msgs,)), sem((2,)), sem((PARTS * C,)),
        sem((Z,)), sem((Z,)), sem((len(operands),)), sem((11,)), sem((8,)),
    ]
    return pl.pallas_call(
        functools.partial(layer_kernel, n_sp, n_tp, X, cap),
        out_shape=jax.ShapeDtypeStruct((piece, width), BF16),
        in_specs=[[hbm] * len(operands), hbm, hbm, hbm, hbm],
        out_specs=pl.BlockSpec(memory_space=pltpu.VMEM),
        scratch_shapes=scratch,
        name="layer",
        compiler_params=pltpu.CompilerParams(
            collective_id=0, has_side_effects=True, vmem_limit_bytes=40 * 1024 * 1024
        ),
    )(
        *jax.tree.map(lambda a: pltpu.with_memory_space_constraint(a, pltpu.HBM), (operands, output_projection, w_gate[0], w_up[0], w_down[0]))
    )


def solution(mesh):
    placed = (
        P("sp", "tp"),
        P("sp", "tp"),
        P("sp", "tp"),
        P("sp", "tp"),
        P("sp", "tp"),
        P("tp"),
        P("sp", "tp"),
        P(),
        P("tp", None),
        P(("sp", "tp"), None),
        P(),
        P(),
        P(),
        P("sp", None, "tp"),
        P("sp", None, "tp"),
        P("sp", "tp", None),
        P("sp", None),
        P("sp", None),
    )
    return jax.shard_map(
        shards, mesh=mesh, in_specs=placed, out_specs=P(("sp", "tp"), None), check_vma=False
    )
```

```python
import functools

import jax
import jax.numpy as jnp
from jax import lax
from jax.experimental import pallas as pl
from jax.experimental.pallas import tpu as pltpu
from jax.sharding import PartitionSpec as P

KEY_CHANNELS = 64
DV = 128
TOP = 2
BLOCK = 64
GROUP_SIZE = 4
CORES = 2

EPSILON = 1e-06
DECAY_NORMALIZER = 16.0
MESH = pl.DeviceIdType.MESH
BF16 = jnp.bfloat16
F32 = jnp.float32
PARTS = 4


def dot(a, b):
    return jnp.dot(a, b, preferred_element_type=F32)


class Place:
    def __init__(self, n_sp, n_tp, group):
        self.X, self.Z = group, n_sp // group
        self.C, self.Y = CORES, n_tp // CORES
        self.n_tp = n_tp
        self.sp, self.tp = lax.axis_index("sp"), lax.axis_index("tp")
        self.z, self.x = self.sp // self.X, self.sp % self.X
        self.y, self.c = self.tp // self.C, self.tp % self.C

    def at(self, z=None, x=None, y=None, c=None):
        z = self.z if z is None else z
        x = self.x if x is None else x
        y = self.y if y is None else y
        c = self.c if c is None else c
        return (z * self.X + x, y * self.C + c)


def remote(src, dst, send, recv, to):
    return pltpu.make_async_remote_copy(
        src_ref=src, dst_ref=dst, send_sem=send, recv_sem=recv, device_id=to, device_id_type=MESH
    )


def ring_index(way, step, part, steps):
    first = part % (PARTS // 2) if step == 1 else PARTS // 2 + (step - 2) * PARTS + part
    return way * ring_size(steps) + first


def ring_size(steps):
    return PARTS // 2 + (steps - 1) * PARTS


def way_parts(way):
    low, high = list(range(PARTS // 2)), list(range(PARTS // 2, PARTS))
    return (low, high) if way == 0 else (high, low)


def both_ways(pick):
    return [(way, part) for pair in zip(pick(0), pick(1)) for way, part in enumerate(pair)]


def whole(ref, sem):
    return pltpu.make_async_copy(ref, ref, sem)


def ring_sum(at, part_of, out, sends, recvs, send_sem, recv_sems):
    Y, steps, y = at.Y, at.Y // 2, at.y

    def copy(way, step, part):
        i = ring_index(way, step, part, steps)
        to = (y + 1) % Y if way == 0 else (y + Y - 1) % Y
        return remote(sends.at[i], recvs.at[i], send_sem, recv_sems.at[i], at.at(y=to))

    def offset(way, step):
        k = steps - step + 1
        return k if way == 0 or k == steps else -k

    def send(way, step, part, value):
        sends[ring_index(way, step, part, steps)] = value.astype(BF16)
        copy(way, step, part).start()

    for way, part in both_ways(lambda w: way_parts(w)[0]):
        send(way, 1, part, part_of(offset(way, 1), part))
    for step in range(2, steps + 1):
        for way, part in both_ways(lambda w: way_parts(w)[1] + way_parts(w)[0]):
            value = part_of(offset(way, step), part)
            if step > 2 or part in way_parts(way)[0]:
                copy(way, step - 1, part).wait_recv()
                value = value + recvs[ring_index(way, step - 1, part, steps)].astype(F32)
            send(way, step, part, value)
    for part in range(PARTS):
        total = part_of(0, part)
        for way in (0, 1):
            copy(way, steps, part).wait_recv()
            total = total + recvs[ring_index(way, steps, part, steps)].astype(F32)
        out(part, total)


def relay_sum(at, prepare, part_of, out, sends, recvs, send_sem, recv_sems):
    Y, y = at.Y, at.y
    hops = (2, 1, 2, 1)
    starts = (0, PARTS // 2, PARTS // 2 + PARTS, PARTS // 2 + 2 * PARTS)

    def slot(way, kind, part):
        return way * ring_size(Y // 2) + starts[kind] + (part % (PARTS // 2) if kind == 0 else part)

    def copy(way, kind, part):
        i = slot(way, kind, part)
        to = (y + hops[kind]) % Y if way == 0 else (y + Y - hops[kind]) % Y
        return remote(sends.at[i], recvs.at[i], send_sem, recv_sems.at[i], at.at(y=to))

    def send(way, kind, part, value):
        sends[slot(way, kind, part)] = value.astype(BF16)
        copy(way, kind, part).start()

    def received(way, kind, part):
        copy(way, kind, part).wait_recv()
        return recvs[slot(way, kind, part)].astype(F32)

    def own(way, k, part):
        return part_of(k if way == 0 or k == Y // 2 else -k, part)

    def direct(part):
        for way in (0, 1):
            send(way, 3, part, own(way, 1, part))

    for pair in zip(way_parts(0)[0], way_parts(1)[0]):
        for part in pair:
            prepare(part)
            for way in (0, 1):
                if part in way_parts(way)[0]:
                    send(way, 0, part, own(way, Y // 2, part))
                send(way, 1, part, own(way, 3, part))
    early = way_parts(0)[0]
    for part in early:
        direct(part)
    for way, part in both_ways(lambda w: way_parts(w)[1] + way_parts(w)[0]):
        value = own(way, 2, part) + received(way, 1, part)
        if part in way_parts(way)[0]:
            value = value + received(way, 0, part)
        send(way, 2, part, value)
    for part in range(PARTS):
        if part not in early:
            direct(part)
    for part in range(PARTS):
        total = part_of(0, part)
        for way in (0, 1):
            total = total + received(way, 3, part) + received(way, 2, part)
        out(part, total)


def far_first(count):
    return sorted(range(1, count), key=lambda k: (-min(k, count - k), k))


def near_order(count):
    return sorted(range(count), key=lambda k: (min(k, count - k), k))


def split(value):
    high = value.astype(BF16)
    rest = value - high.astype(F32)
    middle = rest.astype(BF16)
    return high, middle, (rest - middle.astype(F32)).astype(BF16)


def standing(row, count):
    square = (count, row.shape[1])
    same = lax.broadcasted_iota(jnp.int32, square, 0) == lax.broadcasted_iota(jnp.int32, square, 1)
    return jnp.sum(jnp.where(same, row, 0.0), axis=1, keepdims=True)


def lying(col, width):
    square = (col.shape[0], width)
    same = lax.broadcasted_iota(jnp.int32, square, 0) == lax.broadcasted_iota(jnp.int32, square, 1)
    return jnp.sum(jnp.where(same, col, 0.0), axis=0, keepdims=True)


def layer_kernel(
    n_sp, n_tp, group, cap,
    operands, residual, w_out, w_gate, w_up, w_down,
    out,
    held,
    gated, stack, facts, spread, find, told, heard, serve, merge, sx, rx, sz, rz,
    gu, wd, wo, partner, mixed, summed, both, mid, normed, block, rows, acc, hid, shares, result,
    zs, zr, xs, xb, zs2, zr2, column, branch,
    sa, ra, sb, rb,
    wsem, wrs, wrr, gsem, sums, gr, xrs, xbs, szs, szr, osem, done, came,
):
    at = Place(n_sp, n_tp, group)
    X, Y, Z, C = at.X, at.Y, at.Z, at.C
    x, y, z, c = at.x, at.y, at.z, at.c
    steps = Y // 2
    other = 1 - c

    (
        q_t, k_t, values, gate_rows, decay_t, bias, extra, head_gain,
        attention_gain, before_gain, after_gain, ids_row, weights_row,
    ) = held
    loads = [pltpu.make_async_copy(a, b, osem.at[k]) for k, (a, b) in enumerate(zip(operands, held))]
    for k in loads:
        k.start()
    local = [
        pltpu.make_async_copy(w_gate, gu.at[0], wsem.at[0]),
        pltpu.make_async_copy(w_up, gu.at[1], wsem.at[1]),
        pltpu.make_async_copy(w_down, wd.at[0], wsem.at[2]),
        pltpu.make_async_copy(w_out, wo.at[0], wsem.at[3]),
        pltpu.make_async_copy(residual, both.at[c], wsem.at[4]),
    ]
    rz[...] = jnp.zeros_like(rz)
    barrier = pltpu.get_barrier_semaphore()

    def greet_tp(k, carry):
        pl.semaphore_signal(barrier, inc=1, device_id=(at.sp, (at.tp + k) % n_tp), device_id_type=MESH)
        return carry

    lax.fori_loop(1, n_tp, greet_tp, 0)
    for k in range(1, Z):
        pl.semaphore_signal(barrier, inc=1, device_id=at.at(z=(z + k) % Z), device_id_type=MESH)
    for k in range(1, X):
        for core in range(C):
            pl.semaphore_signal(barrier, inc=1, device_id=at.at(x=(x + k) % X, c=core), device_id_type=MESH)

    for k in (3, 4, 0, 1, 2):
        local[k].start()
    for k in loads:
        k.wait()

    tokens = q_t.shape[1]
    blocks = tokens // BLOCK
    pre = decay_t[...].astype(F32) + standing(bias[...], KEY_CHANNELS)
    log_decay = -(jnp.maximum(-pre, 0.0) + jnp.log1p(jnp.exp(-jnp.abs(pre)))) / DECAY_NORMALIZER + extra[...]
    r, q = (lax.broadcasted_iota(jnp.int32, (tokens, tokens), k) for k in (0, 1))
    one_block = (r // BLOCK) == (q // BLOCK)
    upto = jnp.where((r <= q) & one_block, 1.0, 0.0).astype(BF16)
    inside = sum(dot(term, upto) for term in split(log_decay))
    ends = [inside[:, (b + 1) * BLOCK - 1 : (b + 1) * BLOCK] for b in range(blocks)]
    of_block = lax.broadcasted_iota(jnp.int32, (KEY_CHANNELS, tokens), 1) // BLOCK
    keys = k_t[...].astype(F32)
    to_end = [jnp.where(of_block == b, keys * jnp.exp(jnp.minimum(ends[b] - inside, 0.0)), 0.0) for b in range(blocks)]
    vals = values[...]
    growth = dot(jnp.concatenate(to_end, axis=0).astype(BF16), vals)
    growth = [growth[b * KEY_CHANNELS : (b + 1) * KEY_CHANNELS] for b in range(blocks)]
    fades = [jnp.exp(e) for e in ends]
    state = growth[0]
    for b in range(1, blocks):
        state = fades[b] * state + growth[b]
    fade_row = lying(jnp.exp(sum(ends)), DV)
    tail = KEY_CHANNELS + 16

    def message(ref, state_part, row):
        ref[0:KEY_CHANNELS, :] = state_part.astype(BF16)
        ref[KEY_CHANNELS:tail, :] = jnp.broadcast_to(row, (16, DV)).astype(BF16)

    message(sx, state, fade_row)
    pl.semaphore_wait(barrier, n_tp - 1 + Z - 1 + (X - 1) * C)

    def state_x(k):
        return remote(sx, rx.at[x], done.at[7], came.at[4], at.at(x=(x + k) % X))

    for k in range(1, X):
        state_x(k).start()
    pair = at.at(c=other)
    crossed = [
        remote(w_out, wo.at[1], wrs.at[3], wrr.at[3], pair),
        remote(w_gate, gu.at[2], wrs.at[0], wrr.at[0], pair),
        remote(w_up, gu.at[3], wrs.at[1], wrr.at[1], pair),
        remote(w_down, wd.at[1], wrs.at[2], wrr.at[2], pair),
    ]
    for k in crossed:
        k.start()
    lead = c == C - 1
    lent = remote(residual, both.at[0], gsem.at[4], gsem.at[5], pair)

    @pl.when(jnp.logical_not(lead))
    def _():
        lent.start()

    rx[pl.ds(x, 1)] = sx[...].reshape(1, tail, DV)

    slots = n_sp * cap
    seats = zs.shape[1]
    sub = lax.broadcasted_iota(jnp.int32, (n_sp, tokens), 0)
    chosen = [ids_row[k : k + 1, :] for k in range(TOP)]
    named = jnp.where((sub == chosen[0]) | (sub == chosen[1]), 1.0, 0.0).astype(BF16)
    before = dot(named, jnp.where(r < q, 1.0, 0.0).astype(BF16))
    targets = []
    plane_of = chosen[0] // X
    order = near_order(Z)
    group_size = Z // 2
    away = z - plane_of
    away = jnp.where(away < 0, away + Z, away)
    base = jnp.zeros_like(away)
    for i, k in enumerate(order):
        start = (i // group_size) * (X * group_size * cap) + (i % group_size) * cap
        base = jnp.where(away == k, start, base)
    for e in chosen:
        slot = jnp.sum(jnp.where(sub == e, before, 0.0), axis=0, keepdims=True)
        targets.append((e - plane_of * X) * (group_size * cap) + base + slot.astype(jnp.int32))
    sub = lax.broadcasted_iota(jnp.int32, (Z, tokens), 0)
    before = dot(jnp.where(sub == plane_of, 1.0, 0.0).astype(BF16), jnp.where(r < q, 1.0, 0.0).astype(BF16))
    rank = jnp.sum(jnp.where(sub == plane_of, before, 0.0), axis=0, keepdims=True)
    seat = plane_of * seats + rank.astype(jnp.int32)
    query = q_t[...].astype(F32) * (KEY_CHANNELS**-0.5 * jnp.exp(inside))
    stack[0:KEY_CHANNELS, :] = query
    stack[KEY_CHANNELS:, :] = jnp.zeros((stack.shape[0] - KEY_CHANNELS, tokens), F32)
    stack[KEY_CHANNELS : KEY_CHANNELS + 1, :] = seat.astype(F32)
    facts[...] = jnp.zeros_like(facts)
    for k in range(TOP):
        facts[k : k + 1, :] = (targets[k] + 1).astype(F32)
        facts[TOP + k : TOP + k + 1, :] = weights_row[k : k + 1, :]
    stood = stack[...].T
    query = stood[:, 0:KEY_CHANNELS].astype(BF16)
    seat_col = stood[:, KEY_CHANNELS : KEY_CHANNELS + 1].astype(jnp.int32)
    scores = dot(query, (keys * jnp.exp(-inside)).astype(BF16))
    scores = jnp.where((r >= q) & one_block, scores, 0.0).astype(BF16)
    within = dot(scores, vals)

    whole(rx.at[pl.ds(0, X - 1)], came.at[4]).wait()
    plane, plane_row = rx[0, 0:KEY_CHANNELS].astype(F32), rx[0, KEY_CHANNELS:tail][0:1].astype(F32)
    ahead, ahead_fade = jnp.zeros_like(state), jnp.ones((KEY_CHANNELS, 1), F32)
    for k in range(X):
        part, row = rx[k, 0:KEY_CHANNELS].astype(F32), rx[k, KEY_CHANNELS:tail][0:1].astype(F32)
        fade = standing(row, KEY_CHANNELS)
        ahead = jnp.where(k < x, fade * ahead + part, ahead)
        ahead_fade = jnp.where(k < x, fade * ahead_fade, ahead_fade)
        if k:
            plane, plane_row = fade * plane + part, plane_row * row
    message(sz, plane, plane_row)

    def state_z(k):
        return remote(sz, rz.at[z], szs.at[k], szr.at[k], at.at(z=(z + k) % Z))

    for k in far_first(Z):

        @pl.when(z + k < Z)
        def _(k=k):
            state_z(k).start()

    all_seats = Z * seats
    tall = lax.broadcasted_iota(jnp.int32, (all_seats, tokens), 0)
    spread[...] = jnp.where(tall == seat, 1.0, 0.0).astype(BF16)
    wide = lax.broadcasted_iota(jnp.int32, (tokens, all_seats), 1)
    find[...] = jnp.where(wide == seat_col, 1.0, 0.0).astype(BF16)
    listed = sum(dot(term, find[...]) for term in split(facts[...]))
    near = lax.broadcasted_iota(jnp.int32, (8, DV), 1) < seats
    for k in range(Z):
        moved = pltpu.roll(listed, (all_seats - k * seats) % all_seats, 1) if k else listed
        told[k] = jnp.where(near, moved[:, 0:DV], 0.0)

    def tell(k):
        return remote(
            told.at[(z + k) % Z], heard.at[order.index(Z - k)], done.at[10], came.at[6], at.at(z=(z + k) % Z)
        )

    for k in far_first(Z):
        tell(k).start()
    heard[0:1] = told[pl.ds(z, 1)]
    gate_act = gate_rows[...].astype(F32)
    gate_act = gate_act * jax.nn.sigmoid(gate_act) * head_gain[...]

    for k in range(1, Z):

        @pl.when(z >= k)
        def _(k=k):
            state_z(k).wait_recv()

    carried = jnp.zeros_like(state)
    for k in range(Z - 1):
        fade = standing(rz[k, KEY_CHANNELS:tail][0:1].astype(F32), KEY_CHANNELS)
        carried = jnp.where(k < z, fade * carried + rz[k, 0:KEY_CHANNELS].astype(F32), carried)
    running = ahead_fade * carried + ahead
    across = []
    for b in range(blocks):
        across.append(dot(query[b * BLOCK : (b + 1) * BLOCK], running.astype(BF16)))
        running = fades[b] * running + growth[b]
    heads = within + jnp.concatenate(across, axis=0)
    heads = heads * lax.rsqrt(jnp.mean(heads * heads, axis=1, keepdims=True) + EPSILON) * gate_act
    gated[...] = heads.astype(BF16).reshape(gated.shape)
    swap = remote(gated, partner, gsem.at[0], gsem.at[1], pair)

    @pl.when(jnp.logical_not(lead))
    def _():
        swap.start()


    piece = gated.shape[2]
    width = wo.shape[2]
    local[3].wait()
    crossed[0].wait_recv()
    part_width = width // PARTS
    handed = remote(mid.at[0], mid.at[0], gsem.at[2], gsem.at[3], pair)

    def mixed_part(k, part):
        d = (y + k + Y) % Y
        return mixed[pl.ds(d, 1), :, part * part_width : (part + 1) * part_width].reshape(C * piece, part_width)

    def keep(part, value):
        summed[:, :, part * part_width : (part + 1) * part_width] = value.reshape(C, piece, part_width)

    @pl.when(lead)
    def _():
        swap.wait_recv()
        mine = gated[...].reshape(tokens, DV)
        theirs = partner[...].reshape(tokens, DV)

        def prepare(part):
            cols = slice(part * part_width, (part + 1) * part_width)
            value = dot(mine, wo[0, :, cols]) + dot(theirs, wo[1, :, cols])
            mixed[:, :, cols] = value.reshape(Y, C * piece, part_width)

        relay_sum(at, prepare, mixed_part, keep, sa, ra, done.at[0], sums)
        lent.wait_recv()
        local[4].wait()
        attn = summed[...].reshape(C * piece, width)
        attn = attn * lax.rsqrt(jnp.mean(attn * attn, axis=1, keepdims=True) + EPSILON) * attention_gain[...]
        m = (both[...].reshape(C * piece, width).astype(F32) + attn).astype(BF16)
        mid[...] = m.reshape(C, piece, width)
        m = m.astype(F32)
        m = m * lax.rsqrt(jnp.mean(m * m, axis=1, keepdims=True) + EPSILON) * before_gain[...]
        normed[...] = m.astype(BF16)

    def share_cols(t):
        return pl.ds(pl.multiple_of(t * DV, DV), DV)

    def share_rows(t):
        return pl.ds(pl.multiple_of(t * piece, piece), piece)

    chip_rows = pl.ds(pl.multiple_of(y * (C * piece), C * piece), C * piece)

    def to_width(k):
        t = (at.tp + k) % n_tp
        return remote(normed.at[:, share_cols(t)], block.at[chip_rows, :], done.at[3], came.at[0], (at.sp, t))

    def start_width(k, carry):
        to_width(k).start()
        return carry

    @pl.when(lead)
    def _():
        lax.fori_loop(1, n_tp, start_width, 0)
        handed.start()
        block[chip_rows, :] = normed[:, share_cols(at.tp)]

    @pl.when(jnp.logical_not(lead))
    def _():
        local[4].wait()

    whole(heard.at[pl.ds(1, Z - 1)], came.at[6]).wait()
    lists = None
    for k in range(Z):
        part = jnp.concatenate([heard[k], jnp.zeros((8, all_seats - DV), F32)], axis=1)
        part = pltpu.roll(part, k * seats, 1) if k else part
        lists = part if lists is None else lists + part
    tall = lax.broadcasted_iota(jnp.int32, (slots, all_seats), 0)
    hits = [jnp.where(tall == lists[k : k + 1, :].astype(jnp.int32) - 1, 1.0, 0.0) for k in range(TOP)]
    serve[...] = (hits[0] + hits[1]).astype(BF16)
    stood = jnp.concatenate([lists, jnp.zeros((DV - 8, all_seats), F32)], axis=0).T
    wide = lax.broadcasted_iota(jnp.int32, (all_seats, slots), 1)
    for k in range(TOP):
        merge[k] = jnp.where(wide == stood[:, k : k + 1].astype(jnp.int32) - 1, 1.0, 0.0).astype(BF16)
    shares_of = [stood[:, TOP + k : TOP + k + 1] for k in range(TOP)]
    others = block.at[pl.ds(0, (n_tp - 1) * piece)]

    @pl.when(lead)
    def _():
        whole(block.at[pl.ds(0, (Y - 1) * C * piece)], came.at[0]).wait()

    @pl.when(jnp.logical_not(lead))
    def _():
        whole(block, came.at[0]).wait()

    picked = dot(spread[...], block[...]).astype(BF16)
    zs[...] = picked.reshape(zs.shape)

    def z_out(k):
        i = order.index(Z - k)
        return remote(
            zs.at[(z + k) % Z], zr.at[i], done.at[5], came.at[2 if i < group_size else 7], at.at(z=(z + k) % Z)
        )

    for k in order[1:]:
        z_out(Z - k).start()
    zr[0:1] = zs[pl.ds(z, 1)]

    side = x % C
    mine_half = x // C
    per = PARTS // 2

    def x_out(half, k):
        to = (x + k) % X
        return (
            xs.at[half, to],
            rows.at[y, half * per + mine_half, :, share_cols(c)],
            done.at[8 if k else 9],
            xrs.at[half],
            at.at(x=to, c=side),
        )

    for half in (0, 1):
        first = 1 - half
        arrived = zr.at[pl.ds(half * group_size + first, group_size - first)]
        whole(arrived, came.at[7 if half else 2]).wait()
        listed_rows = slice(half * (slots // 2), (half + 1) * (slots // 2))
        listed_seats = slice(half * (all_seats // 2), (half + 1) * (all_seats // 2))
        group_rows = zr[half * group_size : (half + 1) * group_size].reshape(all_seats // 2, DV)
        picked = dot(serve[listed_rows, listed_seats], group_rows)
        xs[half] = picked.astype(BF16).reshape(xs.shape[1:])
        for k in range(1, X):
            remote(*x_out(half, k)).start()
        src, dst, s_sem, r_sem, to = x_out(half, 0)

        @pl.when(side == c)
        def _(src=src, dst=dst, r_sem=r_sem):
            pltpu.make_async_copy(src, dst, r_sem).start()

        @pl.when(side != c)
        def _(args=(src, dst, s_sem, r_sem, pair)):
            remote(*args).start()

    def gather(way, step, part):
        j = (y + Y - (step - 1)) % Y if way == 0 else (y + step - 1) % Y
        to = (y + 1) % Y if way == 0 else (y + Y - 1) % Y
        i = way * ring_size(steps) + (step - 1) * PARTS + (part if step < steps else part % per)
        return remote(rows.at[j, part], rows.at[j, part], done.at[2], gr.at[i], at.at(y=to))

    def start_gather(way, step, part):
        gather(way, step, part).start()

    for half in (0, 1):
        whole(rows.at[y, pl.ds(half * per, per)], xrs.at[half]).wait()
        for part in range(half * per, half * per + per):
            for way in (0, 1):
                start_gather(way, 1, part)

    count = rows.shape[1] * rows.shape[2]
    chunk = rows.shape[3]
    local[0].wait()
    local[1].wait()
    crossed[1].wait_recv()
    crossed[2].wait_recv()

    def grow(j, first=False):
        a = rows[pl.ds(j, 1)].reshape(count, chunk)
        at_rows = pl.ds(pl.multiple_of(j * chunk, chunk), chunk)
        for k in range(4):
            value = dot(a, gu[k, at_rows, :])
            acc[k] = value if first else acc[k] + value

    grow(y, True)
    for step in range(1, steps):
        for part in range(PARTS):
            for way in (0, 1):
                gather(way, step, part).wait_recv()
                if step + 1 < steps or way == part // per:
                    start_gather(way, step + 1, part)
        grow((y + Y - step) % Y)
        grow((y + step) % Y)
    for part in range(PARTS):
        gather(part // per, steps, part).wait_recv()
    grow((y + steps) % Y)

    for k in (0, 1):
        gate, up = acc[2 * k], acc[2 * k + 1]
        hid[k] = (gate * jax.nn.sigmoid(gate) * up).astype(BF16)

    local[2].wait()
    crossed[3].wait_recv()
    made = {}

    def down(offset):
        d = (y + offset + Y) % Y
        cols = pl.ds(pl.multiple_of(d * chunk, chunk), chunk)
        value = dot(hid[0], wd[0, :, cols]) + dot(hid[1], wd[1, :, cols])
        shares[offset + steps - 1] = value.reshape(PARTS, count // PARTS, chunk)

    def down_part(offset, part):
        if offset not in made:
            down(offset)
            made[offset] = True
        return shares[offset + steps - 1, part]

    def x_back(half, column_of, core):
        home = column_of * C + c
        return (
            result.at[half * per + column_of, :, pl.ds(core * DV, DV)],
            xb.at[half, x],
            xbs.at[(half * per + column_of) * C + core],
            came.at[5],
            at.at(x=home, c=core),
        ), (home == x) & (c == core)

    def keep_result(part, value):
        result[part] = value.astype(BF16)
        for core in range(C):
            args, here = x_back(part // per, part % per, core)

            @pl.when(here)
            def _(args=args):
                pltpu.make_async_copy(args[0], args[1], args[3]).start()

            @pl.when(jnp.logical_not(here))
            def _(args=args):
                remote(*args).start()

    ring_sum(at, down_part, keep_result, sb, rb, done.at[1], sums)

    whole(xb, came.at[5]).wait()
    served = xb[...].reshape(slots, DV)
    served = shares_of[0] * dot(merge[0], served) + shares_of[1] * dot(merge[1], served)
    zs2[...] = served.astype(BF16).reshape(zs2.shape)

    def z_back(k):
        return remote(zs2.at[order.index(k)], zr2.at[z], done.at[6], came.at[3], at.at(z=(z + k) % Z))

    for k in far_first(Z):
        z_back(k).start()
    zr2[pl.ds(z, 1)] = zs2[0:1]
    whole(zr2.at[pl.ds(0, Z - 1)], came.at[3]).wait()
    column[...] = dot(find[...], zr2[...].reshape(all_seats, DV)).astype(BF16)

    def to_rows(k):
        t = (at.tp + k) % n_tp
        return remote(
            column.at[share_rows(t), :], branch.at[:, share_cols(at.tp)], done.at[4], came.at[1], (at.sp, t)
        )

    def start_rows(k, carry):
        to_rows(k).start()
        return carry

    lax.fori_loop(1, n_tp, start_rows, 0)
    branch[:, share_cols(at.tp)] = column[share_rows(at.tp), :]
    whole(others, came.at[1]).wait()
    b = branch[...].astype(F32)
    b = b * lax.rsqrt(jnp.mean(b * b, axis=1, keepdims=True) + EPSILON) * after_gain[...]

    @pl.when(jnp.logical_not(lead))
    def _():
        handed.wait_recv()

    out[...] = (mid[pl.ds(c, 1)].reshape(piece, width).astype(F32) + b).astype(BF16)

    whole(rx.at[pl.ds(0, X - 1)], done.at[7]).wait()
    for k in range(1, Z):

        @pl.when(z + k < Z)
        def _(k=k):
            state_z(k).wait_send()

    @pl.when(jnp.logical_not(lead))
    def _():
        swap.wait_send()
        lent.wait_send()

    @pl.when(lead)
    def _():
        handed.wait_send()
        whole(normed.at[:, pl.ds(0, (n_tp - 1) * DV)], done.at[3]).wait()
        whole(sa, done.at[0]).wait()

    for k in crossed:
        k.wait_send()
    whole(sb, done.at[1]).wait()
    whole(rows.at[pl.ds(0, Y - 1)], done.at[2]).wait()
    whole(others, done.at[4]).wait()
    whole(zr.at[pl.ds(0, Z - 1)], done.at[5]).wait()
    whole(told.at[pl.ds(0, Z - 1)], done.at[10]).wait()
    whole(zr2.at[pl.ds(0, Z - 1)], done.at[6]).wait()
    whole(xs.at[:, pl.ds(0, X - 1)], done.at[8]).wait()

    @pl.when(side != c)
    def _():
        whole(xs.at[:, 0], done.at[9]).wait()

    for part in range(PARTS):
        for core in range(C):
            args, here = x_back(part // per, part % per, core)

            @pl.when(jnp.logical_not(here))
            def _(args=args):
                remote(*args).wait_send()


def shards(
    query, key, value, gate_rows, decay, bias, extra, head_gain, output_projection, residual,
    attention_gain, before_gain, after_gain, w_gate, w_up, w_down, ids, weights,
):
    n_sp, n_tp = lax.axis_size("sp"), lax.axis_size("tp")
    tokens, width = query.shape[0], residual.shape[1]
    piece = residual.shape[0]
    X, C = GROUP_SIZE, CORES
    Z, Y = n_sp // X, n_tp // C
    cap = 5 * tokens // (2 * n_sp)
    slots = n_sp * cap
    seats = -(-(X * cap // TOP) // 16) * 16
    steps = Y // 2
    msgs = 2 * ring_size(steps)
    part = slots // C // PARTS
    chunk = C * DV
    hidden = w_gate.shape[2]
    hbm = pl.BlockSpec(memory_space=pltpu.HBM)
    sem = pltpu.SemaphoreType.DMA
    message = (KEY_CHANNELS + 16, DV)
    operands = [
        query.T, key.T, value, gate_rows, decay.T, bias[None], extra.T, head_gain[None],
        attention_gain[None], before_gain[None], after_gain[None], ids.T, weights.T,
    ]
    scratch = [
        [pltpu.VMEM(a.shape, a.dtype) for a in operands],
        pltpu.VMEM((Y, C, piece, DV), BF16),
        pltpu.VMEM((128, tokens), F32),
        pltpu.VMEM((8, tokens), F32),
        pltpu.VMEM((Z * seats, tokens), BF16),
        pltpu.VMEM((tokens, Z * seats), BF16),
        pltpu.VMEM((Z, 8, DV), F32),
        pltpu.VMEM((Z, 8, DV), F32),
        pltpu.VMEM((slots, Z * seats), BF16),
        pltpu.VMEM((TOP, Z * seats, slots), BF16),
        pltpu.VMEM(message, BF16),
        pltpu.VMEM((X, *message), BF16),
        pltpu.VMEM(message, BF16),
        pltpu.VMEM((Z, *message), BF16),
        pltpu.VMEM((4, width, hidden), BF16),
        pltpu.VMEM((2, hidden, width), BF16),
        pltpu.VMEM((2, DV, width), BF16),
        pltpu.VMEM((Y, C, piece, DV), BF16),
        pltpu.VMEM((Y, C * piece, width), F32),
        pltpu.VMEM((C, piece, width), F32),
        pltpu.VMEM((C, piece, width), BF16),
        pltpu.VMEM((C, piece, width), BF16),
        pltpu.VMEM((C * piece, width), BF16),
        pltpu.VMEM((tokens, DV), BF16),
        pltpu.VMEM((Y, PARTS, part, chunk), BF16),
        pltpu.VMEM((4, PARTS * part, hidden), F32),
        pltpu.VMEM((2, PARTS * part, hidden), BF16),
        pltpu.VMEM((Y, PARTS, part, chunk), F32),
        pltpu.VMEM((PARTS, part, chunk), BF16),
        pltpu.VMEM((Z, seats, DV), BF16),
        pltpu.VMEM((Z, seats, DV), BF16),
        pltpu.VMEM((2, X, part, DV), BF16),
        pltpu.VMEM((2, X, part, DV), BF16),
        pltpu.VMEM((Z, seats, DV), BF16),
        pltpu.VMEM((Z, seats, DV), BF16),
        pltpu.VMEM((tokens, DV), BF16),
        pltpu.VMEM((piece, width), BF16),
        pltpu.VMEM((msgs, C * piece, width // PARTS), BF16),
        pltpu.VMEM((msgs, C * piece, width // PARTS), BF16),
        pltpu.VMEM((msgs, part, chunk), BF16),
        pltpu.VMEM((msgs, part, chunk), BF16),
        sem((5,)), sem((4,)), sem((4,)), sem((6,)), sem((msgs,)), sem((msgs,)), sem((2,)), sem((PARTS * C,)),
        sem((Z,)), sem((Z,)), sem((len(operands),)), sem((11,)), sem((8,)),
    ]
    return pl.pallas_call(
        functools.partial(layer_kernel, n_sp, n_tp, X, cap),
        out_shape=jax.ShapeDtypeStruct((piece, width), BF16),
        in_specs=[[hbm] * len(operands), hbm, hbm, hbm, hbm, hbm],
        out_specs=pl.BlockSpec(memory_space=pltpu.VMEM),
        scratch_shapes=scratch,
        name="layer",
        compiler_params=pltpu.CompilerParams(
            collective_id=0, has_side_effects=True, vmem_limit_bytes=40 * 1024 * 1024
        ),
    )(
        *jax.tree.map(lambda a: pltpu.with_memory_space_constraint(a, pltpu.HBM), (operands, residual, output_projection, w_gate[0], w_up[0], w_down[0]))
    )


def solution(mesh):
    placed = (
        P("sp", "tp"),
        P("sp", "tp"),
        P("sp", "tp"),
        P("sp", "tp"),
        P("sp", "tp"),
        P("tp"),
        P("sp", "tp"),
        P(),
        P("tp", None),
        P(("sp", "tp"), None),
        P(),
        P(),
        P(),
        P("sp", None, "tp"),
        P("sp", None, "tp"),
        P("sp", "tp", None),
        P("sp", None),
        P("sp", None),
    )
    return jax.shard_map(
        shards, mesh=mesh, in_specs=placed, out_specs=P(("sp", "tp"), None), check_vma=False
    )
```

```python
import functools

import jax
import jax.numpy as jnp
from jax import lax
from jax.experimental import pallas as pl
from jax.experimental.pallas import tpu as pltpu
from jax.sharding import PartitionSpec as P

KEY_CHANNELS = 64
DV = 128
TOP = 2
BLOCK = 64
GROUP_SIZE = 4
CORES = 2

EPSILON = 1e-06
DECAY_NORMALIZER = 16.0
MESH = pl.DeviceIdType.MESH
BF16 = jnp.bfloat16
F32 = jnp.float32
PARTS = 4


def dot(a, b):
    return jnp.dot(a, b, preferred_element_type=F32)


class Place:
    def __init__(self, n_sp, n_tp, group):
        self.X, self.Z = group, n_sp // group
        self.C, self.Y = CORES, n_tp // CORES
        self.n_tp = n_tp
        self.sp, self.tp = lax.axis_index("sp"), lax.axis_index("tp")
        self.z, self.x = self.sp // self.X, self.sp % self.X
        self.y, self.c = self.tp // self.C, self.tp % self.C

    def at(self, z=None, x=None, y=None, c=None):
        z = self.z if z is None else z
        x = self.x if x is None else x
        y = self.y if y is None else y
        c = self.c if c is None else c
        return (z * self.X + x, y * self.C + c)


def remote(src, dst, send, recv, to):
    return pltpu.make_async_remote_copy(
        src_ref=src, dst_ref=dst, send_sem=send, recv_sem=recv, device_id=to, device_id_type=MESH
    )


def ring_index(way, step, part, steps):
    first = part % (PARTS // 2) if step == 1 else PARTS // 2 + (step - 2) * PARTS + part
    return way * ring_size(steps) + first


def ring_size(steps):
    return PARTS // 2 + (steps - 1) * PARTS


def way_parts(way):
    low, high = list(range(PARTS // 2)), list(range(PARTS // 2, PARTS))
    return (low, high) if way == 0 else (high, low)


def both_ways(pick):
    return [(way, part) for pair in zip(pick(0), pick(1)) for way, part in enumerate(pair)]


def whole(ref, sem):
    return pltpu.make_async_copy(ref, ref, sem)


def ring_sum(at, part_of, out, sends, recvs, send_sem, recv_sems):
    Y, steps, y = at.Y, at.Y // 2, at.y

    def copy(way, step, part):
        i = ring_index(way, step, part, steps)
        to = (y + 1) % Y if way == 0 else (y + Y - 1) % Y
        return remote(sends.at[i], recvs.at[i], send_sem, recv_sems.at[i], at.at(y=to))

    def offset(way, step):
        k = steps - step + 1
        return k if way == 0 or k == steps else -k

    def send(way, step, part, value):
        sends[ring_index(way, step, part, steps)] = value.astype(BF16)
        copy(way, step, part).start()

    for way, part in both_ways(lambda w: way_parts(w)[0]):
        send(way, 1, part, part_of(offset(way, 1), part))
    for step in range(2, steps + 1):
        for way, part in both_ways(lambda w: way_parts(w)[1] + way_parts(w)[0]):
            value = part_of(offset(way, step), part)
            if step > 2 or part in way_parts(way)[0]:
                copy(way, step - 1, part).wait_recv()
                value = value + recvs[ring_index(way, step - 1, part, steps)].astype(F32)
            send(way, step, part, value)
    for part in range(PARTS):
        total = part_of(0, part)
        for way in (0, 1):
            copy(way, steps, part).wait_recv()
            total = total + recvs[ring_index(way, steps, part, steps)].astype(F32)
        out(part, total)


def relay_sum(at, prepare, part_of, out, sends, recvs, send_sem, recv_sems):
    Y, y = at.Y, at.y
    hops = (2, 1, 2, 1)
    starts = (0, PARTS // 2, PARTS // 2 + PARTS, PARTS // 2 + 2 * PARTS)

    def slot(way, kind, part):
        return way * ring_size(Y // 2) + starts[kind] + (part % (PARTS // 2) if kind == 0 else part)

    def copy(way, kind, part):
        i = slot(way, kind, part)
        to = (y + hops[kind]) % Y if way == 0 else (y + Y - hops[kind]) % Y
        return remote(sends.at[i], recvs.at[i], send_sem, recv_sems.at[i], at.at(y=to))

    def send(way, kind, part, value):
        sends[slot(way, kind, part)] = value.astype(BF16)
        copy(way, kind, part).start()

    def received(way, kind, part):
        copy(way, kind, part).wait_recv()
        return recvs[slot(way, kind, part)].astype(F32)

    def own(way, k, part):
        return part_of(k if way == 0 or k == Y // 2 else -k, part)

    def direct(part):
        for way in (0, 1):
            send(way, 3, part, own(way, 1, part))

    for pair in zip(way_parts(0)[0], way_parts(1)[0]):
        for part in pair:
            prepare(part)
            for way in (0, 1):
                if part in way_parts(way)[0]:
                    send(way, 0, part, own(way, Y // 2, part))
                send(way, 1, part, own(way, 3, part))
    early = ()
    for part in early:
        direct(part)
    for way, part in both_ways(lambda w: way_parts(w)[1] + way_parts(w)[0]):
        value = own(way, 2, part) + received(way, 1, part)
        if part in way_parts(way)[0]:
            value = value + received(way, 0, part)
        send(way, 2, part, value)
    for part in range(PARTS):
        if part not in early:
            direct(part)
    for part in range(PARTS):
        total = part_of(0, part)
        for way in (0, 1):
            total = total + received(way, 3, part) + received(way, 2, part)
        out(part, total)


def far_first(count):
    return sorted(range(1, count), key=lambda k: (-min(k, count - k), k))


def near_order(count):
    return sorted(range(count), key=lambda k: (min(k, count - k), k))


def split(value):
    high = value.astype(BF16)
    rest = value - high.astype(F32)
    middle = rest.astype(BF16)
    return high, middle, (rest - middle.astype(F32)).astype(BF16)


def standing(row, count):
    square = (count, row.shape[1])
    same = lax.broadcasted_iota(jnp.int32, square, 0) == lax.broadcasted_iota(jnp.int32, square, 1)
    return jnp.sum(jnp.where(same, row, 0.0), axis=1, keepdims=True)


def lying(col, width):
    square = (col.shape[0], width)
    same = lax.broadcasted_iota(jnp.int32, square, 0) == lax.broadcasted_iota(jnp.int32, square, 1)
    return jnp.sum(jnp.where(same, col, 0.0), axis=0, keepdims=True)


def layer_kernel(
    n_sp, n_tp, group, cap,
    operands, residual, w_out, w_gate, w_up, w_down,
    out,
    held,
    gated, stack, facts, spread, find, told, heard, serve, merge, sx, rx, sz, rz,
    gu, wd, wo, partner, mixed, summed, both, mid, normed, block, rows, acc, hid, shares, result,
    zs, zr, xs, xb, zs2, zr2, column, branch,
    sa, ra, sb, rb,
    wsem, wrs, wrr, gsem, sums, gr, xrs, xbs, szs, szr, osem, done, came,
):
    at = Place(n_sp, n_tp, group)
    X, Y, Z, C = at.X, at.Y, at.Z, at.C
    x, y, z, c = at.x, at.y, at.z, at.c
    steps = Y // 2
    other = 1 - c

    (
        q_t, k_t, values, gate_rows, decay_t, bias, extra, head_gain,
        attention_gain, before_gain, after_gain, ids_row, weights_row,
    ) = held
    loads = [pltpu.make_async_copy(a, b, osem.at[k]) for k, (a, b) in enumerate(zip(operands, held))]
    for k in loads:
        k.start()
    local = [
        pltpu.make_async_copy(w_gate, gu.at[0], wsem.at[0]),
        pltpu.make_async_copy(w_up, gu.at[1], wsem.at[1]),
        pltpu.make_async_copy(w_down, wd.at[0], wsem.at[2]),
        pltpu.make_async_copy(w_out, wo.at[0], wsem.at[3]),
        pltpu.make_async_copy(residual, both.at[c], wsem.at[4]),
    ]
    rz[...] = jnp.zeros_like(rz)
    barrier = pltpu.get_barrier_semaphore()

    def greet_tp(k, carry):
        pl.semaphore_signal(barrier, inc=1, device_id=(at.sp, (at.tp + k) % n_tp), device_id_type=MESH)
        return carry

    lax.fori_loop(1, n_tp, greet_tp, 0)
    for k in range(1, Z):
        pl.semaphore_signal(barrier, inc=1, device_id=at.at(z=(z + k) % Z), device_id_type=MESH)
    for k in range(1, X):
        for core in range(C):
            pl.semaphore_signal(barrier, inc=1, device_id=at.at(x=(x + k) % X, c=core), device_id_type=MESH)

    for k in (3, 4, 0, 1, 2):
        local[k].start()
    for k in loads:
        k.wait()

    tokens = q_t.shape[1]
    blocks = tokens // BLOCK
    pre = decay_t[...].astype(F32) + standing(bias[...], KEY_CHANNELS)
    log_decay = -(jnp.maximum(-pre, 0.0) + jnp.log1p(jnp.exp(-jnp.abs(pre)))) / DECAY_NORMALIZER + extra[...]
    r, q = (lax.broadcasted_iota(jnp.int32, (tokens, tokens), k) for k in (0, 1))
    one_block = (r // BLOCK) == (q // BLOCK)
    upto = jnp.where((r <= q) & one_block, 1.0, 0.0).astype(BF16)
    inside = sum(dot(term, upto) for term in split(log_decay))
    ends = [inside[:, (b + 1) * BLOCK - 1 : (b + 1) * BLOCK] for b in range(blocks)]
    of_block = lax.broadcasted_iota(jnp.int32, (KEY_CHANNELS, tokens), 1) // BLOCK
    keys = k_t[...].astype(F32)
    to_end = [jnp.where(of_block == b, keys * jnp.exp(jnp.minimum(ends[b] - inside, 0.0)), 0.0) for b in range(blocks)]
    vals = values[...]
    growth = dot(jnp.concatenate(to_end, axis=0).astype(BF16), vals)
    growth = [growth[b * KEY_CHANNELS : (b + 1) * KEY_CHANNELS] for b in range(blocks)]
    fades = [jnp.exp(e) for e in ends]
    state = growth[0]
    for b in range(1, blocks):
        state = fades[b] * state + growth[b]
    fade_row = lying(jnp.exp(sum(ends)), DV)
    tail = KEY_CHANNELS + 16

    def message(ref, state_part, row):
        ref[0:KEY_CHANNELS, :] = state_part.astype(BF16)
        ref[KEY_CHANNELS:tail, :] = jnp.broadcast_to(row, (16, DV)).astype(BF16)

    message(sx, state, fade_row)
    pl.semaphore_wait(barrier, n_tp - 1 + Z - 1 + (X - 1) * C)

    def state_x(k):
        return remote(sx, rx.at[x], done.at[7], came.at[4], at.at(x=(x + k) % X))

    for k in range(1, X):
        state_x(k).start()
    pair = at.at(c=other)
    crossed = [
        remote(w_out, wo.at[1], wrs.at[3], wrr.at[3], pair),
        remote(w_gate, gu.at[2], wrs.at[0], wrr.at[0], pair),
        remote(w_up, gu.at[3], wrs.at[1], wrr.at[1], pair),
        remote(w_down, wd.at[1], wrs.at[2], wrr.at[2], pair),
    ]
    for k in crossed:
        k.start()
    lead = c == C - 1
    lent = remote(residual, both.at[0], gsem.at[4], gsem.at[5], pair)

    @pl.when(jnp.logical_not(lead))
    def _():
        lent.start()

    rx[pl.ds(x, 1)] = sx[...].reshape(1, tail, DV)

    slots = n_sp * cap
    seats = zs.shape[1]
    sub = lax.broadcasted_iota(jnp.int32, (n_sp, tokens), 0)
    chosen = [ids_row[k : k + 1, :] for k in range(TOP)]
    named = jnp.where((sub == chosen[0]) | (sub == chosen[1]), 1.0, 0.0).astype(BF16)
    before = dot(named, jnp.where(r < q, 1.0, 0.0).astype(BF16))
    targets = []
    plane_of = chosen[0] // X
    order = near_order(Z)
    group_size = Z // 2
    away = z - plane_of
    away = jnp.where(away < 0, away + Z, away)
    base = jnp.zeros_like(away)
    for i, k in enumerate(order):
        start = (i // group_size) * (X * group_size * cap) + (i % group_size) * cap
        base = jnp.where(away == k, start, base)
    for e in chosen:
        slot = jnp.sum(jnp.where(sub == e, before, 0.0), axis=0, keepdims=True)
        targets.append((e - plane_of * X) * (group_size * cap) + base + slot.astype(jnp.int32))
    sub = lax.broadcasted_iota(jnp.int32, (Z, tokens), 0)
    before = dot(jnp.where(sub == plane_of, 1.0, 0.0).astype(BF16), jnp.where(r < q, 1.0, 0.0).astype(BF16))
    rank = jnp.sum(jnp.where(sub == plane_of, before, 0.0), axis=0, keepdims=True)
    seat = plane_of * seats + rank.astype(jnp.int32)
    query = q_t[...].astype(F32) * (KEY_CHANNELS**-0.5 * jnp.exp(inside))
    stack[0:KEY_CHANNELS, :] = query
    stack[KEY_CHANNELS:, :] = jnp.zeros((stack.shape[0] - KEY_CHANNELS, tokens), F32)
    stack[KEY_CHANNELS : KEY_CHANNELS + 1, :] = seat.astype(F32)
    facts[...] = jnp.zeros_like(facts)
    for k in range(TOP):
        facts[k : k + 1, :] = (targets[k] + 1).astype(F32)
        facts[TOP + k : TOP + k + 1, :] = weights_row[k : k + 1, :]
    stood = stack[...].T
    query = stood[:, 0:KEY_CHANNELS].astype(BF16)
    seat_col = stood[:, KEY_CHANNELS : KEY_CHANNELS + 1].astype(jnp.int32)
    scores = dot(query, (keys * jnp.exp(-inside)).astype(BF16))
    scores = jnp.where((r >= q) & one_block, scores, 0.0).astype(BF16)
    within = dot(scores, vals)

    whole(rx.at[pl.ds(0, X - 1)], came.at[4]).wait()
    plane, plane_row = rx[0, 0:KEY_CHANNELS].astype(F32), rx[0, KEY_CHANNELS:tail][0:1].astype(F32)
    ahead, ahead_fade = jnp.zeros_like(state), jnp.ones((KEY_CHANNELS, 1), F32)
    for k in range(X):
        part, row = rx[k, 0:KEY_CHANNELS].astype(F32), rx[k, KEY_CHANNELS:tail][0:1].astype(F32)
        fade = standing(row, KEY_CHANNELS)
        ahead = jnp.where(k < x, fade * ahead + part, ahead)
        ahead_fade = jnp.where(k < x, fade * ahead_fade, ahead_fade)
        if k:
            plane, plane_row = fade * plane + part, plane_row * row
    message(sz, plane, plane_row)

    def state_z(k):
        return remote(sz, rz.at[z], szs.at[k], szr.at[k], at.at(z=(z + k) % Z))

    for k in far_first(Z):

        @pl.when(z + k < Z)
        def _(k=k):
            state_z(k).start()

    all_seats = Z * seats
    tall = lax.broadcasted_iota(jnp.int32, (all_seats, tokens), 0)
    spread[...] = jnp.where(tall == seat, 1.0, 0.0).astype(BF16)
    wide = lax.broadcasted_iota(jnp.int32, (tokens, all_seats), 1)
    find[...] = jnp.where(wide == seat_col, 1.0, 0.0).astype(BF16)
    listed = sum(dot(term, find[...]) for term in split(facts[...]))
    near = lax.broadcasted_iota(jnp.int32, (8, DV), 1) < seats
    for k in range(Z):
        moved = pltpu.roll(listed, (all_seats - k * seats) % all_seats, 1) if k else listed
        told[k] = jnp.where(near, moved[:, 0:DV], 0.0)

    def tell(k):
        return remote(
            told.at[(z + k) % Z], heard.at[order.index(Z - k)], done.at[10], came.at[6], at.at(z=(z + k) % Z)
        )

    for k in far_first(Z):
        tell(k).start()
    heard[0:1] = told[pl.ds(z, 1)]
    gate_act = gate_rows[...].astype(F32)
    gate_act = gate_act * jax.nn.sigmoid(gate_act) * head_gain[...]

    for k in range(1, Z):

        @pl.when(z >= k)
        def _(k=k):
            state_z(k).wait_recv()

    carried = jnp.zeros_like(state)
    for k in range(Z - 1):
        fade = standing(rz[k, KEY_CHANNELS:tail][0:1].astype(F32), KEY_CHANNELS)
        carried = jnp.where(k < z, fade * carried + rz[k, 0:KEY_CHANNELS].astype(F32), carried)
    running = ahead_fade * carried + ahead
    across = []
    for b in range(blocks):
        across.append(dot(query[b * BLOCK : (b + 1) * BLOCK], running.astype(BF16)))
        running = fades[b] * running + growth[b]
    heads = within + jnp.concatenate(across, axis=0)
    heads = heads * lax.rsqrt(jnp.mean(heads * heads, axis=1, keepdims=True) + EPSILON) * gate_act
    gated[...] = heads.astype(BF16).reshape(gated.shape)
    swap = remote(gated, partner, gsem.at[0], gsem.at[1], pair)

    @pl.when(jnp.logical_not(lead))
    def _():
        swap.start()


    piece = gated.shape[2]
    width = wo.shape[2]
    local[3].wait()
    crossed[0].wait_recv()
    part_width = width // PARTS
    handed = remote(mid.at[0], mid.at[0], gsem.at[2], gsem.at[3], pair)

    def mixed_part(k, part):
        d = (y + k + Y) % Y
        return mixed[pl.ds(d, 1), :, part * part_width : (part + 1) * part_width].reshape(C * piece, part_width)

    def keep(part, value):
        summed[:, :, part * part_width : (part + 1) * part_width] = value.reshape(C, piece, part_width)

    @pl.when(lead)
    def _():
        swap.wait_recv()
        heads_of = jnp.concatenate([gated[...].reshape(tokens, DV), partner[...].reshape(tokens, DV)], axis=1)

        def prepare(part):
            cols = slice(part * part_width, (part + 1) * part_width)
            value = dot(heads_of, wo[:, :, cols].reshape(2 * DV, part_width))
            mixed[:, :, cols] = value.reshape(Y, C * piece, part_width)

        relay_sum(at, prepare, mixed_part, keep, sa, ra, done.at[0], sums)
        lent.wait_recv()
        local[4].wait()
        attn = summed[...].reshape(C * piece, width)
        attn = attn * lax.rsqrt(jnp.mean(attn * attn, axis=1, keepdims=True) + EPSILON) * attention_gain[...]
        m = (both[...].reshape(C * piece, width).astype(F32) + attn).astype(BF16)
        mid[...] = m.reshape(C, piece, width)
        m = m.astype(F32)
        m = m * lax.rsqrt(jnp.mean(m * m, axis=1, keepdims=True) + EPSILON) * before_gain[...]
        normed[...] = m.astype(BF16)

    def share_cols(t):
        return pl.ds(pl.multiple_of(t * DV, DV), DV)

    def share_rows(t):
        return pl.ds(pl.multiple_of(t * piece, piece), piece)

    chip_rows = pl.ds(pl.multiple_of(y * (C * piece), C * piece), C * piece)

    def to_width(k):
        t = (at.tp + k) % n_tp
        return remote(normed.at[:, share_cols(t)], block.at[chip_rows, :], done.at[3], came.at[0], (at.sp, t))

    def start_width(k, carry):
        to_width(k).start()
        return carry

    @pl.when(lead)
    def _():
        lax.fori_loop(1, n_tp, start_width, 0)
        handed.start()
        block[chip_rows, :] = normed[:, share_cols(at.tp)]

    @pl.when(jnp.logical_not(lead))
    def _():
        local[4].wait()

    whole(heard.at[pl.ds(1, Z - 1)], came.at[6]).wait()
    lists = None
    for k in range(Z):
        part = jnp.concatenate([heard[k], jnp.zeros((8, all_seats - DV), F32)], axis=1)
        part = pltpu.roll(part, k * seats, 1) if k else part
        lists = part if lists is None else lists + part
    tall = lax.broadcasted_iota(jnp.int32, (slots, all_seats), 0)
    hits = [jnp.where(tall == lists[k : k + 1, :].astype(jnp.int32) - 1, 1.0, 0.0) for k in range(TOP)]
    serve[...] = (hits[0] + hits[1]).astype(BF16)
    stood = jnp.concatenate([lists, jnp.zeros((DV - 8, all_seats), F32)], axis=0).T
    wide = lax.broadcasted_iota(jnp.int32, (all_seats, slots), 1)
    for k in range(TOP):
        merge[k] = jnp.where(wide == stood[:, k : k + 1].astype(jnp.int32) - 1, 1.0, 0.0).astype(BF16)
    shares_of = [stood[:, TOP + k : TOP + k + 1] for k in range(TOP)]
    others = block.at[pl.ds(0, (n_tp - 1) * piece)]

    @pl.when(lead)
    def _():
        whole(block.at[pl.ds(0, (Y - 1) * C * piece)], came.at[0]).wait()

    @pl.when(jnp.logical_not(lead))
    def _():
        whole(block, came.at[0]).wait()

    picked = dot(spread[...], block[...]).astype(BF16)
    zs[...] = picked.reshape(zs.shape)

    def z_out(k):
        i = order.index(Z - k)
        return remote(
            zs.at[(z + k) % Z], zr.at[i], done.at[5], came.at[2 if i < group_size else 7], at.at(z=(z + k) % Z)
        )

    for k in order[1:]:
        z_out(Z - k).start()
    zr[0:1] = zs[pl.ds(z, 1)]

    side = x % C
    mine_half = x // C
    per = PARTS // 2

    def x_out(half, k):
        to = (x + k) % X
        return (
            xs.at[half, to],
            rows.at[y, half * per + mine_half, :, share_cols(c)],
            done.at[8 if k else 9],
            xrs.at[half],
            at.at(x=to, c=side),
        )

    for half in (0, 1):
        first = 1 - half
        arrived = zr.at[pl.ds(half * group_size + first, group_size - first)]
        whole(arrived, came.at[7 if half else 2]).wait()
        listed_rows = slice(half * (slots // 2), (half + 1) * (slots // 2))
        listed_seats = slice(half * (all_seats // 2), (half + 1) * (all_seats // 2))
        group_rows = zr[half * group_size : (half + 1) * group_size].reshape(all_seats // 2, DV)
        picked = dot(serve[listed_rows, listed_seats], group_rows)
        xs[half] = picked.astype(BF16).reshape(xs.shape[1:])
        for k in range(1, X):
            remote(*x_out(half, k)).start()
        src, dst, s_sem, r_sem, to = x_out(half, 0)

        @pl.when(side == c)
        def _(src=src, dst=dst, r_sem=r_sem):
            pltpu.make_async_copy(src, dst, r_sem).start()

        @pl.when(side != c)
        def _(args=(src, dst, s_sem, r_sem, pair)):
            remote(*args).start()

    def gather(way, step, part):
        j = (y + Y - (step - 1)) % Y if way == 0 else (y + step - 1) % Y
        to = (y + 1) % Y if way == 0 else (y + Y - 1) % Y
        i = way * ring_size(steps) + (step - 1) * PARTS + (part if step < steps else part % per)
        return remote(rows.at[j, part], rows.at[j, part], done.at[2], gr.at[i], at.at(y=to))

    def start_gather(way, step, part):
        gather(way, step, part).start()

    for half in (0, 1):
        whole(rows.at[y, pl.ds(half * per, per)], xrs.at[half]).wait()
        for part in range(half * per, half * per + per):
            for way in (0, 1):
                start_gather(way, 1, part)

    count = rows.shape[1] * rows.shape[2]
    chunk = rows.shape[3]
    local[0].wait()
    local[1].wait()
    crossed[1].wait_recv()
    crossed[2].wait_recv()

    def grow(j, first=False):
        a = rows[pl.ds(j, 1)].reshape(count, chunk)
        at_rows = pl.ds(pl.multiple_of(j * chunk, chunk), chunk)
        for k in range(4):
            value = dot(a, gu[k, at_rows, :])
            acc[k] = value if first else acc[k] + value

    grow(y, True)
    for step in range(1, steps):
        for part in range(PARTS):
            for way in (0, 1):
                gather(way, step, part).wait_recv()
                if step + 1 < steps or way == part // per:
                    start_gather(way, step + 1, part)
        grow((y + Y - step) % Y)
        grow((y + step) % Y)
    for part in range(PARTS):
        gather(part // per, steps, part).wait_recv()
    grow((y + steps) % Y)

    for k in (0, 1):
        gate, up = acc[2 * k], acc[2 * k + 1]
        hid[k] = (gate * jax.nn.sigmoid(gate) * up).astype(BF16)

    local[2].wait()
    crossed[3].wait_recv()
    made = {}

    def down(offset):
        d = (y + offset + Y) % Y
        cols = pl.ds(pl.multiple_of(d * chunk, chunk), chunk)
        value = dot(hid[0], wd[0, :, cols]) + dot(hid[1], wd[1, :, cols])
        shares[offset + steps - 1] = value.reshape(PARTS, count // PARTS, chunk)

    def down_part(offset, part):
        if offset not in made:
            down(offset)
            made[offset] = True
        return shares[offset + steps - 1, part]

    def x_back(half, column_of, core):
        home = column_of * C + c
        return (
            result.at[half * per + column_of, :, pl.ds(core * DV, DV)],
            xb.at[half, x],
            xbs.at[(half * per + column_of) * C + core],
            came.at[5],
            at.at(x=home, c=core),
        ), (home == x) & (c == core)

    def keep_result(part, value):
        result[part] = value.astype(BF16)
        for core in range(C):
            args, here = x_back(part // per, part % per, core)

            @pl.when(here)
            def _(args=args):
                pltpu.make_async_copy(args[0], args[1], args[3]).start()

            @pl.when(jnp.logical_not(here))
            def _(args=args):
                remote(*args).start()

    ring_sum(at, down_part, keep_result, sb, rb, done.at[1], sums)

    whole(xb, came.at[5]).wait()
    served = xb[...].reshape(slots, DV)
    served = shares_of[0] * dot(merge[0], served) + shares_of[1] * dot(merge[1], served)
    zs2[...] = served.astype(BF16).reshape(zs2.shape)

    def z_back(k):
        return remote(zs2.at[order.index(k)], zr2.at[z], done.at[6], came.at[3], at.at(z=(z + k) % Z))

    for k in far_first(Z):
        z_back(k).start()
    zr2[pl.ds(z, 1)] = zs2[0:1]
    whole(zr2.at[pl.ds(0, Z - 1)], came.at[3]).wait()
    column[...] = dot(find[...], zr2[...].reshape(all_seats, DV)).astype(BF16)

    def to_rows(k):
        t = (at.tp + k) % n_tp
        return remote(
            column.at[share_rows(t), :], branch.at[:, share_cols(at.tp)], done.at[4], came.at[1], (at.sp, t)
        )

    def start_rows(k, carry):
        to_rows(k).start()
        return carry

    lax.fori_loop(1, n_tp, start_rows, 0)
    branch[:, share_cols(at.tp)] = column[share_rows(at.tp), :]
    whole(others, came.at[1]).wait()
    b = branch[...].astype(F32)
    b = b * lax.rsqrt(jnp.mean(b * b, axis=1, keepdims=True) + EPSILON) * after_gain[...]

    @pl.when(jnp.logical_not(lead))
    def _():
        handed.wait_recv()

    out[...] = (mid[pl.ds(c, 1)].reshape(piece, width).astype(F32) + b).astype(BF16)

    whole(rx.at[pl.ds(0, X - 1)], done.at[7]).wait()
    for k in range(1, Z):

        @pl.when(z + k < Z)
        def _(k=k):
            state_z(k).wait_send()

    @pl.when(jnp.logical_not(lead))
    def _():
        swap.wait_send()
        lent.wait_send()

    @pl.when(lead)
    def _():
        handed.wait_send()
        whole(normed.at[:, pl.ds(0, (n_tp - 1) * DV)], done.at[3]).wait()
        whole(sa, done.at[0]).wait()

    for k in crossed:
        k.wait_send()
    whole(sb, done.at[1]).wait()
    whole(rows.at[pl.ds(0, Y - 1)], done.at[2]).wait()
    whole(others, done.at[4]).wait()
    whole(zr.at[pl.ds(0, Z - 1)], done.at[5]).wait()
    whole(told.at[pl.ds(0, Z - 1)], done.at[10]).wait()
    whole(zr2.at[pl.ds(0, Z - 1)], done.at[6]).wait()
    whole(xs.at[:, pl.ds(0, X - 1)], done.at[8]).wait()

    @pl.when(side != c)
    def _():
        whole(xs.at[:, 0], done.at[9]).wait()

    for part in range(PARTS):
        for core in range(C):
            args, here = x_back(part // per, part % per, core)

            @pl.when(jnp.logical_not(here))
            def _(args=args):
                remote(*args).wait_send()


def shards(
    query, key, value, gate_rows, decay, bias, extra, head_gain, output_projection, residual,
    attention_gain, before_gain, after_gain, w_gate, w_up, w_down, ids, weights,
):
    n_sp, n_tp = lax.axis_size("sp"), lax.axis_size("tp")
    tokens, width = query.shape[0], residual.shape[1]
    piece = residual.shape[0]
    X, C = GROUP_SIZE, CORES
    Z, Y = n_sp // X, n_tp // C
    cap = 5 * tokens // (2 * n_sp)
    slots = n_sp * cap
    seats = -(-(X * cap // TOP) // 16) * 16
    steps = Y // 2
    msgs = 2 * ring_size(steps)
    part = slots // C // PARTS
    chunk = C * DV
    hidden = w_gate.shape[2]
    hbm = pl.BlockSpec(memory_space=pltpu.HBM)
    sem = pltpu.SemaphoreType.DMA
    message = (KEY_CHANNELS + 16, DV)
    operands = [
        query.T, key.T, value, gate_rows, decay.T, bias[None], extra.T, head_gain[None],
        attention_gain[None], before_gain[None], after_gain[None], ids.T, weights.T,
    ]
    scratch = [
        [pltpu.VMEM(a.shape, a.dtype) for a in operands],
        pltpu.VMEM((Y, C, piece, DV), BF16),
        pltpu.VMEM((128, tokens), F32),
        pltpu.VMEM((8, tokens), F32),
        pltpu.VMEM((Z * seats, tokens), BF16),
        pltpu.VMEM((tokens, Z * seats), BF16),
        pltpu.VMEM((Z, 8, DV), F32),
        pltpu.VMEM((Z, 8, DV), F32),
        pltpu.VMEM((slots, Z * seats), BF16),
        pltpu.VMEM((TOP, Z * seats, slots), BF16),
        pltpu.VMEM(message, BF16),
        pltpu.VMEM((X, *message), BF16),
        pltpu.VMEM(message, BF16),
        pltpu.VMEM((Z, *message), BF16),
        pltpu.VMEM((4, width, hidden), BF16),
        pltpu.VMEM((2, hidden, width), BF16),
        pltpu.VMEM((2, DV, width), BF16),
        pltpu.VMEM((Y, C, piece, DV), BF16),
        pltpu.VMEM((Y, C * piece, width), F32),
        pltpu.VMEM((C, piece, width), F32),
        pltpu.VMEM((C, piece, width), BF16),
        pltpu.VMEM((C, piece, width), BF16),
        pltpu.VMEM((C * piece, width), BF16),
        pltpu.VMEM((tokens, DV), BF16),
        pltpu.VMEM((Y, PARTS, part, chunk), BF16),
        pltpu.VMEM((4, PARTS * part, hidden), F32),
        pltpu.VMEM((2, PARTS * part, hidden), BF16),
        pltpu.VMEM((Y, PARTS, part, chunk), F32),
        pltpu.VMEM((PARTS, part, chunk), BF16),
        pltpu.VMEM((Z, seats, DV), BF16),
        pltpu.VMEM((Z, seats, DV), BF16),
        pltpu.VMEM((2, X, part, DV), BF16),
        pltpu.VMEM((2, X, part, DV), BF16),
        pltpu.VMEM((Z, seats, DV), BF16),
        pltpu.VMEM((Z, seats, DV), BF16),
        pltpu.VMEM((tokens, DV), BF16),
        pltpu.VMEM((piece, width), BF16),
        pltpu.VMEM((msgs, C * piece, width // PARTS), BF16),
        pltpu.VMEM((msgs, C * piece, width // PARTS), BF16),
        pltpu.VMEM((msgs, part, chunk), BF16),
        pltpu.VMEM((msgs, part, chunk), BF16),
        sem((5,)), sem((4,)), sem((4,)), sem((6,)), sem((msgs,)), sem((msgs,)), sem((2,)), sem((PARTS * C,)),
        sem((Z,)), sem((Z,)), sem((len(operands),)), sem((11,)), sem((8,)),
    ]
    return pl.pallas_call(
        functools.partial(layer_kernel, n_sp, n_tp, X, cap),
        out_shape=jax.ShapeDtypeStruct((piece, width), BF16),
        in_specs=[[hbm] * len(operands), hbm, hbm, hbm, hbm, hbm],
        out_specs=pl.BlockSpec(memory_space=pltpu.VMEM),
        scratch_shapes=scratch,
        name="layer",
        compiler_params=pltpu.CompilerParams(
            collective_id=0, has_side_effects=True, vmem_limit_bytes=40 * 1024 * 1024
        ),
    )(
        *jax.tree.map(lambda a: pltpu.with_memory_space_constraint(a, pltpu.HBM), (operands, residual, output_projection, w_gate[0], w_up[0], w_down[0]))
    )


def solution(mesh):
    placed = (
        P("sp", "tp"),
        P("sp", "tp"),
        P("sp", "tp"),
        P("sp", "tp"),
        P("sp", "tp"),
        P("tp"),
        P("sp", "tp"),
        P(),
        P("tp", None),
        P(("sp", "tp"), None),
        P(),
        P(),
        P(),
        P("sp", None, "tp"),
        P("sp", None, "tp"),
        P("sp", "tp", None),
        P("sp", None),
        P("sp", None),
    )
    return jax.shard_map(
        shards, mesh=mesh, in_specs=placed, out_specs=P(("sp", "tp"), None), check_vma=False
    )
```
